32 devices in a mesh: sp: 8 (over z, x), tp: 4 (over y, core).
Axes of the slice: x: 2, y: 2, z: 4, core: 2. Of those that a mesh axis runs over, the one named last changes fastest.
Arguments:
- tokens: bfloat16 [2048, 3072], P('sp', 'tp'), may hold values from -6 to 6
- norm_gain: float32 [3072], replicated, may hold values from 0.1 to 1.9
- state_in_weight: bfloat16 [3072, 1024], P('sp', 'tp'), may hold values from -0.109375 to 0.109375
- pool_in_weight: bfloat16 [3072, 1024], P('sp', 'tp'), may hold values from -0.109375 to 0.109375
- rate_real: float32 [64, 64], replicated, may hold values from -1.5 to -0.5
- rate_imag: float32 [64, 64], replicated, may hold values from 0 to 200
- log_step: float32 [64], replicated, may hold values from -2 to 0.7
- input_real: float32 [64, 64, 16], replicated, may hold values from -1 to 1
- input_imag: float32 [64, 64, 16], replicated, may hold values from -1 to 1
- output_real: float32 [64, 16, 64], replicated, may hold values from -64 to 64
- output_imag: float32 [64, 16, 64], replicated, may hold values from -64 to 64
- skip_gain: float32 [1024], replicated, may hold values from -3 to 3
- pool_weight: bfloat16 [16, 64, 64], replicated, may hold values from -0.75 to 0.75
- pool_gain: float32 [1024], replicated, may hold values from 0.1 to 1.9
- state_out_weight: bfloat16 [1024, 3072], P('sp', 'tp'), may hold values from -0.125 to 0.125
- pool_out_weight: bfloat16 [1024, 3072], P('sp', 'tp'), may hold values from -0.125 to 0.125
Outputs:
- mixer_output: bfloat16 [2048, 3072], P('sp', 'tp')
The draws below stay inside these ranges and needn't reach their ends.
All inputs are finite; a program needn't handle non-finite values.
Results may differ from the reference program's by a relative error of at most 0.0065.
Values may be sent and summed in bfloat16 or wider, within the bound.
A program may use at most 64 MiB of HBM per device.

```python
import jax
import jax.numpy as jnp
from jax import lax

D = 3072
SSM_GROUP = 16
SSM_GROUPS = 64
SSM_STATE = 64
POOL_GROUP = 64
POOL_GROUPS = 16
TOKENS = 2048
D_SSM = 1024
D_POOL = 1024


def level_of(key, dims, cuts, smallest, largest):
    gain, own = 1.0, jax.random.fold_in(key, 6)
    for axis_at, shards_of in cuts:
        draws = jnp.exp(jax.random.uniform(jax.random.fold_in(own, axis_at), (shards_of,), jnp.float32, smallest / len(cuts), largest / len(cuts)))
        gain = gain * jnp.repeat(draws, dims[axis_at] // shards_of).reshape([-1 if axis == axis_at else 1 for axis in range(len(dims))])
    return gain


def normal_values(rng, extent, scale, limit, split=(), held_as=jnp.bfloat16):
    array = scale * jax.random.normal(rng, extent, jnp.float32)
    if split:
        array = array * level_of(rng, extent, split, -0.22, 0.18)
    return jnp.clip(array, -limit, limit).astype(held_as)


def setup_inputs(seed: int = 0) -> dict:
    streams_of = jax.random.split(jax.random.key(seed), 17)
    return {
        "tokens": normal_values(streams_of[0], (TOKENS, D), 1.0, 6.0, ((0, 8), (1, 4))),
        "norm_gain": jnp.clip(1.0 + 0.18 * jax.random.normal(streams_of[1], (D,), jnp.float32), 0.1, 1.9),
        "state_in_weight": normal_values(streams_of[2], (D, D_SSM), D ** -0.5, 0.109375, ((0, 8), (1, 4))),
        "pool_in_weight": normal_values(streams_of[3], (D, D_POOL), D ** -0.5, 0.109375, ((0, 8), (1, 4))),
        "rate_real": jnp.clip(jax.random.uniform(streams_of[4], (SSM_GROUPS, SSM_STATE), jnp.float32, -1.5, -0.5), -1.5, -0.5),
        "rate_imag": jnp.clip(jax.random.uniform(streams_of[5], (SSM_GROUPS, SSM_STATE), jnp.float32, 0.0, 200.0), 0.0, 200.0),
        "log_step": jnp.clip(jax.random.uniform(streams_of[6], (SSM_GROUPS,), jnp.float32, -2.0, 0.7), -2.0, 0.7),
        "input_real": normal_values(streams_of[7], (SSM_GROUPS, SSM_STATE, SSM_GROUP), (2 * SSM_GROUP) ** -0.5, 1.0, (), jnp.float32),
        "input_imag": normal_values(streams_of[8], (SSM_GROUPS, SSM_STATE, SSM_GROUP), (2 * SSM_GROUP) ** -0.5, 1.0, (), jnp.float32),
        "output_real": normal_values(streams_of[9], (SSM_GROUPS, SSM_GROUP, SSM_STATE), (TOKENS // 256 + 2), 64.0, (), jnp.float32),
        "output_imag": normal_values(streams_of[10], (SSM_GROUPS, SSM_GROUP, SSM_STATE), (TOKENS // 256 + 2), 64.0, (), jnp.float32),
        "skip_gain": normal_values(streams_of[11], (D_SSM,), 0.5, 3.0, (), jnp.float32),
        "pool_weight": normal_values(streams_of[12], (POOL_GROUPS, POOL_GROUP, POOL_GROUP), POOL_GROUP ** -0.5, 0.75),
        "pool_gain": jnp.clip(1.0 + 0.18 * jax.random.normal(streams_of[13], (D_POOL,), jnp.float32), 0.1, 1.9),
        "state_out_weight": normal_values(streams_of[14], (D_SSM, D), (D_SSM + D_POOL) ** -0.5, 0.125, ((0, 8), (1, 4))),
        "pool_out_weight": normal_values(streams_of[15], (D_POOL, D), (D_SSM + D_POOL) ** -0.5, 0.125, ((0, 8), (1, 4))),
    }


epsilon = 1e-06
highest = lax.Precision.HIGHEST

def discretize(rate_real, rate_imag, log_step, length):
    step_size = jnp.exp(log_step)[:, None] / length
    exponent = rate_real * step_size
    angle = rate_imag * step_size
    magnitude = jnp.exp(exponent)
    decay_real = magnitude * jnp.cos(angle)
    decay_imag = magnitude * jnp.sin(angle)
    less_one = jnp.expm1(exponent) * jnp.cos(angle) - 2.0 * jnp.square(jnp.sin(0.5 * angle))
    denominator = rate_real * rate_real + rate_imag * rate_imag
    factor_real = (less_one * rate_real + decay_imag * rate_imag) / denominator
    factor_imag = (decay_imag * rate_real - less_one * rate_imag) / denominator
    return (exponent, angle, decay_real, decay_imag, factor_real, factor_imag)

def drive_terms(signal, factor_real, factor_imag, input_real, input_imag):
    drive_real = factor_real[..., None] * input_real - factor_imag[..., None] * input_imag
    drive_imag = factor_real[..., None] * input_imag + factor_imag[..., None] * input_real
    push_real = jnp.einsum('tgc,gnc->tgn', signal, drive_real, precision=highest)
    push_imag = jnp.einsum('tgc,gnc->tgn', signal, drive_imag, precision=highest)
    return (push_real, push_imag)

def readout(states_real, states_imag, output_real, output_imag, signal, skip_gain):
    row_count = states_real.shape[0]
    readout_sum = jnp.einsum('tgn,gcn->tgc', states_real, output_real, precision=highest)
    readout_sum = readout_sum - jnp.einsum('tgn,gcn->tgc', states_imag, output_imag, precision=highest)
    readout_sum = readout_sum.reshape(row_count, -1) + skip_gain * signal.reshape(row_count, -1)
    return jax.nn.gelu(readout_sum).astype(jnp.bfloat16)

def pool_mixer(pool_in, pool_weight, pool_gain):
    row_count = pool_in.shape[0]
    signal = pool_in.astype(jnp.float32).reshape(row_count, POOL_GROUPS, POOL_GROUP)
    running = jnp.cumsum(signal, axis=0)
    padded = jnp.pad(running, ((16, 0), (0, 0), (0, 0)))
    positions = jnp.arange(1, row_count + 1)
    window_means = []
    for group_index in range(POOL_GROUPS):
        window = 2 ** (group_index % 4 + 1)
        lagged = padded[16 - window:16 - window + row_count, group_index]
        divisor = jnp.minimum(positions, window).astype(jnp.float32)[:, None]
        window_means.append((running[:, group_index] - lagged) / divisor)
    pooled = jnp.stack(window_means, axis=1) - signal
    projected = jnp.einsum('tgc,gcd->tgd', pooled, pool_weight.astype(jnp.float32), precision=highest)
    return (projected.reshape(row_count, -1) * pool_gain).astype(jnp.bfloat16)

def reference(tokens, norm_gain, state_in_weight, pool_in_weight, rate_real, rate_imag, log_step, input_real, input_imag, output_real, output_imag, skip_gain, pool_weight, pool_gain, state_out_weight, pool_out_weight):
    features = tokens.astype(jnp.float32)
    inverse = lax.rsqrt(lax.optimization_barrier(jnp.sum(features * features, axis=1)) / D + epsilon)[:, None]
    scaled = (features * norm_gain).astype(jnp.bfloat16)
    state_in = (jnp.dot(scaled, state_in_weight, preferred_element_type=jnp.float32) * inverse).astype(jnp.bfloat16)
    pool_in = (jnp.dot(scaled, pool_in_weight, preferred_element_type=jnp.float32) * inverse).astype(jnp.bfloat16)
    signal = state_in.astype(jnp.float32).reshape(TOKENS, SSM_GROUPS, SSM_GROUP)
    exponent, angle, decay_real, decay_imag, factor_real, factor_imag = discretize(rate_real, rate_imag, log_step, TOKENS)
    push_real, push_imag = drive_terms(signal, factor_real, factor_imag, input_real, input_imag)

    def advance(carry, pushes):
        state_real, state_imag = carry
        next_real = decay_real * state_real - decay_imag * state_imag + pushes[0]
        next_imag = decay_real * state_imag + decay_imag * state_real + pushes[1]
        return ((next_real, next_imag), (next_real, next_imag))
    zero_state = jnp.zeros((SSM_GROUPS, SSM_STATE), jnp.float32)
    _, (states_real, states_imag) = lax.scan(advance, (zero_state, zero_state), (push_real, push_imag))
    state_out = readout(states_real, states_imag, output_real, output_imag, signal, skip_gain)
    pool_out = pool_mixer(pool_in, pool_weight, pool_gain)
    combined = jnp.dot(state_out, state_out_weight, preferred_element_type=jnp.float32)
    combined = combined + jnp.dot(pool_out, pool_out_weight, preferred_element_type=jnp.float32)
    return combined.astype(jnp.bfloat16)
```

```python
import functools

import jax
import jax.numpy as jnp
from jax import lax
from jax.experimental import pallas as pl
from jax.experimental.pallas import tpu as pltpu
from jax.sharding import PartitionSpec as P

SSM_GROUP = 16
POOL_GROUP = 64
CHUNKS = 8
PIECES = 2

epsilon = 1e-06
window_reach = 16
f32, bf16 = jnp.float32, jnp.bfloat16
MESH = pl.DeviceIdType.MESH


def discretize(rate_real, rate_imag, log_step, length):
    step_size = jnp.exp(log_step)[:, None] / length
    exponent = rate_real * step_size
    angle = rate_imag * step_size
    magnitude = jnp.exp(exponent)
    decay_real = magnitude * jnp.cos(angle)
    decay_imag = magnitude * jnp.sin(angle)
    less_one = jnp.expm1(exponent) * jnp.cos(angle) - 2.0 * jnp.square(jnp.sin(0.5 * angle))
    denominator = rate_real * rate_real + rate_imag * rate_imag
    factor_real = (less_one * rate_real + decay_imag * rate_imag) / denominator
    factor_imag = (decay_imag * rate_real - less_one * rate_imag) / denominator
    return decay_real, decay_imag, factor_real, factor_imag


def iota(shape, axis):
    return lax.broadcasted_iota(jnp.int32, shape, axis)


def dot(a, b):
    return jnp.dot(a, b, preferred_element_type=f32)


def dot_nt(a, b):
    return lax.dot_general(a, b, (((1,), (1,)), ((), ())), preferred_element_type=f32)


def split(a):
    high = a.astype(bf16)
    return high, (a - high.astype(f32)).astype(bf16)


def cmul(ar, ai, br, bi):
    return ar * br - ai * bi, ar * bi + ai * br


def kernel(
    n_sp, n_tp, n_x, states,
    tok_ref, gain_ref, wsi_ref, wpi_ref, rr_ref, ri_ref, step_ref, inr_ref, ini_ref, outr_ref,
    outi_ref, skip_ref, pw_ref, pg_ref, wso_ref, wpo_ref,
    out_ref,
    tok_full, wsi, wpi, wso, wpo, scaled, dmat, rmat, pmat, push, ext, halo, ends, act,
    mine_s, mine_p, halo_out, rates, matrices, pool_own, dec_ref,
    own_sem, ring_send, ring_recv, tok_send, tok_recv, act_send, act_recv, halo_sem, end_send, end_recv,
):
    me, tp = lax.axis_index("sp"), lax.axis_index("tp")
    n_z = n_sp // n_x
    rows = tok_ref.shape[0]
    features = tok_ref.shape[1]
    width = wsi_ref.shape[1]
    pool_width = wpi_ref.shape[1]
    groups = width // SSM_GROUP
    columns = groups * states
    pool_groups = pool_width // POOL_GROUP
    span = rows // CHUNKS

    def place(p):
        x, r = p // n_z, p % n_z
        return (r + (x % 2) * (n_z - 1 - 2 * r)) * n_x + x

    my_x, my_z = me % n_x, me // n_x
    at = my_x * n_z + my_z + (my_x % 2) * (n_z - 1 - 2 * my_z)

    barrier = pltpu.get_barrier_semaphore()
    for k in range(1, n_sp):
        pl.semaphore_signal(barrier, inc=1, device_id=((me + k) % n_sp, tp), device_id_type=MESH)
    for k in range(1, n_tp):
        pl.semaphore_signal(barrier, inc=1, device_id=(me, (tp + k) % n_tp), device_id_type=MESH)

    fulls = ((wsi_ref, wsi), (wpi_ref, wpi), (wso_ref, wso), (wpo_ref, wpo))
    owns = []
    for a, (own, full) in enumerate(fulls):
        count = own.shape[0]
        owns.append(
            pltpu.make_async_copy(
                own, full.at[pl.ds(pl.multiple_of(me * count, count), count)], own_sem.at[a]
            )
        )
    owns.append(pltpu.make_async_copy(tok_ref, tok_full.at[tp], own_sem.at[4]))
    def heads(ref, count):
        return ref.at[pl.ds(pl.multiple_of(tp * count, count), count)]

    loads = [
        pltpu.make_async_copy(heads(ref, groups), there, own_sem.at[5 + k])
        for k, (ref, there) in enumerate(
            (
                (rr_ref, rates.at[0]), (ri_ref, rates.at[1]), (inr_ref, matrices.at[0]),
                (ini_ref, matrices.at[1]), (outr_ref, matrices.at[2]), (outi_ref, matrices.at[3]),
            )
        )
    ]
    loads.append(pltpu.make_async_copy(heads(pw_ref, pool_groups), pool_own, own_sem.at[11]))
    for c in owns + loads:
        c.start()
    pl.semaphore_wait(barrier, n_sp - 1 + n_tp - 1)

    ways = (1, -1)

    def reach_of(a, d):
        return n_sp // 2 if a % 2 == d else n_sp - 1 - n_sp // 2

    def part(a, d, s, h):
        own, full = fulls[a]
        count = own.shape[0]
        size = count // PIECES
        way = ways[d]
        owner = place((at - way * s + n_sp) % n_sp)
        there = full.at[pl.ds(pl.multiple_of(owner * count + h * size, size), size)]
        source = own.at[pl.ds(h * size, size)] if s == 0 else there
        return source, there, (place((at + way + n_sp) % n_sp), tp)

    def sender(a, d, s, h):
        source, there, target = part(a, d, s, h)
        return pltpu.make_async_remote_copy(
            source, there, ring_send.at[a, d, s, h], ring_recv.at[a, d, s, h],
            device_id=target, device_id_type=MESH,
        )

    def arrive(a, d, s, h):
        _, there, target = part(a, d, s + 1, h)
        pltpu.make_async_remote_copy(
            there, there, ring_send.at[a, d, s, h], ring_recv.at[a, d, s, h],
            device_id=target, device_id_type=MESH,
        ).wait_recv()

    longest = n_sp // 2

    def ring(phase, s, h):
        streams = [
            (a, d) for a in (2 * phase, 2 * phase + 1) for d in range(2) if s < reach_of(a, d)
        ]
        for a, d in sorted(streams, key=lambda i: -reach_of(*i)):
            arrive(a, d, s, h)
            if s + 1 < reach_of(a, d):
                sender(a, d, s + 1, h).start()
        if phase == 0 and h == PIECES - 1:
            for a, d in streams:
                if s + 1 == reach_of(a, d):
                    for g in range(PIECES):
                        sender(a + 2, d, 0, g).start()

    turns = [(phase, s, h) for phase in range(2) for s in range(longest) for h in range(PIECES)]
    turn = [0]

    def step(stop=len(turns)):
        if turn[0] < stop:
            ring(*turns[turn[0]])
            turn[0] += 1

    def token_copy(k):
        return pltpu.make_async_remote_copy(
            tok_ref, tok_full.at[tp], tok_send.at[k - 1], tok_recv.at[k - 1],
            device_id=(me, (tp + k) % n_tp), device_id_type=MESH,
        )

    for h in range(PIECES):
        for a, d in ((0, 0), (1, 1), (0, 1), (1, 0)):
            sender(a, d, 0, h).start()
    for k in range(1, n_tp):
        token_copy(k).start()

    tile = iota((states, columns), 0) == iota((states, columns), 1) % states
    tile_exact, tile_half = tile.astype(f32), tile.astype(bf16)

    def exactly(a, b):
        return jnp.dot(a, b, precision=lax.Precision.HIGHEST, preferred_element_type=f32)

    factors = []

    def build_decay():
        for c in loads:
            c.wait()
        own_head = iota((groups, columns), 0) == iota((groups, columns), 1) // states

        def flat(a):
            return jnp.sum(jnp.where(own_head, exactly(a, tile_exact), 0.0), axis=0, keepdims=True)

        rate_real, rate_imag = flat(rates[0]), flat(rates[1])
        all_groups = step_ref.shape[1]
        head = iota((all_groups, columns), 0) == tp * groups + iota((all_groups, columns), 1) // states
        log_step = exactly(jnp.broadcast_to(step_ref[...], (8, all_groups)), head.astype(f32))[0:1]
        step_size = jnp.exp(log_step) / (rows * n_sp)
        exponent, angle = rate_real * step_size, rate_imag * step_size
        magnitude = jnp.exp(exponent)
        cosine = jnp.cos(angle)
        decay_real, decay_imag = magnitude * cosine, magnitude * jnp.sin(angle)
        series = jnp.ones_like(exponent)
        for k in range(10, 1, -1):
            series = 1.0 + series * exponent * (1.0 / k)
        growth = jnp.where(jnp.abs(exponent) < 0.5, exponent * series, magnitude - 1.0)
        less_one = growth * cosine - 2.0 * jnp.square(jnp.sin(0.5 * angle))
        denominator = rate_real * rate_real + rate_imag * rate_imag
        factors.append((less_one * rate_real + decay_imag * rate_imag) / denominator)
        factors.append((decay_imag * rate_real - less_one * rate_imag) / denominator)
        dec_ref[0:1, :] = decay_real
        dec_ref[1:2, :] = decay_imag

    def spread(k):
        high, low = split(matrices[k].reshape(width, states))
        return dot(high, tile_half) + dot(low, tile_half)

    def build_drive(i):
        same = iota((width, columns), 0) // SSM_GROUP == iota((width, columns), 1) // states
        real, imag = spread(0), spread(1)
        if i == 0:
            drive = factors[0] * real - factors[1] * imag
        else:
            drive = factors[0] * imag + factors[1] * real
        for j, piece in enumerate(split(jnp.where(same, drive, 0.0))):
            dmat[i, j] = piece

    def build_read(i):
        across = (iota((columns, states), 0) % states == iota((columns, states), 1)).astype(bf16)
        same = iota((columns, width), 0) // states == iota((columns, width), 1) // SSM_GROUP
        for j, piece in enumerate(split(matrices[2 + i].reshape(width, states))):
            rmat[i, j] = jnp.where(same, dot_nt(across, piece), 0.0).astype(bf16)

    def build_pool():
        across = (
            iota((POOL_GROUP, pool_width), 0) == iota((POOL_GROUP, pool_width), 1) % POOL_GROUP
        ).astype(bf16)
        same = iota((pool_width, pool_width), 0) // POOL_GROUP == iota((pool_width, pool_width), 1) // POOL_GROUP
        own = pool_own[...].reshape(pool_width, POOL_GROUP)
        pmat[...] = jnp.where(same, dot(own, across), 0.0).astype(bf16)

    squares = []

    def take(t):
        block = tok_full[t].astype(f32)
        squares.append(jnp.sum(block * block, axis=1, keepdims=True))
        cut = slice(t * features, (t + 1) * features)
        scaled[:, cut] = (block * gain_ref[:, cut]).astype(bf16)

    def tokens_in():
        owns[4].wait()
        for k in range(1, n_tp):
            pltpu.make_async_remote_copy(
                tok_ref, tok_full.at[(tp - k + n_tp) % n_tp], tok_send.at[k - 1], tok_recv.at[k - 1],
                device_id=(me, (tp + k) % n_tp), device_id_type=MESH,
            ).wait_recv()

    half = len(turns) // 2
    for at_work, work in enumerate(
        (
            build_decay, lambda: build_drive(0), lambda: build_drive(1), lambda: build_read(0),
            lambda: build_read(1), build_pool,
        )
    ):
        work()
        if at_work in (0, 1, 3, 5):
            step(half)
    while turn[0] < half - 3:
        step(half)
    tokens_in()
    for t in range(n_tp):
        take(t)
        if t == n_tp // 2 - 1:
            step(half)
    while turn[0] < half:
        step(half)
    owns[0].wait()
    owns[1].wait()
    inverse = lax.rsqrt(sum(squares) / (features * n_tp) + epsilon)
    state_in = (dot(scaled[...], wsi[...]) * inverse).astype(bf16)
    pool_in = (dot(scaled[...], wpi[...]) * inverse).astype(bf16)
    ext[window_reach:] = pool_in
    halo_out[...] = pool_in[rows - window_reach :]
    halo_copy = pltpu.make_async_remote_copy(
        halo_out, halo, halo_sem.at[0], halo_sem.at[1],
        device_id=((me + 1) % n_sp, tp), device_id_type=MESH,
    )
    shuffle = (
        iota((rows, rows), 1)
        == (iota((rows, rows), 0) % CHUNKS) * span + iota((rows, rows), 0) // CHUNKS
    ).astype(bf16)
    signal = dot(shuffle, state_in).astype(bf16)
    for i in range(2):
        push[i] = dot(signal, dmat[i, 0]) + dot(signal, dmat[i, 1])
        if i == 0:
            halo_copy.start()
        else:
            step()
    decay_real = jnp.broadcast_to(dec_ref[0:1, :], (CHUNKS, columns))
    decay_imag = jnp.broadcast_to(dec_ref[1:2, :], (CHUNKS, columns))

    def advance(p, carry):
        cut = pl.ds(pl.multiple_of(p * CHUNKS, CHUNKS), CHUNKS)
        real, imag = cmul(decay_real, decay_imag, *carry)
        real, imag = real + push[0, cut, :], imag + push[1, cut, :]
        push[0, cut, :] = real
        push[1, cut, :] = imag
        return real, imag

    zero = jnp.zeros((CHUNKS, columns), f32)
    end_real, end_imag = lax.fori_loop(0, span, advance, (zero, zero))

    def power(real, imag, count):
        out = None
        while count:
            if count % 2:
                out = (real, imag) if out is None else cmul(*out, real, imag)
            real, imag = cmul(real, imag, real, imag)
            count //= 2
        return out

    chunk_decay = power(dec_ref[0:1, :], dec_ref[1:2, :], span)
    block_decay = power(*chunk_decay, CHUNKS)
    row_zero = jnp.zeros((1, columns), f32)
    total = (row_zero, row_zero)
    for j in range(CHUNKS):
        moved = cmul(*chunk_decay, *total)
        total = (moved[0] + end_real[j : j + 1], moved[1] + end_imag[j : j + 1])
    which = iota((CHUNKS, columns), 0)
    ends[me] = jnp.where(which == 0, total[0], jnp.where(which == 1, total[1], 0.0))

    def end_copy(k):
        return pltpu.make_async_remote_copy(
            ends.at[me], ends.at[me], end_send.at[k - 1], end_recv.at[k - 1],
            device_id=((me + k) % n_sp, tp), device_id_type=MESH,
        )

    for k in range(1, n_sp):
        end_copy(k).start()

    halo_copy.wait_recv()
    ext[:window_reach] = jnp.where(me == 0, jnp.zeros_like(halo), halo[...])
    group = tp * (pool_width // POOL_GROUP) + iota((rows, pool_width), 1) // POOL_GROUP
    window = jnp.left_shift(jnp.ones_like(group), group % 4 + 1)
    targets = iota((rows, rows + window_reach), 0) + window_reach
    sources = iota((rows, rows + window_reach), 1)
    whole = ext[...]
    sums = jnp.zeros((rows, pool_width), f32)
    for power_index in range(1, 5):
        reach = 2**power_index
        band = ((sources <= targets) & (sources > targets - reach)).astype(bf16)
        sums = jnp.where(window == reach, dot(band, whole), sums)
        if power_index == 2:
            step()
    position = me * rows + iota((rows, pool_width), 0)
    divisor = jnp.minimum(position + 1, window).astype(f32)
    pooled = sums / divisor - ext[window_reach:].astype(f32)
    pooled_high, pooled_low = split(pooled)
    pool_gain = pg_ref[:, pl.ds(pl.multiple_of(tp * pool_width, pool_width), pool_width)]
    projected = dot(pooled_high, pmat[...]) + dot(pooled_low, pmat[...])
    mine_p[...] = (projected * pool_gain).astype(bf16)
    step()

    def act_copy(which, k, source):
        mine = mine_s if which == 0 else mine_p
        return pltpu.make_async_remote_copy(
            mine, act.at[which, source], act_send.at[which, k - 1], act_recv.at[which, k - 1],
            device_id=(me, (tp + k) % n_tp), device_id_type=MESH,
        )

    for k in range(1, n_tp):
        act_copy(1, k, tp).start()
    act[1, tp] = mine_p[...]

    for k in range(1, n_sp):
        there = ends.at[(me - k + n_sp) % n_sp]
        pltpu.make_async_remote_copy(
            there, there, end_send.at[k - 1], end_recv.at[k - 1],
            device_id=((me + k) % n_sp, tp), device_id_type=MESH,
        ).wait_recv()
    total = (row_zero, row_zero)
    for s in range(n_sp - 1):
        moved = cmul(*block_decay, *total)
        use = s < me
        total = (
            jnp.where(use, moved[0] + ends[s, 0:1, :], total[0]),
            jnp.where(use, moved[1] + ends[s, 1:2, :], total[1]),
        )
    begin_real, begin_imag = zero, zero
    for j in range(CHUNKS):
        begin_real = jnp.where(which == j, total[0], begin_real)
        begin_imag = jnp.where(which == j, total[1], begin_imag)
        moved = cmul(*chunk_decay, *total)
        total = (moved[0] + end_real[j : j + 1], moved[1] + end_imag[j : j + 1])

    def add_carry(p, carry):
        cut = pl.ds(pl.multiple_of(p * CHUNKS, CHUNKS), CHUNKS)
        real, imag = cmul(decay_real, decay_imag, *carry)
        push[0, cut, :] = push[0, cut, :] + real
        push[1, cut, :] = push[1, cut, :] + imag
        return real, imag

    lax.fori_loop(0, span, add_carry, (begin_real, begin_imag))
    step()
    real_high, real_low = split(push[0])
    imag_high, imag_low = split(push[1])
    readout = dot(real_high, rmat[0, 0]) + dot(real_high, rmat[0, 1]) + dot(real_low, rmat[0, 0])
    step()
    readout -= dot(imag_high, rmat[1, 0]) + dot(imag_high, rmat[1, 1]) + dot(imag_low, rmat[1, 0])
    skip = skip_ref[:, pl.ds(pl.multiple_of(tp * width, width), width)]
    readout += skip * signal.astype(f32)
    shuffled = jax.nn.gelu(readout).astype(bf16)
    restore = (
        iota((rows, rows), 0)
        == (iota((rows, rows), 1) % CHUNKS) * span + iota((rows, rows), 1) // CHUNKS
    ).astype(bf16)
    mine_s[...] = dot(restore, shuffled).astype(bf16)
    for k in range(1, n_tp):
        act_copy(0, k, tp).start()
    act[0, tp] = mine_s[...]
    while turn[0] < len(turns):
        step()
    for which in (1, 0):
        for k in range(1, n_tp):
            act_copy(which, k, (tp - k + n_tp) % n_tp).wait_recv()
    owns[2].wait()
    owns[3].wait()
    result = None
    for t in range(n_tp):
        for which, full, size in ((1, wpo, pool_width), (0, wso, width)):
            term = dot(act[which, t], full[t * size : (t + 1) * size, :])
            result = term if result is None else result + term
    out_ref[...] = result.astype(bf16)

    for a in range(4):
        for d in range(2):
            for s in range(reach_of(a, d)):
                for h in range(PIECES):
                    sender(a, d, s, h).wait_send()
    for k in range(1, n_tp):
        token_copy(k).wait_send()
        act_copy(0, k, tp).wait_send()
        act_copy(1, k, tp).wait_send()
    halo_copy.wait_send()
    for k in range(1, n_sp):
        end_copy(k).wait_send()

LANES = 128
HALVES = 2


def slab_kernel(
    n_sp, n_tp, n_x, states,
    tok_ref, gain_ref, wsi_ref, wpi_ref, rr_ref, ri_ref, step_ref, inr_ref, ini_ref, outr_ref,
    outi_ref, skip_ref, pw_ref, pg_ref, wso_ref, wpo_ref,
    out_ref,
    tok, scaled, squares, w_in, w_out, dmat, rmat, pmat, push, order, halo, halo_out, ends, act,
    mine_s, mine_p, made, outx, rates, matrices, pool_own, dec_ref,
    own_sem, xw_send, xw_recv, z_send, z_recv, tok_send, tok_recv, act_send, act_recv, halo_sem, end_send, end_recv,
    out_send, out_recv,
):
    me, tp = lax.axis_index("sp"), lax.axis_index("tp")
    n_z = n_sp // n_x
    z, x = me // n_x, me % n_x
    y, core = tp // 2, tp % 2
    rows = tok_ref.shape[0]
    slab = rows * n_x
    features = tok_ref.shape[1]
    in_rows = wsi_ref.shape[0]
    out_rows = wso_ref.shape[0]
    width = wsi_ref.shape[1] // n_x
    out_width = wso_ref.shape[1] // n_x
    chunk_count = out_width // LANES
    groups = width // SSM_GROUP
    columns = groups * states
    pool_groups = width // POOL_GROUP
    span = slab // CHUNKS
    q = tp * n_x + x

    across, pair, both = (1 - y) * 2 + core, y * 2 + 1 - core, (1 - y) * 2 + 1 - core
    beside = me + 1 - 2 * x
    to_x, to_y, to_pair = (beside, tp), (me, across), (me, pair)
    ways = (1, -1)

    def to_z(way):
        return (me + way * n_x, tp)

    def inside(at):
        return jnp.logical_and(at >= 0, at < n_z)

    def aligned(index, size):
        return pl.ds(pl.multiple_of(index * size, size), size)

    barrier = pltpu.get_barrier_semaphore()
    for there in (to_x, to_y, to_pair):
        pl.semaphore_signal(barrier, inc=1, device_id=there, device_id_type=MESH)
    for way in ways:
        @pl.when(inside(z + way))
        def _():
            pl.semaphore_signal(barrier, inc=1, device_id=to_z(way), device_id_type=MESH)

    def remote(source, there, send, recv, target):
        return pltpu.make_async_remote_copy(
            source, there, send, recv, device_id=target, device_id_type=MESH
        )

    def in_part(ref, half):
        return ref.at[:, aligned(half, width)]

    def out_part(ref, half, j):
        return ref.at[:, pl.ds(pl.multiple_of(half * out_width + j * LANES, LANES), LANES)]

    own_in, own_out = (wsi_ref, wpi_ref), (wso_ref, wpo_ref)

    def in_at(m, sp):
        return w_in.at[m, aligned(sp, in_rows)]

    def out_at(j, m, sp):
        return w_out.at[j, m, aligned(sp, out_rows)]

    own_copies = [pltpu.make_async_copy(in_part(own_in[m], x), in_at(m, me), own_sem.at[m]) for m in range(2)]
    for j in range(chunk_count):
        for m in range(2):
            own_copies.append(
                pltpu.make_async_copy(out_part(own_out[m], x, j), out_at(j, m, me), own_sem.at[2 + 2 * j + m])
            )
    base = 2 + 2 * chunk_count
    tok_copy = pltpu.make_async_copy(tok_ref, tok.at[tp, aligned(x, rows)], own_sem.at[base])

    def heads(ref, count):
        return ref.at[aligned(q, count)]

    loads = [
        pltpu.make_async_copy(heads(ref, groups), there, own_sem.at[base + 1 + k])
        for k, (ref, there) in enumerate(
            (
                (rr_ref, rates.at[0]), (ri_ref, rates.at[1]), (inr_ref, matrices.at[0]),
                (ini_ref, matrices.at[1]), (outr_ref, matrices.at[2]), (outi_ref, matrices.at[3]),
            )
        )
    ]
    loads.append(pltpu.make_async_copy(heads(pw_ref, pool_groups), pool_own, own_sem.at[base + 7]))
    for c in loads + [tok_copy] + own_copies:
        c.start()

    def x_weights(k, sp):
        if k < 2:
            return in_part(own_in[k], 1 - x), in_at(k, sp)
        j, m = (k - 2) // 2, k % 2
        return out_part(own_out[m], 1 - x, j), out_at(j, m, sp)

    def x_send(k):
        return remote(*x_weights(k, me), xw_send.at[k], xw_recv.at[k], to_x)

    @jax.named_scope("across_wait")
    def x_wait(k):
        here = x_weights(k, beside)[1]
        remote(here, here, xw_send.at[k], xw_recv.at[k], to_x).wait_recv()

    x_kinds = 2 + 2 * chunk_count
    stage_count = 2 + chunk_count

    def z_part(stage, h, at):
        if stage < 2:
            return in_at(stage, at * n_x + (x if h == 0 else 1 - x))
        return w_out.at[stage - 2, h, aligned(at, out_rows * n_x)]

    def z_copy(d, stage, s, h):
        there = z_part(stage, h, z - ways[d] * s)
        source = in_part(own_in[stage], x) if s == 0 and stage < 2 and h == 0 else there
        return remote(source, there, z_send.at[d, stage, s, h], z_recv.at[d, stage, s, h], to_z(ways[d]))

    def z_own(stage, h):
        for d in range(2):
            @pl.when(inside(z + ways[d]))
            def _():
                z_copy(d, stage, 0, h).start()

    def middle():
        return jnp.logical_and(inside(z + 1), inside(z - 1))

    def z_arrive(d, stage, s, h):
        here = z_part(stage, h, z - ways[d] * (s + 1))
        remote(here, here, z_send.at[d, stage, s, h], z_recv.at[d, stage, s, h], to_z(ways[d])).wait_recv()

    @jax.named_scope("relay_wait")
    def z_relay(stage, s, h):
        for d in range(2):
            @pl.when(jnp.logical_and(inside(z - ways[d] * (s + 1)), inside(z + ways[d])))
            def _():
                z_arrive(d, stage, s, h)
                z_copy(d, stage, s + 1, h).start()

    @jax.named_scope("final_wait")
    def z_final(stage):
        for d in range(2):
            for s in range(n_z - 1):
                @pl.when(jnp.logical_and(inside(z - ways[d] * (s + 1)), jnp.logical_not(inside(z + ways[d]))))
                def _():
                    for h in range(2):
                        z_arrive(d, stage, s, h)

    def out_own(j):
        for m in range(2):
            x_wait(2 + 2 * j + m)
            own_copies[2 + 2 * j + m].wait()
            z_own(2 + j, m)

    relays = [(m, 0, h) for h in range(2) for m in range(2)]
    relays += [(m, s, h) for m in range(2) for s in range(1, n_z - 2) for h in range(2)]
    in_relays = len(relays)
    for j in range(chunk_count):
        relays += [(2 + j, s, m) for s in range(n_z - 2) for m in range(2)]
    turn = [0]

    def progress(count=1, stop=None):
        while count and turn[0] < (len(relays) if stop is None else stop):
            z_relay(*relays[turn[0]])
            turn[0] += 1
            count -= 1

    class Gather:
        def __init__(self, own, region, send, recv):
            self.own, self.region, self.send, self.recv = own, region, send, recv

        def copy(self, slot, p):
            region = self.region
            source, there, target = {
                0: (self.own(p), region(tp, x, p), to_x),
                1: (self.own(p), region(tp, x, p), to_y),
                2: (None, region(tp, 1 - x, p), to_y),
                3: (self.own(p), region(tp, x, p), to_pair),
                4: (None, region(tp, 1 - x, p), to_pair),
                5: (None, region(across, x, p), to_pair),
                6: (None, region(across, 1 - x, p), to_pair),
            }[slot]
            source = there if source is None else source
            return remote(source, there, self.send.at[slot, p], self.recv.at[slot, p], target)

        def start(self, *slots, p):
            for slot in slots:
                self.copy(slot, p).start()

        @jax.named_scope("gather_wait")
        def wait(self, slot, p):
            at_tp, at_x = (
                (tp, 1 - x), (across, x), (across, 1 - x), (pair, x), (pair, 1 - x), (both, x), (both, 1 - x)
            )[slot]
            here = self.region(at_tp, at_x, p)
            remote(here, here, self.send.at[slot, p], self.recv.at[slot, p], to_pair).wait_recv()

        def relay_x(self, p):
            self.wait(0, p)
            self.start(2, 4, p=p)

        def relay_y(self, p):
            self.wait(1, p)
            self.start(5, p=p)

        def relay_both(self, p):
            self.wait(2, p)
            self.start(6, p=p)

        def drain(self):
            for slot in range(7):
                for p in range(HALVES):
                    self.copy(slot, p).wait_send()

    piece = rows // HALVES

    def tok_region(at_tp, at_x, p):
        return tok.at[at_tp, pl.ds(pl.multiple_of(at_x * rows + p * piece, piece), piece)]

    tokens = Gather(lambda p: tok_ref.at[pl.ds(p * piece, piece)], tok_region, tok_send, tok_recv)

    def act_gather(which, mine):
        size = slab // HALVES

        def region(at_tp, at_x, p):
            return act.at[which, pl.ds(p * size, size), aligned(at_tp * n_x + at_x, width)]

        return Gather(lambda p: mine.at[pl.ds(p * size, size)], region, act_send.at[which], act_recv.at[which])

    acts = (act_gather(0, mine_s), act_gather(1, mine_p))

    pl.semaphore_wait(barrier, 3 + inside(z + 1).astype(jnp.int32) + inside(z - 1).astype(jnp.int32))

    x_send(0).start()
    z_own(0, 0)
    z_own(1, 0)
    x_send(1).start()
    for p in range(HALVES):
        tokens.start(0, 1, 3, p=p)
    for k in range(2, x_kinds):
        x_send(k).start()

    tile = iota((states, columns), 0) == iota((states, columns), 1) % states
    tile_exact, tile_half = tile.astype(f32), tile.astype(bf16)

    def exactly(a, b):
        return jnp.dot(a, b, precision=lax.Precision.HIGHEST, preferred_element_type=f32)

    factors = []

    @jax.named_scope("build_decay")
    def build_decay():
        for c in loads:
            c.wait()
        own_head = iota((groups, columns), 0) == iota((groups, columns), 1) // states

        def flat(a):
            return jnp.sum(jnp.where(own_head, exactly(a, tile_exact), 0.0), axis=0, keepdims=True)

        rate_real, rate_imag = flat(rates[0]), flat(rates[1])
        all_groups = step_ref.shape[1]
        head = iota((all_groups, columns), 0) == q * groups + iota((all_groups, columns), 1) // states
        log_step = exactly(jnp.broadcast_to(step_ref[...], (8, all_groups)), head.astype(f32))[0:1]
        step_size = jnp.exp(log_step) / (rows * n_sp)
        exponent, angle = rate_real * step_size, rate_imag * step_size
        magnitude = jnp.exp(exponent)
        cosine = jnp.cos(angle)
        decay_real, decay_imag = magnitude * cosine, magnitude * jnp.sin(angle)
        series = jnp.ones_like(exponent)
        for k in range(10, 1, -1):
            series = 1.0 + series * exponent * (1.0 / k)
        growth = jnp.where(jnp.abs(exponent) < 0.5, exponent * series, magnitude - 1.0)
        less_one = growth * cosine - 2.0 * jnp.square(jnp.sin(0.5 * angle))
        denominator = rate_real * rate_real + rate_imag * rate_imag
        factors.append((less_one * rate_real + decay_imag * rate_imag) / denominator)
        factors.append((decay_imag * rate_real - less_one * rate_imag) / denominator)
        dec_ref[0:1, :] = decay_real
        dec_ref[1:2, :] = decay_imag

    def spread(k):
        high, low = split(matrices[k].reshape(width, states))
        return dot(high, tile_half) + dot(low, tile_half)

    @jax.named_scope("build_drive")
    def build_drive(i):
        same = iota((width, columns), 0) // SSM_GROUP == iota((width, columns), 1) // states
        real, imag = spread(0), spread(1)
        if i == 0:
            drive = factors[0] * real - factors[1] * imag
        else:
            drive = factors[0] * imag + factors[1] * real
        for j, part in enumerate(split(jnp.where(same, drive, 0.0))):
            dmat[i, j] = part

    @jax.named_scope("build_read")
    def build_read(i):
        onto = (iota((columns, states), 0) % states == iota((columns, states), 1)).astype(bf16)
        same = iota((columns, width), 0) // states == iota((columns, width), 1) // SSM_GROUP
        for j, part in enumerate(split(matrices[2 + i].reshape(width, states))):
            rmat[i, j] = jnp.where(same, dot_nt(onto, part), 0.0).astype(bf16)

    @jax.named_scope("build_pool")
    def build_pool():
        onto = (iota((POOL_GROUP, width), 0) == iota((POOL_GROUP, width), 1) % POOL_GROUP).astype(bf16)
        same = iota((width, width), 0) // POOL_GROUP == iota((width, width), 1) // POOL_GROUP
        own = pool_own[...].reshape(width, POOL_GROUP)
        pmat[...] = jnp.where(same, dot(own, onto), 0.0).astype(bf16)

    @jax.named_scope("build_order")
    def build_order(i):
        a, b = iota((slab, slab), i), iota((slab, slab), 1 - i)
        order[i] = (b == (a % CHUNKS) * span + a // CHUNKS).astype(bf16)

    @jax.named_scope("take")
    def take(at_tp, first):
        cut = pl.ds(pl.multiple_of(at_tp * features, features), features)
        gain = gain_ref[:, cut]
        size = min(64, slab)

        def step(i, _):
            here = pl.ds(pl.multiple_of(i * size, size), size)
            block = tok[at_tp, here].astype(f32)
            total = jnp.broadcast_to(jnp.sum(block * block, axis=1, keepdims=True), (size, LANES))
            squares[here] = total if first else squares[here] + total
            scaled[here, cut] = (block * gain).astype(bf16)
            return 0

        lax.fori_loop(0, slab // size, step, 0)

    build_decay()
    build_drive(0)
    progress()
    x_wait(0)
    z_own(0, 1)
    progress()
    x_wait(1)
    z_own(1, 1)
    build_drive(1)
    build_read(0)
    progress()
    build_read(1)
    progress()
    tokens.relay_x(0)
    build_order(0)
    progress()
    build_pool()
    tokens.relay_y(0)
    tokens.relay_x(1)
    progress()
    tok_copy.wait()
    build_order(1)
    progress(stop=in_relays)
    tokens.relay_y(1)
    for p in range(HALVES):
        tokens.wait(3, p)
        tokens.wait(4, p)
    take(tp, True)
    progress(stop=in_relays)
    take(pair, False)
    tokens.relay_both(0)
    progress(stop=in_relays)
    tokens.relay_both(1)
    take(across, False)
    for p in range(HALVES):
        tokens.wait(5, p)
        tokens.wait(6, p)
    take(both, False)
    progress(in_relays, stop=in_relays)
    inverse = lax.rsqrt(squares[...] / (features * n_tp) + epsilon)
    own_copies[0].wait()
    z_final(0)
    state_in = (dot(scaled[...], w_in[0]) * inverse).astype(bf16)
    out_own(0)
    signal = dot(order[0], state_in).astype(bf16)
    for i in range(2):
        push[i] = dot(signal, dmat[i, 0]) + dot(signal, dmat[i, 1])
    decay_real = jnp.broadcast_to(dec_ref[0:1, :], (CHUNKS, columns))
    decay_imag = jnp.broadcast_to(dec_ref[1:2, :], (CHUNKS, columns))

    def advance(p, carry):
        cut = pl.ds(pl.multiple_of(p * CHUNKS, CHUNKS), CHUNKS)
        real, imag = cmul(decay_real, decay_imag, *carry)
        real, imag = real + push[0, cut, :], imag + push[1, cut, :]
        push[0, cut, :] = real
        push[1, cut, :] = imag
        return real, imag

    zero = jnp.zeros((CHUNKS, columns), f32)
    end_real, end_imag = lax.fori_loop(0, span, advance, (zero, zero), unroll=4)

    def power(real, imag, count):
        out = None
        while count:
            if count % 2:
                out = (real, imag) if out is None else cmul(*out, real, imag)
            real, imag = cmul(real, imag, real, imag)
            count //= 2
        return out

    chunk_decay = power(dec_ref[0:1, :], dec_ref[1:2, :], span)
    block_decay = power(*chunk_decay, CHUNKS)
    row_zero = jnp.zeros((1, columns), f32)
    total = (row_zero, row_zero)
    for j in range(CHUNKS):
        moved = cmul(*chunk_decay, *total)
        total = (moved[0] + end_real[j : j + 1], moved[1] + end_imag[j : j + 1])
    which = iota((CHUNKS, columns), 0)
    ends[z] = jnp.where(which == 0, total[0], jnp.where(which == 1, total[1], 0.0))

    def end_copy(k):
        return remote(ends.at[z], ends.at[z], end_send.at[k - 1], end_recv.at[k - 1], (me + k * n_x, tp))

    for k in range(1, n_z):
        @pl.when(inside(z + k))
        def _():
            end_copy(k).start()

    out_own(1)
    progress()
    z_final(1)
    own_copies[1].wait()
    pool_in = (dot(scaled[...], w_in[1]) * inverse).astype(bf16)
    halo_out[...] = pool_in[slab - window_reach :]
    halo_copy = remote(halo_out, halo, halo_sem.at[0], halo_sem.at[1], to_z(1))

    @pl.when(inside(z + 1))
    def _():
        halo_copy.start()

    progress()
    for k in range(1, n_z):
        @pl.when(inside(z - k))
        @jax.named_scope("ends_wait")
        def _():
            there = ends.at[z - k]
            remote(there, there, end_send.at[k - 1], end_recv.at[k - 1], to_z(1)).wait_recv()

    total = (row_zero, row_zero)
    for s in range(n_z - 1):
        moved = cmul(*block_decay, *total)
        use = s < z
        total = (
            jnp.where(use, moved[0] + ends[s, 0:1, :], total[0]),
            jnp.where(use, moved[1] + ends[s, 1:2, :], total[1]),
        )
    begin_real, begin_imag = zero, zero
    for j in range(CHUNKS):
        begin_real = jnp.where(which == j, total[0], begin_real)
        begin_imag = jnp.where(which == j, total[1], begin_imag)
        moved = cmul(*chunk_decay, *total)
        total = (moved[0] + end_real[j : j + 1], moved[1] + end_imag[j : j + 1])

    def add_carry(p, carry):
        cut = pl.ds(pl.multiple_of(p * CHUNKS, CHUNKS), CHUNKS)
        real, imag = cmul(decay_real, decay_imag, *carry)
        push[0, cut, :] = push[0, cut, :] + real
        push[1, cut, :] = push[1, cut, :] + imag
        return real, imag

    lax.fori_loop(0, span, add_carry, (begin_real, begin_imag), unroll=4)
    progress()
    real_high, real_low = split(push[0])
    imag_high, imag_low = split(push[1])
    readout = dot(real_high, rmat[0, 0]) + dot(real_high, rmat[0, 1]) + dot(real_low, rmat[0, 0])
    readout -= dot(imag_high, rmat[1, 0]) + dot(imag_high, rmat[1, 1]) + dot(imag_low, rmat[1, 0])
    skip = skip_ref[:, aligned(q, width)]
    readout += skip * signal.astype(f32)
    shuffled = jax.nn.gelu(readout).astype(bf16)
    mine_s[...] = dot(order[1], shuffled).astype(bf16)
    for p in range(HALVES):
        acts[0].start(0, 1, 3, p=p)
    act[0, :, aligned(q, width)] = mine_s[...]
    out_own(2) if chunk_count > 2 else None
    progress()

    @pl.when(z > 0)
    @jax.named_scope("halo_wait")
    def _():
        halo_copy.wait_recv()

    before = jnp.where(z == 0, jnp.zeros_like(halo), halo[...])
    whole = jnp.concatenate([before, pool_in], axis=0).astype(f32)
    window = jnp.left_shift(2, (q * pool_groups + iota((slab, width), 1) // POOL_GROUP) % 4)
    sums = jnp.zeros((slab, width), f32)
    running = whole
    for level in range(4):
        running = running + pltpu.roll(running, 2**level, 0)
        sums = jnp.where(window == 2 ** (level + 1), running[window_reach:], sums)
    position = z * slab + iota((slab, width), 0)
    divisor = jnp.minimum(position + 1, window).astype(f32)
    pooled = sums / divisor - whole[window_reach:]
    pooled_high, pooled_low = split(pooled)
    pool_gain = pg_ref[:, aligned(q, width)]
    projected = dot(pooled_high, pmat[...]) + dot(pooled_low, pmat[...])
    mine_p[...] = (projected * pool_gain).astype(bf16)
    for p in range(HALVES):
        acts[1].start(0, 1, 3, p=p)
    act[1, :, aligned(q, width)] = mine_p[...]
    for k in range(2):
        for p in range(HALVES):
            acts[k].relay_x(p)
            progress()
            acts[k].relay_y(p)
        progress()
    for k in range(2):
        for p in range(HALVES):
            acts[k].relay_both(p)
            progress()
    progress(len(relays))
    for k in range(2):
        for slot in (3, 4, 5, 6):
            for p in range(HALVES):
                acts[k].wait(slot, p)

    def out_copy(j):
        return remote(made.at[j, aligned(1 - x, rows)], outx.at[j], out_send.at[j], out_recv.at[j], to_x)

    def out_columns(half, j):
        return pl.ds(pl.multiple_of(half * out_width + j * LANES, LANES), LANES)

    def keep(j):
        return pltpu.make_async_copy(made.at[j, aligned(x, rows)], out_ref.at[:, out_columns(x, j)], own_sem.at[base + 8 + j])

    def fetch(j):
        return pltpu.make_async_copy(outx.at[j], out_ref.at[:, out_columns(1 - x, j)], own_sem.at[base + 8 + chunk_count + j])

    def make(j, half):
        cut = aligned(half, rows)
        made[j, cut] = (dot(act[0, cut], w_out[j, 0]) + dot(act[1, cut], w_out[j, 1])).astype(bf16)

    for j in range(chunk_count):
        z_final(2 + j)
        make(j, 1 - x)
        out_copy(j).start()
        make(j, x)
        keep(j).start()

    for k in range(x_kinds):
        x_send(k).wait_send()
    for d in range(2):
        for stage in range(stage_count):
            for s in range(n_z - 1):
                @pl.when(jnp.logical_and(inside(z + ways[d]), inside(z - ways[d] * s)))
                def _():
                    for h in range(2):
                        z_copy(d, stage, s, h).wait_send()
    tokens.drain()
    acts[0].drain()
    acts[1].drain()

    @pl.when(inside(z + 1))
    def _():
        halo_copy.wait_send()

    for k in range(1, n_z):
        @pl.when(inside(z + k))
        def _():
            end_copy(k).wait_send()
    for j in range(chunk_count):
        out_copy(j).wait_recv()
        fetch(j).start()
    for j in range(chunk_count):
        out_copy(j).wait_send()
        keep(j).wait()
        fetch(j).wait()


def slab_call(n_sp, n_tp, n_x, arrays):
    tokens, state_in_weight, state_out_weight = arrays[0], arrays[2], arrays[14]
    rows, features = tokens.shape
    in_rows, width = state_in_weight.shape
    out_rows, out_columns = state_out_weight.shape
    width //= n_x
    n_z, slab, chunk_count = n_sp // n_x, rows * n_x, out_columns // n_x // LANES
    groups, states = width // SSM_GROUP, arrays[4].shape[1]
    columns, pool_groups = groups * states, width // POOL_GROUP
    vmem = pl.BlockSpec(memory_space=pltpu.VMEM)
    anywhere = pl.BlockSpec(memory_space=pl.ANY)
    dma = pltpu.SemaphoreType.DMA
    return pl.pallas_call(
        functools.partial(slab_kernel, n_sp, n_tp, n_x, states),
        out_shape=jax.ShapeDtypeStruct((rows, out_columns), bf16),
        in_specs=[anywhere, vmem] + [anywhere] * 4 + [vmem] + [anywhere] * 4 + [vmem, anywhere, vmem]
        + [anywhere] * 2,
        out_specs=anywhere,
        scratch_shapes=[
            pltpu.VMEM((n_tp, slab, features), bf16),
            pltpu.VMEM((slab, features * n_tp), bf16),
            pltpu.VMEM((slab, LANES), f32),
            pltpu.VMEM((2, n_sp * in_rows, width), bf16),
            pltpu.VMEM((chunk_count, 2, n_sp * out_rows, LANES), bf16),
            pltpu.VMEM((2, 2, width, columns), bf16),
            pltpu.VMEM((2, 2, columns, width), bf16),
            pltpu.VMEM((width, width), bf16),
            pltpu.VMEM((2, slab, columns), f32),
            pltpu.VMEM((2, slab, slab), bf16),
            pltpu.VMEM((window_reach, width), bf16),
            pltpu.VMEM((window_reach, width), bf16),
            pltpu.VMEM((n_z, CHUNKS, columns), f32),
            pltpu.VMEM((2, slab, n_tp * n_x * width), bf16),
            pltpu.VMEM((slab, width), bf16),
            pltpu.VMEM((slab, width), bf16),
            pltpu.VMEM((chunk_count, slab, LANES), bf16),
            pltpu.VMEM((chunk_count, rows, LANES), bf16),
            pltpu.VMEM((2, groups, states), f32),
            pltpu.VMEM((4, groups, SSM_GROUP, states), f32),
            pltpu.VMEM((pool_groups, POOL_GROUP, POOL_GROUP), bf16),
            pltpu.VMEM((2, columns), f32),
            dma((10 + 4 * chunk_count,)),
            dma((2 + 2 * chunk_count,)),
            dma((2 + 2 * chunk_count,)),
            dma((2, 2 + chunk_count, n_z - 1, 2)),
            dma((2, 2 + chunk_count, n_z - 1, 2)),
            dma((7, HALVES)),
            dma((7, HALVES)),
            dma((2, 7, HALVES)),
            dma((2, 7, HALVES)),
            dma((2,)),
            dma((n_z - 1,)),
            dma((n_z - 1,)),
            dma((chunk_count,)),
            dma((chunk_count,)),
        ],
        compiler_params=pltpu.CompilerParams(
            collective_id=0, has_side_effects=True, vmem_limit_bytes=60 * 2**20
        ),
    )(*arrays)


def slab_fits(n_sp, n_tp, n_x, width, pool_width, out_columns):
    return (
        n_x == 2 and n_tp == 4 and n_sp // n_x >= 3 and width == n_x * LANES
        and pool_width == width and out_columns % (n_x * LANES) == 0
    )


def body(
    n_sp, n_tp, n_x,
    tokens, norm_gain, state_in_weight, pool_in_weight, rate_real, rate_imag, log_step,
    input_real, input_imag, output_real, output_imag, skip_gain, pool_weight, pool_gain,
    state_out_weight, pool_out_weight,
):
    rows, features = tokens.shape
    in_rows, width = state_in_weight.shape
    pool_width = pool_in_weight.shape[1]
    out_rows, out_columns = state_out_weight.shape
    groups = width // SSM_GROUP
    states = rate_real.shape[1]
    columns = groups * states
    pool_groups = pool_width // POOL_GROUP
    if slab_fits(n_sp, n_tp, n_x, width, pool_width, out_columns):
        return slab_call(n_sp, n_tp, n_x, (
            tokens, norm_gain[None], state_in_weight, pool_in_weight, rate_real, rate_imag, log_step[None],
            jnp.swapaxes(input_real, 1, 2), jnp.swapaxes(input_imag, 1, 2), output_real, output_imag,
            skip_gain[None], pool_weight, pool_gain[None], state_out_weight, pool_out_weight,
        ))
    vmem = pl.BlockSpec(memory_space=pltpu.VMEM)
    anywhere = pl.BlockSpec(memory_space=pl.ANY)
    dma = pltpu.SemaphoreType.DMA
    return pl.pallas_call(
        functools.partial(kernel, n_sp, n_tp, n_x, states),
        out_shape=jax.ShapeDtypeStruct((rows, out_columns), bf16),
        in_specs=[anywhere, vmem] + [anywhere] * 4 + [vmem] + [anywhere] * 4 + [vmem, anywhere, vmem]
        + [anywhere] * 2,
        out_specs=vmem,
        scratch_shapes=[
            pltpu.VMEM((n_tp, rows, features), bf16),
            pltpu.VMEM((n_sp * in_rows, width), bf16),
            pltpu.VMEM((n_sp * in_rows, pool_width), bf16),
            pltpu.VMEM((n_sp * out_rows, out_columns), bf16),
            pltpu.VMEM((n_sp * out_rows, out_columns), bf16),
            pltpu.VMEM((rows, features * n_tp), bf16),
            pltpu.VMEM((2, 2, width, columns), bf16),
            pltpu.VMEM((2, 2, columns, width), bf16),
            pltpu.VMEM((pool_width, pool_width), bf16),
            pltpu.VMEM((2, rows, columns), f32),
            pltpu.VMEM((rows + window_reach, pool_width), bf16),
            pltpu.VMEM((window_reach, pool_width), bf16),
            pltpu.VMEM((n_sp, CHUNKS, columns), f32),
            pltpu.VMEM((2, n_tp, rows, width), bf16),
            pltpu.VMEM((rows, width), bf16),
            pltpu.VMEM((rows, pool_width), bf16),
            pltpu.VMEM((window_reach, pool_width), bf16),
            pltpu.VMEM((2, groups, states), f32),
            pltpu.VMEM((4, groups, SSM_GROUP, states), f32),
            pltpu.VMEM((pool_groups, POOL_GROUP, POOL_GROUP), bf16),
            pltpu.VMEM((2, columns), f32),
            dma((12,)),
            dma((4, 2, n_sp // 2, PIECES)),
            dma((4, 2, n_sp // 2, PIECES)),
            dma((n_tp - 1,)),
            dma((n_tp - 1,)),
            dma((2, n_tp - 1)),
            dma((2, n_tp - 1)),
            dma((2,)),
            dma((n_sp - 1,)),
            dma((n_sp - 1,)),
        ],
        compiler_params=pltpu.CompilerParams(
            collective_id=0, has_side_effects=True, vmem_limit_bytes=60 * 2**20
        ),
    )(
        tokens, norm_gain[None], state_in_weight, pool_in_weight, rate_real, rate_imag, log_step[None],
        jnp.swapaxes(input_real, 1, 2), jnp.swapaxes(input_imag, 1, 2), output_real, output_imag,
        skip_gain[None], pool_weight, pool_gain[None], state_out_weight, pool_out_weight,
    )


def solution(mesh):
    n_sp, n_tp = mesh.shape["sp"], mesh.shape["tp"]
    n_x = 2 ** ((n_sp.bit_length() - 1) // 2)
    both, whole = P("sp", "tp"), P()
    return jax.shard_map(
        functools.partial(body, n_sp, n_tp, n_x),
        mesh=mesh,
        in_specs=(both, whole, both, both) + (whole,) * 10 + (both, both),
        out_specs=both,
        check_vma=False,
    )
```

```python
import functools

import jax
import jax.numpy as jnp
from jax import lax
from jax.experimental import pallas as pl
from jax.experimental.pallas import tpu as pltpu
from jax.sharding import PartitionSpec as P

SSM_GROUP = 16
POOL_GROUP = 64
CHUNKS = 8
PIECES = 2

epsilon = 1e-06
window_reach = 16
f32, bf16 = jnp.float32, jnp.bfloat16
MESH = pl.DeviceIdType.MESH


def discretize(rate_real, rate_imag, log_step, length):
    step_size = jnp.exp(log_step)[:, None] / length
    exponent = rate_real * step_size
    angle = rate_imag * step_size
    magnitude = jnp.exp(exponent)
    decay_real = magnitude * jnp.cos(angle)
    decay_imag = magnitude * jnp.sin(angle)
    less_one = jnp.expm1(exponent) * jnp.cos(angle) - 2.0 * jnp.square(jnp.sin(0.5 * angle))
    denominator = rate_real * rate_real + rate_imag * rate_imag
    factor_real = (less_one * rate_real + decay_imag * rate_imag) / denominator
    factor_imag = (decay_imag * rate_real - less_one * rate_imag) / denominator
    return decay_real, decay_imag, factor_real, factor_imag


def iota(shape, axis):
    return lax.broadcasted_iota(jnp.int32, shape, axis)


def dot(a, b):
    return jnp.dot(a, b, preferred_element_type=f32)


def dot_nt(a, b):
    return lax.dot_general(a, b, (((1,), (1,)), ((), ())), preferred_element_type=f32)


def split(a):
    high = a.astype(bf16)
    return high, (a - high.astype(f32)).astype(bf16)


def cmul(ar, ai, br, bi):
    return ar * br - ai * bi, ar * bi + ai * br


def kernel(
    n_sp, n_tp, n_x, states,
    tok_ref, gain_ref, wsi_ref, wpi_ref, rr_ref, ri_ref, step_ref, inr_ref, ini_ref, outr_ref,
    outi_ref, skip_ref, pw_ref, pg_ref, wso_ref, wpo_ref,
    out_ref,
    tok_full, wsi, wpi, wso, wpo, scaled, dmat, rmat, pmat, push, ext, halo, ends, act,
    mine_s, mine_p, halo_out, rates, matrices, pool_own, dec_ref,
    own_sem, ring_send, ring_recv, tok_send, tok_recv, act_send, act_recv, halo_sem, end_send, end_recv,
):
    me, tp = lax.axis_index("sp"), lax.axis_index("tp")
    n_z = n_sp // n_x
    rows = tok_ref.shape[0]
    features = tok_ref.shape[1]
    width = wsi_ref.shape[1]
    pool_width = wpi_ref.shape[1]
    groups = width // SSM_GROUP
    columns = groups * states
    pool_groups = pool_width // POOL_GROUP
    span = rows // CHUNKS

    def place(p):
        x, r = p // n_z, p % n_z
        return (r + (x % 2) * (n_z - 1 - 2 * r)) * n_x + x

    my_x, my_z = me % n_x, me // n_x
    at = my_x * n_z + my_z + (my_x % 2) * (n_z - 1 - 2 * my_z)

    barrier = pltpu.get_barrier_semaphore()
    for k in range(1, n_sp):
        pl.semaphore_signal(barrier, inc=1, device_id=((me + k) % n_sp, tp), device_id_type=MESH)
    for k in range(1, n_tp):
        pl.semaphore_signal(barrier, inc=1, device_id=(me, (tp + k) % n_tp), device_id_type=MESH)

    fulls = ((wsi_ref, wsi), (wpi_ref, wpi), (wso_ref, wso), (wpo_ref, wpo))
    owns = []
    for a, (own, full) in enumerate(fulls):
        count = own.shape[0]
        owns.append(
            pltpu.make_async_copy(
                own, full.at[pl.ds(pl.multiple_of(me * count, count), count)], own_sem.at[a]
            )
        )
    owns.append(pltpu.make_async_copy(tok_ref, tok_full.at[tp], own_sem.at[4]))
    def heads(ref, count):
        return ref.at[pl.ds(pl.multiple_of(tp * count, count), count)]

    loads = [
        pltpu.make_async_copy(heads(ref, groups), there, own_sem.at[5 + k])
        for k, (ref, there) in enumerate(
            (
                (rr_ref, rates.at[0]), (ri_ref, rates.at[1]), (inr_ref, matrices.at[0]),
                (ini_ref, matrices.at[1]), (outr_ref, matrices.at[2]), (outi_ref, matrices.at[3]),
            )
        )
    ]
    loads.append(pltpu.make_async_copy(heads(pw_ref, pool_groups), pool_own, own_sem.at[11]))
    for c in owns + loads:
        c.start()
    pl.semaphore_wait(barrier, n_sp - 1 + n_tp - 1)

    ways = (1, -1)

    def reach_of(a, d):
        return n_sp // 2 if a % 2 == d else n_sp - 1 - n_sp // 2

    def part(a, d, s, h):
        own, full = fulls[a]
        count = own.shape[0]
        size = count // PIECES
        way = ways[d]
        owner = place((at - way * s + n_sp) % n_sp)
        there = full.at[pl.ds(pl.multiple_of(owner * count + h * size, size), size)]
        source = own.at[pl.ds(h * size, size)] if s == 0 else there
        return source, there, (place((at + way + n_sp) % n_sp), tp)

    def sender(a, d, s, h):
        source, there, target = part(a, d, s, h)
        return pltpu.make_async_remote_copy(
            source, there, ring_send.at[a, d, s, h], ring_recv.at[a, d, s, h],
            device_id=target, device_id_type=MESH,
        )

    def arrive(a, d, s, h):
        _, there, target = part(a, d, s + 1, h)
        pltpu.make_async_remote_copy(
            there, there, ring_send.at[a, d, s, h], ring_recv.at[a, d, s, h],
            device_id=target, device_id_type=MESH,
        ).wait_recv()

    longest = n_sp // 2

    def ring(phase, s, h):
        streams = [
            (a, d) for a in (2 * phase, 2 * phase + 1) for d in range(2) if s < reach_of(a, d)
        ]
        for a, d in sorted(streams, key=lambda i: -reach_of(*i)):
            arrive(a, d, s, h)
            if s + 1 < reach_of(a, d):
                sender(a, d, s + 1, h).start()
        if phase == 0 and h == PIECES - 1:
            for a, d in streams:
                if s + 1 == reach_of(a, d):
                    for g in range(PIECES):
                        sender(a + 2, d, 0, g).start()

    turns = [(phase, s, h) for phase in range(2) for s in range(longest) for h in range(PIECES)]
    turn = [0]

    def step(stop=len(turns)):
        if turn[0] < stop:
            ring(*turns[turn[0]])
            turn[0] += 1

    def token_copy(k):
        return pltpu.make_async_remote_copy(
            tok_ref, tok_full.at[tp], tok_send.at[k - 1], tok_recv.at[k - 1],
            device_id=(me, (tp + k) % n_tp), device_id_type=MESH,
        )

    for h in range(PIECES):
        for a, d in ((0, 0), (1, 1), (0, 1), (1, 0)):
            sender(a, d, 0, h).start()
    for k in range(1, n_tp):
        token_copy(k).start()

    tile = iota((states, columns), 0) == iota((states, columns), 1) % states
    tile_exact, tile_half = tile.astype(f32), tile.astype(bf16)

    def exactly(a, b):
        return jnp.dot(a, b, precision=lax.Precision.HIGHEST, preferred_element_type=f32)

    factors = []

    def build_decay():
        for c in loads:
            c.wait()
        own_head = iota((groups, columns), 0) == iota((groups, columns), 1) // states

        def flat(a):
            return jnp.sum(jnp.where(own_head, exactly(a, tile_exact), 0.0), axis=0, keepdims=True)

        rate_real, rate_imag = flat(rates[0]), flat(rates[1])
        all_groups = step_ref.shape[1]
        head = iota((all_groups, columns), 0) == tp * groups + iota((all_groups, columns), 1) // states
        log_step = exactly(jnp.broadcast_to(step_ref[...], (8, all_groups)), head.astype(f32))[0:1]
        step_size = jnp.exp(log_step) / (rows * n_sp)
        exponent, angle = rate_real * step_size, rate_imag * step_size
        magnitude = jnp.exp(exponent)
        cosine = jnp.cos(angle)
        decay_real, decay_imag = magnitude * cosine, magnitude * jnp.sin(angle)
        series = jnp.ones_like(exponent)
        for k in range(10, 1, -1):
            series = 1.0 + series * exponent * (1.0 / k)
        growth = jnp.where(jnp.abs(exponent) < 0.5, exponent * series, magnitude - 1.0)
        less_one = growth * cosine - 2.0 * jnp.square(jnp.sin(0.5 * angle))
        denominator = rate_real * rate_real + rate_imag * rate_imag
        factors.append((less_one * rate_real + decay_imag * rate_imag) / denominator)
        factors.append((decay_imag * rate_real - less_one * rate_imag) / denominator)
        dec_ref[0:1, :] = decay_real
        dec_ref[1:2, :] = decay_imag

    def spread(k):
        high, low = split(matrices[k].reshape(width, states))
        return dot(high, tile_half) + dot(low, tile_half)

    def build_drive(i):
        same = iota((width, columns), 0) // SSM_GROUP == iota((width, columns), 1) // states
        real, imag = spread(0), spread(1)
        if i == 0:
            drive = factors[0] * real - factors[1] * imag
        else:
            drive = factors[0] * imag + factors[1] * real
        for j, piece in enumerate(split(jnp.where(same, drive, 0.0))):
            dmat[i, j] = piece

    def build_read(i):
        across = (iota((columns, states), 0) % states == iota((columns, states), 1)).astype(bf16)
        same = iota((columns, width), 0) // states == iota((columns, width), 1) // SSM_GROUP
        for j, piece in enumerate(split(matrices[2 + i].reshape(width, states))):
            rmat[i, j] = jnp.where(same, dot_nt(across, piece), 0.0).astype(bf16)

    def build_pool():
        across = (
            iota((POOL_GROUP, pool_width), 0) == iota((POOL_GROUP, pool_width), 1) % POOL_GROUP
        ).astype(bf16)
        same = iota((pool_width, pool_width), 0) // POOL_GROUP == iota((pool_width, pool_width), 1) // POOL_GROUP
        own = pool_own[...].reshape(pool_width, POOL_GROUP)
        pmat[...] = jnp.where(same, dot(own, across), 0.0).astype(bf16)

    squares = []

    def take(t):
        block = tok_full[t].astype(f32)
        squares.append(jnp.sum(block * block, axis=1, keepdims=True))
        cut = slice(t * features, (t + 1) * features)
        scaled[:, cut] = (block * gain_ref[:, cut]).astype(bf16)

    def tokens_in():
        owns[4].wait()
        for k in range(1, n_tp):
            pltpu.make_async_remote_copy(
                tok_ref, tok_full.at[(tp - k + n_tp) % n_tp], tok_send.at[k - 1], tok_recv.at[k - 1],
                device_id=(me, (tp + k) % n_tp), device_id_type=MESH,
            ).wait_recv()

    half = len(turns) // 2
    for at_work, work in enumerate(
        (
            build_decay, lambda: build_drive(0), lambda: build_drive(1), lambda: build_read(0),
            lambda: build_read(1), build_pool,
        )
    ):
        work()
        if at_work in (0, 1, 3, 5):
            step(half)
    while turn[0] < half - 3:
        step(half)
    tokens_in()
    for t in range(n_tp):
        take(t)
        if t == n_tp // 2 - 1:
            step(half)
    while turn[0] < half:
        step(half)
    owns[0].wait()
    owns[1].wait()
    inverse = lax.rsqrt(sum(squares) / (features * n_tp) + epsilon)
    state_in = (dot(scaled[...], wsi[...]) * inverse).astype(bf16)
    pool_in = (dot(scaled[...], wpi[...]) * inverse).astype(bf16)
    ext[window_reach:] = pool_in
    halo_out[...] = pool_in[rows - window_reach :]
    halo_copy = pltpu.make_async_remote_copy(
        halo_out, halo, halo_sem.at[0], halo_sem.at[1],
        device_id=((me + 1) % n_sp, tp), device_id_type=MESH,
    )
    shuffle = (
        iota((rows, rows), 1)
        == (iota((rows, rows), 0) % CHUNKS) * span + iota((rows, rows), 0) // CHUNKS
    ).astype(bf16)
    signal = dot(shuffle, state_in).astype(bf16)
    for i in range(2):
        push[i] = dot(signal, dmat[i, 0]) + dot(signal, dmat[i, 1])
        if i == 0:
            halo_copy.start()
        else:
            step()
    decay_real = jnp.broadcast_to(dec_ref[0:1, :], (CHUNKS, columns))
    decay_imag = jnp.broadcast_to(dec_ref[1:2, :], (CHUNKS, columns))

    def advance(p, carry):
        cut = pl.ds(pl.multiple_of(p * CHUNKS, CHUNKS), CHUNKS)
        real, imag = cmul(decay_real, decay_imag, *carry)
        real, imag = real + push[0, cut, :], imag + push[1, cut, :]
        push[0, cut, :] = real
        push[1, cut, :] = imag
        return real, imag

    zero = jnp.zeros((CHUNKS, columns), f32)
    end_real, end_imag = lax.fori_loop(0, span, advance, (zero, zero))

    def power(real, imag, count):
        out = None
        while count:
            if count % 2:
                out = (real, imag) if out is None else cmul(*out, real, imag)
            real, imag = cmul(real, imag, real, imag)
            count //= 2
        return out

    chunk_decay = power(dec_ref[0:1, :], dec_ref[1:2, :], span)
    block_decay = power(*chunk_decay, CHUNKS)
    row_zero = jnp.zeros((1, columns), f32)
    total = (row_zero, row_zero)
    for j in range(CHUNKS):
        moved = cmul(*chunk_decay, *total)
        total = (moved[0] + end_real[j : j + 1], moved[1] + end_imag[j : j + 1])
    which = iota((CHUNKS, columns), 0)
    ends[me] = jnp.where(which == 0, total[0], jnp.where(which == 1, total[1], 0.0))

    def end_copy(k):
        return pltpu.make_async_remote_copy(
            ends.at[me], ends.at[me], end_send.at[k - 1], end_recv.at[k - 1],
            device_id=((me + k) % n_sp, tp), device_id_type=MESH,
        )

    for k in range(1, n_sp):
        end_copy(k).start()

    halo_copy.wait_recv()
    ext[:window_reach] = jnp.where(me == 0, jnp.zeros_like(halo), halo[...])
    group = tp * (pool_width // POOL_GROUP) + iota((rows, pool_width), 1) // POOL_GROUP
    window = jnp.left_shift(jnp.ones_like(group), group % 4 + 1)
    targets = iota((rows, rows + window_reach), 0) + window_reach
    sources = iota((rows, rows + window_reach), 1)
    whole = ext[...]
    sums = jnp.zeros((rows, pool_width), f32)
    for power_index in range(1, 5):
        reach = 2**power_index
        band = ((sources <= targets) & (sources > targets - reach)).astype(bf16)
        sums = jnp.where(window == reach, dot(band, whole), sums)
        if power_index == 2:
            step()
    position = me * rows + iota((rows, pool_width), 0)
    divisor = jnp.minimum(position + 1, window).astype(f32)
    pooled = sums / divisor - ext[window_reach:].astype(f32)
    pooled_high, pooled_low = split(pooled)
    pool_gain = pg_ref[:, pl.ds(pl.multiple_of(tp * pool_width, pool_width), pool_width)]
    projected = dot(pooled_high, pmat[...]) + dot(pooled_low, pmat[...])
    mine_p[...] = (projected * pool_gain).astype(bf16)
    step()

    def act_copy(which, k, source):
        mine = mine_s if which == 0 else mine_p
        return pltpu.make_async_remote_copy(
            mine, act.at[which, source], act_send.at[which, k - 1], act_recv.at[which, k - 1],
            device_id=(me, (tp + k) % n_tp), device_id_type=MESH,
        )

    for k in range(1, n_tp):
        act_copy(1, k, tp).start()
    act[1, tp] = mine_p[...]

    for k in range(1, n_sp):
        there = ends.at[(me - k + n_sp) % n_sp]
        pltpu.make_async_remote_copy(
            there, there, end_send.at[k - 1], end_recv.at[k - 1],
            device_id=((me + k) % n_sp, tp), device_id_type=MESH,
        ).wait_recv()
    total = (row_zero, row_zero)
    for s in range(n_sp - 1):
        moved = cmul(*block_decay, *total)
        use = s < me
        total = (
            jnp.where(use, moved[0] + ends[s, 0:1, :], total[0]),
            jnp.where(use, moved[1] + ends[s, 1:2, :], total[1]),
        )
    begin_real, begin_imag = zero, zero
    for j in range(CHUNKS):
        begin_real = jnp.where(which == j, total[0], begin_real)
        begin_imag = jnp.where(which == j, total[1], begin_imag)
        moved = cmul(*chunk_decay, *total)
        total = (moved[0] + end_real[j : j + 1], moved[1] + end_imag[j : j + 1])

    def add_carry(p, carry):
        cut = pl.ds(pl.multiple_of(p * CHUNKS, CHUNKS), CHUNKS)
        real, imag = cmul(decay_real, decay_imag, *carry)
        push[0, cut, :] = push[0, cut, :] + real
        push[1, cut, :] = push[1, cut, :] + imag
        return real, imag

    lax.fori_loop(0, span, add_carry, (begin_real, begin_imag))
    step()
    real_high, real_low = split(push[0])
    imag_high, imag_low = split(push[1])
    readout = dot(real_high, rmat[0, 0]) + dot(real_high, rmat[0, 1]) + dot(real_low, rmat[0, 0])
    step()
    readout -= dot(imag_high, rmat[1, 0]) + dot(imag_high, rmat[1, 1]) + dot(imag_low, rmat[1, 0])
    skip = skip_ref[:, pl.ds(pl.multiple_of(tp * width, width), width)]
    readout += skip * signal.astype(f32)
    shuffled = jax.nn.gelu(readout).astype(bf16)
    restore = (
        iota((rows, rows), 0)
        == (iota((rows, rows), 1) % CHUNKS) * span + iota((rows, rows), 1) // CHUNKS
    ).astype(bf16)
    mine_s[...] = dot(restore, shuffled).astype(bf16)
    for k in range(1, n_tp):
        act_copy(0, k, tp).start()
    act[0, tp] = mine_s[...]
    while turn[0] < len(turns):
        step()
    for which in (1, 0):
        for k in range(1, n_tp):
            act_copy(which, k, (tp - k + n_tp) % n_tp).wait_recv()
    owns[2].wait()
    owns[3].wait()
    result = None
    for t in range(n_tp):
        for which, full, size in ((1, wpo, pool_width), (0, wso, width)):
            term = dot(act[which, t], full[t * size : (t + 1) * size, :])
            result = term if result is None else result + term
    out_ref[...] = result.astype(bf16)

    for a in range(4):
        for d in range(2):
            for s in range(reach_of(a, d)):
                for h in range(PIECES):
                    sender(a, d, s, h).wait_send()
    for k in range(1, n_tp):
        token_copy(k).wait_send()
        act_copy(0, k, tp).wait_send()
        act_copy(1, k, tp).wait_send()
    halo_copy.wait_send()
    for k in range(1, n_sp):
        end_copy(k).wait_send()

LANES = 128
HALVES = 2


def slab_kernel(
    n_sp, n_tp, n_x, states,
    tok_ref, gain_ref, wsi_ref, wpi_ref, rr_ref, ri_ref, step_ref, inr_ref, ini_ref, outr_ref,
    outi_ref, skip_ref, pw_ref, pg_ref, wso_ref, wpo_ref,
    out_ref,
    tok, scaled, squares, w_in, w_out, dmat, rmat, pmat, push, order, halo, halo_out, ends, act,
    made, rates, matrices, pool_own, dec_ref,
    own_sem, xw_send, xw_recv, z_send, z_recv, tok_send, tok_recv, act_send, act_recv, halo_sem, end_send, end_recv,
    out_send, out_recv,
):
    me, tp = lax.axis_index("sp"), lax.axis_index("tp")
    n_z = n_sp // n_x
    z, x = me // n_x, me % n_x
    y, core = tp // 2, tp % 2
    rows = tok_ref.shape[0]
    slab = rows * n_x
    features = tok_ref.shape[1]
    in_rows = wsi_ref.shape[0]
    out_rows = wso_ref.shape[0]
    width = wsi_ref.shape[1] // n_x
    out_width = wso_ref.shape[1] // n_x
    chunk_count = out_width // LANES
    groups = width // SSM_GROUP
    columns = groups * states
    pool_groups = width // POOL_GROUP
    span = slab // CHUNKS
    q = tp * n_x + x

    across, pair, both = (1 - y) * 2 + core, y * 2 + 1 - core, (1 - y) * 2 + 1 - core
    beside = me + 1 - 2 * x
    to_x, to_y, to_pair = (beside, tp), (me, across), (me, pair)
    ways = (1, -1)

    def to_z(way):
        return (me + way * n_x, tp)

    def inside(at):
        return jnp.logical_and(at >= 0, at < n_z)

    def aligned(index, size):
        return pl.ds(pl.multiple_of(index * size, size), size)

    barrier = pltpu.get_barrier_semaphore()
    for there in (to_x, to_y, to_pair):
        pl.semaphore_signal(barrier, inc=1, device_id=there, device_id_type=MESH)
    for way in ways:
        @pl.when(inside(z + way))
        def _():
            pl.semaphore_signal(barrier, inc=1, device_id=to_z(way), device_id_type=MESH)

    def remote(source, there, send, recv, target):
        return pltpu.make_async_remote_copy(
            source, there, send, recv, device_id=target, device_id_type=MESH
        )

    def in_part(ref, half):
        return ref.at[:, aligned(half, width)]

    def out_part(ref, half, j):
        return ref.at[:, pl.ds(pl.multiple_of(half * out_width + j * LANES, LANES), LANES)]

    own_in, own_out = (wsi_ref, wpi_ref), (wso_ref, wpo_ref)

    def in_at(m, sp):
        return w_in.at[m, aligned(sp, in_rows)]

    def out_at(j, m, sp):
        return w_out.at[j, m, aligned(sp, out_rows)]

    def own_copy(k):
        if k < 2:
            return [pltpu.make_async_copy(in_part(own_in[k], x), in_at(k, me), own_sem.at[k])]
        return [
            pltpu.make_async_copy(out_part(own_out[m], x, k - 2), out_at(k - 2, m, me), own_sem.at[k])
            for m in range(2)
        ]

    def own_wait(k):
        here = in_at(k, me) if k < 2 else w_out.at[k - 2, :, aligned(me, out_rows)]
        pltpu.make_async_copy(here, here, own_sem.at[k]).wait()

    base = 2 + chunk_count
    tok_copy = pltpu.make_async_copy(tok_ref, tok.at[tp, aligned(x, rows)], own_sem.at[base])

    def heads(ref, count):
        return ref.at[aligned(q, count)]

    loads = [
        pltpu.make_async_copy(heads(ref, count), there, own_sem.at[base + 1 + k])
        for ref, count, there, k in (
            (rr_ref, groups, rates.at[0], 0), (ri_ref, groups, rates.at[1], 0),
            (inr_ref, groups, matrices.at[0], 1), (ini_ref, groups, matrices.at[1], 1),
            (outr_ref, groups, matrices.at[2], 1), (outi_ref, groups, matrices.at[3], 1),
            (pw_ref, pool_groups, pool_own, 2),
        )
    ]
    for c in own_copy(0) + [tok_copy] + loads + [c for k in range(1, base) for c in own_copy(k)]:
        c.start()

    def x_weights(k, sp):
        if k < 2:
            return in_part(own_in[k], 1 - x), in_at(k, sp)
        j, m = (k - 2) // 2, k % 2
        return out_part(own_out[m], 1 - x, j), out_at(j, m, sp)

    x_kinds = 2 + 2 * chunk_count

    def x_slot(k):
        return xw_recv.at[k if k < 2 else 2 + (k - 2) // 2]

    def x_send(k):
        return remote(*x_weights(k, me), xw_send.at[0], x_slot(k), to_x)

    @jax.named_scope("across_wait")
    def x_wait(k):
        here = in_at(k, beside) if k < 2 else w_out.at[k - 2, :, aligned(beside, out_rows)]
        remote(here, here, xw_send.at[0], xw_recv.at[k], to_x).wait_recv()

    stage_count = 2 + chunk_count

    def z_part(stage, h, at):
        if stage < 2:
            return in_at(stage, at * n_x + (x if h == 0 else 1 - x))
        return w_out.at[stage - 2, h, aligned(at, out_rows * n_x)]

    def z_copy(d, stage, s, h):
        at = z - ways[d] * s
        there = z_part(stage, h, at)
        return remote(there, there, z_send.at[d, s], z_recv.at[stage, at, h], to_z(ways[d]))

    def z_own(stage, h):
        for d in range(2):
            @pl.when(inside(z + ways[d]))
            def _():
                z_copy(d, stage, 0, h).start()

    def z_arrive(d, stage, s, h):
        at = z - ways[d] * (s + 1)
        here = z_part(stage, h, at)
        remote(here, here, z_send.at[d, s], z_recv.at[stage, at, h], to_z(ways[d])).wait_recv()

    @jax.named_scope("relay_wait")
    def z_relay(stage, s, h):
        for d in range(2):
            @pl.when(jnp.logical_and(inside(z - ways[d] * (s + 1)), inside(z + ways[d])))
            def _():
                z_arrive(d, stage, s, h)
                z_copy(d, stage, s + 1, h).start()

    @jax.named_scope("final_wait")
    def z_final(stage, distances=range(n_z - 1)):
        for d in range(2):
            for s in distances:
                @pl.when(jnp.logical_and(inside(z - ways[d] * (s + 1)), jnp.logical_not(inside(z + ways[d]))))
                def _():
                    for h in range(2):
                        z_arrive(d, stage, s, h)

    def out_own(j):
        x_wait(2 + j)
        own_wait(2 + j)
        for m in range(2):
            z_own(2 + j, m)

    relays = [(m, 0, h) for h in range(2) for m in range(2)]
    relays += [(m, s, h) for m in range(2) for s in range(1, n_z - 2) for h in range(2)]
    in_relays = len(relays)
    later = [(2 + j, s, m) for j in range(chunk_count) for s in range(n_z - 2) for m in range(2)]
    relays += sorted(later, key=lambda r: (r[0] > 2, r[1], r[0], r[2]))
    turn = [0]

    def progress(count=1, stop=None):
        while count and turn[0] < (len(relays) if stop is None else stop):
            z_relay(*relays[turn[0]])
            turn[0] += 1
            count -= 1

    class Gather:
        def __init__(self, region, pair_region, send, recv):
            self.region, self.pair_region, self.send, self.recv = region, pair_region, send, recv

        def copy(self, slot, p):
            at_tp, at_x = ((tp, x), (tp, x), (tp, 1 - x), (tp, x), (tp, 1 - x), (across, x), (across, 1 - x))[slot]
            here = self.region(at_tp, at_x, p)
            recv = self.recv.at[2 * slot + p if slot < 3 else 6 if slot < 5 else 7]
            return remote(here, here, self.send, recv, (to_x, to_y, to_y, to_pair, to_pair, to_pair, to_pair)[slot])

        def start(self, *slots, p):
            for slot in slots:
                self.copy(slot, p).start()

        @jax.named_scope("gather_wait")
        def wait(self, slot, p):
            here = self.region(*((tp, 1 - x), (across, x), (across, 1 - x))[slot], p)
            remote(here, here, self.send, self.recv.at[2 * slot + p], to_pair).wait_recv()

        @jax.named_scope("pair_wait")
        def wait_pair(self, at_tp, k):
            here = self.pair_region(at_tp)
            remote(here, here, self.send, self.recv.at[6 + k], to_pair).wait_recv()

        def relay_x(self, p):
            self.wait(0, p)
            self.start(2, 4, p=p)

        def relay_y(self, p):
            self.wait(1, p)
            self.start(5, p=p)

        def relay_both(self, p):
            self.wait(2, p)
            self.start(6, p=p)

        def drain(self, sent):
            remote(sent, sent, self.send, self.recv.at[0], to_pair).wait_send()

    piece = rows // HALVES

    def tok_region(at_tp, at_x, p):
        return tok.at[at_tp, pl.ds(pl.multiple_of(at_x * rows + p * piece, piece), piece)]

    tokens = Gather(tok_region, lambda at_tp: tok.at[at_tp], tok_send.at[0], tok_recv)

    def act_gather(which):
        size = slab // HALVES

        def region(at_tp, at_x, p):
            return act.at[which, pl.ds(p * size, size), aligned(at_tp * n_x + at_x, width)]

        def pair_region(at_tp):
            return act.at[which, :, aligned(at_tp, n_x * width)]

        return Gather(region, pair_region, act_send.at[which], act_recv.at[which])

    acts = (act_gather(0), act_gather(1))

    pl.semaphore_wait(barrier, 3 + inside(z + 1).astype(jnp.int32) + inside(z - 1).astype(jnp.int32))

    x_send(0).start()
    own_wait(0)
    z_own(0, 0)
    own_wait(1)
    z_own(1, 0)
    x_send(1).start()
    tok_copy.wait()
    for p in range(HALVES):
        tokens.start(0, 1, 3, p=p)
    for k in range(2, x_kinds):
        x_send(k).start()

    tile = iota((states, columns), 0) == iota((states, columns), 1) % states
    tile_exact, tile_half = tile.astype(f32), tile.astype(bf16)

    def exactly(a, b):
        return jnp.dot(a, b, precision=lax.Precision.HIGHEST, preferred_element_type=f32)

    factors = []

    @jax.named_scope("build_decay")
    def build_decay():
        for c in loads:
            c.wait()
        own_head = iota((groups, columns), 0) == iota((groups, columns), 1) // states

        def flat(a):
            return jnp.sum(jnp.where(own_head, exactly(a, tile_exact), 0.0), axis=0, keepdims=True)

        rate_real, rate_imag = flat(rates[0]), flat(rates[1])
        all_groups = step_ref.shape[1]
        head = iota((all_groups, columns), 0) == q * groups + iota((all_groups, columns), 1) // states
        log_step = exactly(jnp.broadcast_to(step_ref[...], (8, all_groups)), head.astype(f32))[0:1]
        step_size = jnp.exp(log_step) / (rows * n_sp)
        exponent, angle = rate_real * step_size, rate_imag * step_size
        magnitude = jnp.exp(exponent)
        cosine = jnp.cos(angle)
        decay_real, decay_imag = magnitude * cosine, magnitude * jnp.sin(angle)
        series = jnp.ones_like(exponent)
        for k in range(10, 1, -1):
            series = 1.0 + series * exponent * (1.0 / k)
        growth = jnp.where(jnp.abs(exponent) < 0.5, exponent * series, magnitude - 1.0)
        less_one = growth * cosine - 2.0 * jnp.square(jnp.sin(0.5 * angle))
        denominator = rate_real * rate_real + rate_imag * rate_imag
        factors.append((less_one * rate_real + decay_imag * rate_imag) / denominator)
        factors.append((decay_imag * rate_real - less_one * rate_imag) / denominator)
        dec_ref[0:1, :] = decay_real
        dec_ref[1:2, :] = decay_imag

    def spread(k):
        high, low = split(matrices[k].reshape(width, states))
        return dot(high, tile_half) + dot(low, tile_half)

    @jax.named_scope("build_drive")
    def build_drive(i):
        same = iota((width, columns), 0) // SSM_GROUP == iota((width, columns), 1) // states
        real, imag = spread(0), spread(1)
        if i == 0:
            drive = factors[0] * real - factors[1] * imag
        else:
            drive = factors[0] * imag + factors[1] * real
        for j, part in enumerate(split(jnp.where(same, drive, 0.0))):
            dmat[i, j] = part

    @jax.named_scope("build_read")
    def build_read(i):
        onto = (iota((columns, states), 0) % states == iota((columns, states), 1)).astype(bf16)
        same = iota((columns, width), 0) // states == iota((columns, width), 1) // SSM_GROUP
        for j, part in enumerate(split(matrices[2 + i].reshape(width, states))):
            rmat[i, j] = jnp.where(same, dot_nt(onto, part), 0.0).astype(bf16)

    @jax.named_scope("build_pool")
    def build_pool():
        onto = (iota((POOL_GROUP, width), 0) == iota((POOL_GROUP, width), 1) % POOL_GROUP).astype(bf16)
        same = iota((width, width), 0) // POOL_GROUP == iota((width, width), 1) // POOL_GROUP
        own = pool_own[...].reshape(width, POOL_GROUP)
        pmat[...] = jnp.where(same, dot(own, onto), 0.0).astype(bf16)

    @jax.named_scope("build_order")
    def build_order(i):
        a, b = iota((slab, slab), i), iota((slab, slab), 1 - i)
        order[i] = (b == (a % CHUNKS) * span + a // CHUNKS).astype(bf16)

    @jax.named_scope("take")
    def take(at_tp, first):
        cut = pl.ds(pl.multiple_of(at_tp * features, features), features)
        gain = gain_ref[:, cut]
        size = min(64, slab)

        def step(i, _):
            here = pl.ds(pl.multiple_of(i * size, size), size)
            block = tok[at_tp, here].astype(f32)
            total = jnp.broadcast_to(jnp.sum(block * block, axis=1, keepdims=True), (size, LANES))
            squares[here] = total if first else squares[here] + total
            scaled[here, cut] = (block * gain).astype(bf16)
            return 0

        lax.fori_loop(0, slab // size, step, 0)

    build_decay()
    build_drive(0)
    progress()
    x_wait(0)
    z_own(0, 1)
    progress()
    x_wait(1)
    z_own(1, 1)
    build_drive(1)
    build_read(0)
    progress()
    build_read(1)
    progress()
    tokens.relay_x(0)
    build_order(0)
    progress()
    build_pool()
    tokens.relay_y(0)
    tokens.relay_x(1)
    progress()
    build_order(1)
    progress(stop=in_relays)
    tokens.relay_y(1)
    tokens.wait_pair(pair, 0)
    take(tp, True)
    progress(stop=in_relays)
    take(pair, False)
    progress(stop=in_relays)
    tokens.relay_both(0)
    out_own(0)
    tokens.relay_both(1)
    take(across, False)
    tokens.wait_pair(both, 1)
    take(both, False)
    progress(2)
    inverse = lax.rsqrt(squares[...] / (features * n_tp) + epsilon)
    z_final(0)
    state_in = (dot(scaled[...], w_in[0]) * inverse).astype(bf16)
    signal = dot(order[0], state_in).astype(bf16)
    for i in range(2):
        push[i] = dot(signal, dmat[i, 0]) + dot(signal, dmat[i, 1])
    decay_real = jnp.broadcast_to(dec_ref[0:1, :], (CHUNKS, columns))
    decay_imag = jnp.broadcast_to(dec_ref[1:2, :], (CHUNKS, columns))

    def advance(p, carry):
        cut = pl.ds(pl.multiple_of(p * CHUNKS, CHUNKS), CHUNKS)
        real, imag = cmul(decay_real, decay_imag, *carry)
        real, imag = real + push[0, cut, :], imag + push[1, cut, :]
        push[0, cut, :] = real
        push[1, cut, :] = imag
        return real, imag

    zero = jnp.zeros((CHUNKS, columns), f32)
    end_real, end_imag = lax.fori_loop(0, span, advance, (zero, zero), unroll=4)

    def power(real, imag, count):
        out = None
        while count:
            if count % 2:
                out = (real, imag) if out is None else cmul(*out, real, imag)
            real, imag = cmul(real, imag, real, imag)
            count //= 2
        return out

    chunk_decay = power(dec_ref[0:1, :], dec_ref[1:2, :], span)
    block_decay = power(*chunk_decay, CHUNKS)
    row_zero = jnp.zeros((1, columns), f32)
    total = (row_zero, row_zero)
    for j in range(CHUNKS):
        moved = cmul(*chunk_decay, *total)
        total = (moved[0] + end_real[j : j + 1], moved[1] + end_imag[j : j + 1])
    which = iota((CHUNKS, columns), 0)
    ends[z] = jnp.where(which == 0, total[0], jnp.where(which == 1, total[1], 0.0))

    def end_copy(k):
        return remote(ends.at[z], ends.at[z], end_send.at[k - 1], end_recv.at[k - 1], (me + k * n_x, tp))

    for k in range(1, n_z):
        @pl.when(inside(z + k))
        def _():
            end_copy(k).start()

    if chunk_count > 1:
        out_own(1)
    z_final(1)
    pool_in = (dot(scaled[...], w_in[1]) * inverse).astype(bf16)
    halo_out[...] = pool_in[slab - window_reach :]
    halo_copy = remote(halo_out, halo, halo_sem.at[0], halo_sem.at[1], to_z(1))

    @pl.when(inside(z + 1))
    def _():
        halo_copy.start()

    progress(2)
    for j in range(2, chunk_count):
        out_own(j)
    for k in range(1, n_z):
        @pl.when(inside(z - k))
        @jax.named_scope("ends_wait")
        def _():
            there = ends.at[z - k]
            remote(there, there, end_send.at[k - 1], end_recv.at[k - 1], to_z(1)).wait_recv()

    total = (row_zero, row_zero)
    for s in range(n_z - 1):
        moved = cmul(*block_decay, *total)
        use = s < z
        total = (
            jnp.where(use, moved[0] + ends[s, 0:1, :], total[0]),
            jnp.where(use, moved[1] + ends[s, 1:2, :], total[1]),
        )
    begin_real, begin_imag = zero, zero
    for j in range(CHUNKS):
        begin_real = jnp.where(which == j, total[0], begin_real)
        begin_imag = jnp.where(which == j, total[1], begin_imag)
        moved = cmul(*chunk_decay, *total)
        total = (moved[0] + end_real[j : j + 1], moved[1] + end_imag[j : j + 1])

    def add_carry(p, carry):
        cut = pl.ds(pl.multiple_of(p * CHUNKS, CHUNKS), CHUNKS)
        real, imag = cmul(decay_real, decay_imag, *carry)
        push[0, cut, :] = push[0, cut, :] + real
        push[1, cut, :] = push[1, cut, :] + imag
        return real, imag

    lax.fori_loop(0, span, add_carry, (begin_real, begin_imag), unroll=4)
    progress(2)
    real_high, real_low = split(push[0])
    imag_high, imag_low = split(push[1])
    readout = dot(real_high, rmat[0, 0]) + dot(real_high, rmat[0, 1]) + dot(real_low, rmat[0, 0])
    readout -= dot(imag_high, rmat[1, 0]) + dot(imag_high, rmat[1, 1]) + dot(imag_low, rmat[1, 0])
    skip = skip_ref[:, aligned(q, width)]
    readout += skip * signal.astype(f32)
    shuffled = jax.nn.gelu(readout).astype(bf16)
    act[0, :, aligned(q, width)] = dot(order[1], shuffled).astype(bf16)
    for p in range(HALVES):
        acts[0].start(0, 1, 3, p=p)
    progress(2)

    @pl.when(z > 0)
    @jax.named_scope("halo_wait")
    def _():
        halo_copy.wait_recv()

    before = jnp.where(z == 0, jnp.zeros_like(halo), halo[...])
    whole = jnp.concatenate([before, pool_in], axis=0).astype(f32)
    window = jnp.left_shift(2, (q * pool_groups + iota((slab, width), 1) // POOL_GROUP) % 4)
    sums = jnp.zeros((slab, width), f32)
    running = whole
    for level in range(4):
        running = running + pltpu.roll(running, 2**level, 0)
        sums = jnp.where(window == 2 ** (level + 1), running[window_reach:], sums)
    position = z * slab + iota((slab, width), 0)
    divisor = jnp.minimum(position + 1, window).astype(f32)
    pooled = sums / divisor - whole[window_reach:]
    pooled_high, pooled_low = split(pooled)
    pool_gain = pg_ref[:, aligned(q, width)]
    projected = dot(pooled_high, pmat[...]) + dot(pooled_low, pmat[...])
    act[1, :, aligned(q, width)] = (projected * pool_gain).astype(bf16)
    for p in range(HALVES):
        acts[1].start(0, 1, 3, p=p)
    progress(2)
    for k in range(2):
        for p in range(HALVES):
            acts[k].relay_x(p)
            acts[k].relay_y(p)
            progress()
    for k in range(2):
        for p in range(HALVES):
            acts[k].relay_both(p)
            progress()
    progress(len(relays))
    for k in range(2):
        acts[k].wait_pair(pair, 0)
        acts[k].wait_pair(both, 1)

    def out_columns(half, j):
        return pl.ds(pl.multiple_of(half * out_width + j * LANES, LANES), LANES)

    def out_copy(j):
        return remote(made.at[j], out_ref.at[:, out_columns(x, j)], out_send.at[0], out_recv.at[0], to_x)

    def part(j, half, at):
        cut, depth = aligned(half, rows), aligned(at, n_x * out_rows)
        return dot(act[0, cut, depth], w_out[j, 0, depth]) + dot(act[1, cut, depth], w_out[j, 1, depth])

    def make(j, half):
        cut = aligned(half, rows)
        return dot(act[0, cut], w_out[j, 0]) + dot(act[1, cut], w_out[j, 1])

    for j in range(chunk_count):
        if j + 1 < chunk_count:
            z_final(2 + j)
            made[j] = make(j, 1 - x).astype(bf16)
            out_copy(j).start()
            out_ref[:, out_columns(x, j)] = make(j, x).astype(bf16)
        else:
            far = n_z - 1 - z
            z_final(2 + j, range(n_z - 2))
            sums = [
                sum(part(j, half, (far + 1 + r) % n_z) for r in range(n_z - 1)) for half in (1 - x, x)
            ]
            z_final(2 + j, range(n_z - 2, n_z - 1))
            made[j] = (sums[0] + part(j, 1 - x, far)).astype(bf16)
            out_copy(j).start()
            out_ref[:, out_columns(x, j)] = (sums[1] + part(j, x, far)).astype(bf16)

    @jax.named_scope("drain")
    def drain():
        sent = w_in.at[0, pl.ds(0, 2 * in_rows + 2 * chunk_count * out_rows)]
        remote(sent, sent, xw_send.at[0], xw_recv.at[0], to_x).wait_send()
        sent = w_in.at[0, pl.ds(0, n_x * (2 * in_rows + 2 * chunk_count * out_rows))]
        for d in range(2):
            for s in range(n_z - 1):
                @pl.when(jnp.logical_and(inside(z + ways[d]), inside(z - ways[d] * s)))
                def _():
                    remote(sent, sent, z_send.at[d, s], z_recv.at[0, 0, 0], to_z(ways[d])).wait_send()
        tokens.drain(scaled.at[pl.ds(0, 7 * rows // n_tp)])
        for k in range(2):
            acts[k].drain(act.at[k, :, pl.ds(0, 7 * width)])

        @pl.when(inside(z + 1))
        def _():
            halo_copy.wait_send()

        for k in range(1, n_z):
            @pl.when(inside(z + k))
            def _():
                end_copy(k).wait_send()

        remote(made, made, out_send.at[0], out_recv.at[0], to_x).wait_send()

    drain()
    with jax.named_scope("out_wait"):
        here = out_ref.at[:, aligned(1 - x, out_width)]
        remote(here, here, out_send.at[0], out_recv.at[0], to_x).wait_recv()


def slab_call(n_sp, n_tp, n_x, arrays):
    tokens, state_in_weight, state_out_weight = arrays[0], arrays[2], arrays[14]
    rows, features = tokens.shape
    in_rows, width = state_in_weight.shape
    out_rows, out_columns = state_out_weight.shape
    width //= n_x
    n_z, slab, chunk_count = n_sp // n_x, rows * n_x, out_columns // n_x // LANES
    groups, states = width // SSM_GROUP, arrays[4].shape[1]
    columns, pool_groups = groups * states, width // POOL_GROUP
    vmem = pl.BlockSpec(memory_space=pltpu.VMEM)
    anywhere = pl.BlockSpec(memory_space=pl.ANY)
    dma = pltpu.SemaphoreType.DMA
    return pl.pallas_call(
        functools.partial(slab_kernel, n_sp, n_tp, n_x, states),
        out_shape=pltpu.VMEM((rows, out_columns), bf16),
        in_specs=[anywhere, vmem] + [anywhere] * 4 + [vmem] + [anywhere] * 4 + [vmem, anywhere, vmem]
        + [anywhere] * 2,
        out_specs=vmem,
        scratch_shapes=[
            pltpu.VMEM((n_tp, slab, features), bf16),
            pltpu.VMEM((slab, features * n_tp), bf16),
            pltpu.VMEM((slab, LANES), f32),
            pltpu.VMEM((2, n_sp * in_rows, width), bf16),
            pltpu.VMEM((chunk_count, 2, n_sp * out_rows, LANES), bf16),
            pltpu.VMEM((2, 2, width, columns), bf16),
            pltpu.VMEM((2, 2, columns, width), bf16),
            pltpu.VMEM((width, width), bf16),
            pltpu.VMEM((2, slab, columns), f32),
            pltpu.VMEM((2, slab, slab), bf16),
            pltpu.VMEM((window_reach, width), bf16),
            pltpu.VMEM((window_reach, width), bf16),
            pltpu.VMEM((n_z, CHUNKS, columns), f32),
            pltpu.VMEM((2, slab, n_tp * n_x * width), bf16),
            pltpu.VMEM((chunk_count, rows, LANES), bf16),
            pltpu.VMEM((2, groups, states), f32),
            pltpu.VMEM((4, groups, SSM_GROUP, states), f32),
            pltpu.VMEM((pool_groups, POOL_GROUP, POOL_GROUP), bf16),
            pltpu.VMEM((2, columns), f32),
            dma((6 + chunk_count,)),
            dma((1,)),
            dma((2 + chunk_count,)),
            dma((2, n_z - 1)),
            dma((2 + chunk_count, n_z, 2)),
            dma((1,)),
            dma((8,)),
            dma((2,)),
            dma((2, 8)),
            dma((2,)),
            dma((n_z - 1,)),
            dma((n_z - 1,)),
            dma((1,)),
            dma((1,)),
        ],
        compiler_params=pltpu.CompilerParams(
            collective_id=0, has_side_effects=True, vmem_limit_bytes=60 * 2**20
        ),
    )(*arrays)


def slab_fits(n_sp, n_tp, n_x, in_rows, width, pool_width, out_rows, out_columns):
    return (
        n_x == 2 and n_tp == 4 and n_sp // n_x >= 3 and width == n_x * LANES
        and pool_width == width and out_columns % (n_x * LANES) == 0
        and n_x * (2 * in_rows + out_columns // (n_x * LANES) * 2 * out_rows) <= n_sp * in_rows
    )


def body(
    n_sp, n_tp, n_x,
    tokens, norm_gain, state_in_weight, pool_in_weight, rate_real, rate_imag, log_step,
    input_real, input_imag, output_real, output_imag, skip_gain, pool_weight, pool_gain,
    state_out_weight, pool_out_weight,
):
    rows, features = tokens.shape
    in_rows, width = state_in_weight.shape
    pool_width = pool_in_weight.shape[1]
    out_rows, out_columns = state_out_weight.shape
    groups = width // SSM_GROUP
    states = rate_real.shape[1]
    columns = groups * states
    pool_groups = pool_width // POOL_GROUP
    if slab_fits(n_sp, n_tp, n_x, in_rows, width, pool_width, out_rows, out_columns):
        return slab_call(n_sp, n_tp, n_x, (
            tokens, norm_gain[None], state_in_weight, pool_in_weight, rate_real, rate_imag, log_step[None],
            jnp.swapaxes(input_real, 1, 2), jnp.swapaxes(input_imag, 1, 2), output_real, output_imag,
            skip_gain[None], pool_weight, pool_gain[None], state_out_weight, pool_out_weight,
        ))
    vmem = pl.BlockSpec(memory_space=pltpu.VMEM)
    anywhere = pl.BlockSpec(memory_space=pl.ANY)
    dma = pltpu.SemaphoreType.DMA
    return pl.pallas_call(
        functools.partial(kernel, n_sp, n_tp, n_x, states),
        out_shape=jax.ShapeDtypeStruct((rows, out_columns), bf16),
        in_specs=[anywhere, vmem] + [anywhere] * 4 + [vmem] + [anywhere] * 4 + [vmem, anywhere, vmem]
        + [anywhere] * 2,
        out_specs=vmem,
        scratch_shapes=[
            pltpu.VMEM((n_tp, rows, features), bf16),
            pltpu.VMEM((n_sp * in_rows, width), bf16),
            pltpu.VMEM((n_sp * in_rows, pool_width), bf16),
            pltpu.VMEM((n_sp * out_rows, out_columns), bf16),
            pltpu.VMEM((n_sp * out_rows, out_columns), bf16),
            pltpu.VMEM((rows, features * n_tp), bf16),
            pltpu.VMEM((2, 2, width, columns), bf16),
            pltpu.VMEM((2, 2, columns, width), bf16),
            pltpu.VMEM((pool_width, pool_width), bf16),
            pltpu.VMEM((2, rows, columns), f32),
            pltpu.VMEM((rows + window_reach, pool_width), bf16),
            pltpu.VMEM((window_reach, pool_width), bf16),
            pltpu.VMEM((n_sp, CHUNKS, columns), f32),
            pltpu.VMEM((2, n_tp, rows, width), bf16),
            pltpu.VMEM((rows, width), bf16),
            pltpu.VMEM((rows, pool_width), bf16),
            pltpu.VMEM((window_reach, pool_width), bf16),
            pltpu.VMEM((2, groups, states), f32),
            pltpu.VMEM((4, groups, SSM_GROUP, states), f32),
            pltpu.VMEM((pool_groups, POOL_GROUP, POOL_GROUP), bf16),
            pltpu.VMEM((2, columns), f32),
            dma((12,)),
            dma((4, 2, n_sp // 2, PIECES)),
            dma((4, 2, n_sp // 2, PIECES)),
            dma((n_tp - 1,)),
            dma((n_tp - 1,)),
            dma((2, n_tp - 1)),
            dma((2, n_tp - 1)),
            dma((2,)),
            dma((n_sp - 1,)),
            dma((n_sp - 1,)),
        ],
        compiler_params=pltpu.CompilerParams(
            collective_id=0, has_side_effects=True, vmem_limit_bytes=60 * 2**20
        ),
    )(
        tokens, norm_gain[None], state_in_weight, pool_in_weight, rate_real, rate_imag, log_step[None],
        jnp.swapaxes(input_real, 1, 2), jnp.swapaxes(input_imag, 1, 2), output_real, output_imag,
        skip_gain[None], pool_weight, pool_gain[None], state_out_weight, pool_out_weight,
    )


def solution(mesh):
    n_sp, n_tp = mesh.shape["sp"], mesh.shape["tp"]
    n_x = 2 ** ((n_sp.bit_length() - 1) // 2)
    both, whole = P("sp", "tp"), P()
    return jax.shard_map(
        functools.partial(body, n_sp, n_tp, n_x),
        mesh=mesh,
        in_specs=(both, whole, both, both) + (whole,) * 10 + (both, both),
        out_specs=both,
        check_vma=False,
    )
```

```python
import functools

import jax
import jax.numpy as jnp
from jax import lax
from jax.experimental import pallas as pl
from jax.experimental.pallas import tpu as pltpu
from jax.sharding import PartitionSpec as P

SSM_GROUP = 16
POOL_GROUP = 64
CHUNKS = 8
PIECES = 2

epsilon = 1e-06
window_reach = 16
f32, bf16 = jnp.float32, jnp.bfloat16
MESH = pl.DeviceIdType.MESH


def discretize(rate_real, rate_imag, log_step, length):
    step_size = jnp.exp(log_step)[:, None] / length
    exponent = rate_real * step_size
    angle = rate_imag * step_size
    magnitude = jnp.exp(exponent)
    decay_real = magnitude * jnp.cos(angle)
    decay_imag = magnitude * jnp.sin(angle)
    less_one = jnp.expm1(exponent) * jnp.cos(angle) - 2.0 * jnp.square(jnp.sin(0.5 * angle))
    denominator = rate_real * rate_real + rate_imag * rate_imag
    factor_real = (less_one * rate_real + decay_imag * rate_imag) / denominator
    factor_imag = (decay_imag * rate_real - less_one * rate_imag) / denominator
    return decay_real, decay_imag, factor_real, factor_imag


def iota(shape, axis):
    return lax.broadcasted_iota(jnp.int32, shape, axis)


def dot(a, b):
    return jnp.dot(a, b, preferred_element_type=f32)


def dot_nt(a, b):
    return lax.dot_general(a, b, (((1,), (1,)), ((), ())), preferred_element_type=f32)


def split(a):
    high = a.astype(bf16)
    return high, (a - high.astype(f32)).astype(bf16)


def cmul(ar, ai, br, bi):
    return ar * br - ai * bi, ar * bi + ai * br


def kernel(
    n_sp, n_tp, n_x, states,
    tok_ref, gain_ref, wsi_ref, wpi_ref, rr_ref, ri_ref, step_ref, inr_ref, ini_ref, outr_ref,
    outi_ref, skip_ref, pw_ref, pg_ref, wso_ref, wpo_ref,
    out_ref,
    tok_full, wsi, wpi, wso, wpo, scaled, dmat, rmat, pmat, push, ext, halo, ends, act,
    mine_s, mine_p, halo_out, rates, matrices, pool_own, dec_ref,
    own_sem, ring_send, ring_recv, tok_send, tok_recv, act_send, act_recv, halo_sem, end_send, end_recv,
):
    me, tp = lax.axis_index("sp"), lax.axis_index("tp")
    n_z = n_sp // n_x
    rows = tok_ref.shape[0]
    features = tok_ref.shape[1]
    width = wsi_ref.shape[1]
    pool_width = wpi_ref.shape[1]
    groups = width // SSM_GROUP
    columns = groups * states
    pool_groups = pool_width // POOL_GROUP
    span = rows // CHUNKS

    def place(p):
        x, r = p // n_z, p % n_z
        return (r + (x % 2) * (n_z - 1 - 2 * r)) * n_x + x

    my_x, my_z = me % n_x, me // n_x
    at = my_x * n_z + my_z + (my_x % 2) * (n_z - 1 - 2 * my_z)

    barrier = pltpu.get_barrier_semaphore()
    for k in range(1, n_sp):
        pl.semaphore_signal(barrier, inc=1, device_id=((me + k) % n_sp, tp), device_id_type=MESH)
    for k in range(1, n_tp):
        pl.semaphore_signal(barrier, inc=1, device_id=(me, (tp + k) % n_tp), device_id_type=MESH)

    fulls = ((wsi_ref, wsi), (wpi_ref, wpi), (wso_ref, wso), (wpo_ref, wpo))
    owns = []
    for a, (own, full) in enumerate(fulls):
        count = own.shape[0]
        owns.append(
            pltpu.make_async_copy(
                own, full.at[pl.ds(pl.multiple_of(me * count, count), count)], own_sem.at[a]
            )
        )
    owns.append(pltpu.make_async_copy(tok_ref, tok_full.at[tp], own_sem.at[4]))
    def heads(ref, count):
        return ref.at[pl.ds(pl.multiple_of(tp * count, count), count)]

    loads = [
        pltpu.make_async_copy(heads(ref, groups), there, own_sem.at[5 + k])
        for k, (ref, there) in enumerate(
            (
                (rr_ref, rates.at[0]), (ri_ref, rates.at[1]), (inr_ref, matrices.at[0]),
                (ini_ref, matrices.at[1]), (outr_ref, matrices.at[2]), (outi_ref, matrices.at[3]),
            )
        )
    ]
    loads.append(pltpu.make_async_copy(heads(pw_ref, pool_groups), pool_own, own_sem.at[11]))
    for c in owns + loads:
        c.start()
    pl.semaphore_wait(barrier, n_sp - 1 + n_tp - 1)

    ways = (1, -1)

    def reach_of(a, d):
        return n_sp // 2 if a % 2 == d else n_sp - 1 - n_sp // 2

    def part(a, d, s, h):
        own, full = fulls[a]
        count = own.shape[0]
        size = count // PIECES
        way = ways[d]
        owner = place((at - way * s + n_sp) % n_sp)
        there = full.at[pl.ds(pl.multiple_of(owner * count + h * size, size), size)]
        source = own.at[pl.ds(h * size, size)] if s == 0 else there
        return source, there, (place((at + way + n_sp) % n_sp), tp)

    def sender(a, d, s, h):
        source, there, target = part(a, d, s, h)
        return pltpu.make_async_remote_copy(
            source, there, ring_send.at[a, d, s, h], ring_recv.at[a, d, s, h],
            device_id=target, device_id_type=MESH,
        )

    def arrive(a, d, s, h):
        _, there, target = part(a, d, s + 1, h)
        pltpu.make_async_remote_copy(
            there, there, ring_send.at[a, d, s, h], ring_recv.at[a, d, s, h],
            device_id=target, device_id_type=MESH,
        ).wait_recv()

    longest = n_sp // 2

    def ring(phase, s, h):
        streams = [
            (a, d) for a in (2 * phase, 2 * phase + 1) for d in range(2) if s < reach_of(a, d)
        ]
        for a, d in sorted(streams, key=lambda i: -reach_of(*i)):
            arrive(a, d, s, h)
            if s + 1 < reach_of(a, d):
                sender(a, d, s + 1, h).start()
        if phase == 0 and h == PIECES - 1:
            for a, d in streams:
                if s + 1 == reach_of(a, d):
                    for g in range(PIECES):
                        sender(a + 2, d, 0, g).start()

    turns = [(phase, s, h) for phase in range(2) for s in range(longest) for h in range(PIECES)]
    turn = [0]

    def step(stop=len(turns)):
        if turn[0] < stop:
            ring(*turns[turn[0]])
            turn[0] += 1

    def token_copy(k):
        return pltpu.make_async_remote_copy(
            tok_ref, tok_full.at[tp], tok_send.at[k - 1], tok_recv.at[k - 1],
            device_id=(me, (tp + k) % n_tp), device_id_type=MESH,
        )

    for h in range(PIECES):
        for a, d in ((0, 0), (1, 1), (0, 1), (1, 0)):
            sender(a, d, 0, h).start()
    for k in range(1, n_tp):
        token_copy(k).start()

    tile = iota((states, columns), 0) == iota((states, columns), 1) % states
    tile_exact, tile_half = tile.astype(f32), tile.astype(bf16)

    def exactly(a, b):
        return jnp.dot(a, b, precision=lax.Precision.HIGHEST, preferred_element_type=f32)

    factors = []

    def build_decay():
        for c in loads:
            c.wait()
        own_head = iota((groups, columns), 0) == iota((groups, columns), 1) // states

        def flat(a):
            return jnp.sum(jnp.where(own_head, exactly(a, tile_exact), 0.0), axis=0, keepdims=True)

        rate_real, rate_imag = flat(rates[0]), flat(rates[1])
        all_groups = step_ref.shape[1]
        head = iota((all_groups, columns), 0) == tp * groups + iota((all_groups, columns), 1) // states
        log_step = exactly(jnp.broadcast_to(step_ref[...], (8, all_groups)), head.astype(f32))[0:1]
        step_size = jnp.exp(log_step) / (rows * n_sp)
        exponent, angle = rate_real * step_size, rate_imag * step_size
        magnitude = jnp.exp(exponent)
        cosine = jnp.cos(angle)
        decay_real, decay_imag = magnitude * cosine, magnitude * jnp.sin(angle)
        series = jnp.ones_like(exponent)
        for k in range(10, 1, -1):
            series = 1.0 + series * exponent * (1.0 / k)
        growth = jnp.where(jnp.abs(exponent) < 0.5, exponent * series, magnitude - 1.0)
        less_one = growth * cosine - 2.0 * jnp.square(jnp.sin(0.5 * angle))
        denominator = rate_real * rate_real + rate_imag * rate_imag
        factors.append((less_one * rate_real + decay_imag * rate_imag) / denominator)
        factors.append((decay_imag * rate_real - less_one * rate_imag) / denominator)
        dec_ref[0:1, :] = decay_real
        dec_ref[1:2, :] = decay_imag

    def spread(k):
        high, low = split(matrices[k].reshape(width, states))
        return dot(high, tile_half) + dot(low, tile_half)

    def build_drive(i):
        same = iota((width, columns), 0) // SSM_GROUP == iota((width, columns), 1) // states
        real, imag = spread(0), spread(1)
        if i == 0:
            drive = factors[0] * real - factors[1] * imag
        else:
            drive = factors[0] * imag + factors[1] * real
        for j, piece in enumerate(split(jnp.where(same, drive, 0.0))):
            dmat[i, j] = piece

    def build_read(i):
        across = (iota((columns, states), 0) % states == iota((columns, states), 1)).astype(bf16)
        same = iota((columns, width), 0) // states == iota((columns, width), 1) // SSM_GROUP
        for j, piece in enumerate(split(matrices[2 + i].reshape(width, states))):
            rmat[i, j] = jnp.where(same, dot_nt(across, piece), 0.0).astype(bf16)

    def build_pool():
        across = (
            iota((POOL_GROUP, pool_width), 0) == iota((POOL_GROUP, pool_width), 1) % POOL_GROUP
        ).astype(bf16)
        same = iota((pool_width, pool_width), 0) // POOL_GROUP == iota((pool_width, pool_width), 1) // POOL_GROUP
        own = pool_own[...].reshape(pool_width, POOL_GROUP)
        pmat[...] = jnp.where(same, dot(own, across), 0.0).astype(bf16)

    squares = []

    def take(t):
        block = tok_full[t].astype(f32)
        squares.append(jnp.sum(block * block, axis=1, keepdims=True))
        cut = slice(t * features, (t + 1) * features)
        scaled[:, cut] = (block * gain_ref[:, cut]).astype(bf16)

    def tokens_in():
        owns[4].wait()
        for k in range(1, n_tp):
            pltpu.make_async_remote_copy(
                tok_ref, tok_full.at[(tp - k + n_tp) % n_tp], tok_send.at[k - 1], tok_recv.at[k - 1],
                device_id=(me, (tp + k) % n_tp), device_id_type=MESH,
            ).wait_recv()

    half = len(turns) // 2
    for at_work, work in enumerate(
        (
            build_decay, lambda: build_drive(0), lambda: build_drive(1), lambda: build_read(0),
            lambda: build_read(1), build_pool,
        )
    ):
        work()
        if at_work in (0, 1, 3, 5):
            step(half)
    while turn[0] < half - 3:
        step(half)
    tokens_in()
    for t in range(n_tp):
        take(t)
        if t == n_tp // 2 - 1:
            step(half)
    while turn[0] < half:
        step(half)
    owns[0].wait()
    owns[1].wait()
    inverse = lax.rsqrt(sum(squares) / (features * n_tp) + epsilon)
    state_in = (dot(scaled[...], wsi[...]) * inverse).astype(bf16)
    pool_in = (dot(scaled[...], wpi[...]) * inverse).astype(bf16)
    ext[window_reach:] = pool_in
    halo_out[...] = pool_in[rows - window_reach :]
    halo_copy = pltpu.make_async_remote_copy(
        halo_out, halo, halo_sem.at[0], halo_sem.at[1],
        device_id=((me + 1) % n_sp, tp), device_id_type=MESH,
    )
    shuffle = (
        iota((rows, rows), 1)
        == (iota((rows, rows), 0) % CHUNKS) * span + iota((rows, rows), 0) // CHUNKS
    ).astype(bf16)
    signal = dot(shuffle, state_in).astype(bf16)
    for i in range(2):
        push[i] = dot(signal, dmat[i, 0]) + dot(signal, dmat[i, 1])
        if i == 0:
            halo_copy.start()
        else:
            step()
    decay_real = jnp.broadcast_to(dec_ref[0:1, :], (CHUNKS, columns))
    decay_imag = jnp.broadcast_to(dec_ref[1:2, :], (CHUNKS, columns))

    def advance(p, carry):
        cut = pl.ds(pl.multiple_of(p * CHUNKS, CHUNKS), CHUNKS)
        real, imag = cmul(decay_real, decay_imag, *carry)
        real, imag = real + push[0, cut, :], imag + push[1, cut, :]
        push[0, cut, :] = real
        push[1, cut, :] = imag
        return real, imag

    zero = jnp.zeros((CHUNKS, columns), f32)
    end_real, end_imag = lax.fori_loop(0, span, advance, (zero, zero))

    def power(real, imag, count):
        out = None
        while count:
            if count % 2:
                out = (real, imag) if out is None else cmul(*out, real, imag)
            real, imag = cmul(real, imag, real, imag)
            count //= 2
        return out

    chunk_decay = power(dec_ref[0:1, :], dec_ref[1:2, :], span)
    block_decay = power(*chunk_decay, CHUNKS)
    row_zero = jnp.zeros((1, columns), f32)
    total = (row_zero, row_zero)
    for j in range(CHUNKS):
        moved = cmul(*chunk_decay, *total)
        total = (moved[0] + end_real[j : j + 1], moved[1] + end_imag[j : j + 1])
    which = iota((CHUNKS, columns), 0)
    ends[me] = jnp.where(which == 0, total[0], jnp.where(which == 1, total[1], 0.0))

    def end_copy(k):
        return pltpu.make_async_remote_copy(
            ends.at[me], ends.at[me], end_send.at[k - 1], end_recv.at[k - 1],
            device_id=((me + k) % n_sp, tp), device_id_type=MESH,
        )

    for k in range(1, n_sp):
        end_copy(k).start()

    halo_copy.wait_recv()
    ext[:window_reach] = jnp.where(me == 0, jnp.zeros_like(halo), halo[...])
    group = tp * (pool_width // POOL_GROUP) + iota((rows, pool_width), 1) // POOL_GROUP
    window = jnp.left_shift(jnp.ones_like(group), group % 4 + 1)
    targets = iota((rows, rows + window_reach), 0) + window_reach
    sources = iota((rows, rows + window_reach), 1)
    whole = ext[...]
    sums = jnp.zeros((rows, pool_width), f32)
    for power_index in range(1, 5):
        reach = 2**power_index
        band = ((sources <= targets) & (sources > targets - reach)).astype(bf16)
        sums = jnp.where(window == reach, dot(band, whole), sums)
        if power_index == 2:
            step()
    position = me * rows + iota((rows, pool_width), 0)
    divisor = jnp.minimum(position + 1, window).astype(f32)
    pooled = sums / divisor - ext[window_reach:].astype(f32)
    pooled_high, pooled_low = split(pooled)
    pool_gain = pg_ref[:, pl.ds(pl.multiple_of(tp * pool_width, pool_width), pool_width)]
    projected = dot(pooled_high, pmat[...]) + dot(pooled_low, pmat[...])
    mine_p[...] = (projected * pool_gain).astype(bf16)
    step()

    def act_copy(which, k, source):
        mine = mine_s if which == 0 else mine_p
        return pltpu.make_async_remote_copy(
            mine, act.at[which, source], act_send.at[which, k - 1], act_recv.at[which, k - 1],
            device_id=(me, (tp + k) % n_tp), device_id_type=MESH,
        )

    for k in range(1, n_tp):
        act_copy(1, k, tp).start()
    act[1, tp] = mine_p[...]

    for k in range(1, n_sp):
        there = ends.at[(me - k + n_sp) % n_sp]
        pltpu.make_async_remote_copy(
            there, there, end_send.at[k - 1], end_recv.at[k - 1],
            device_id=((me + k) % n_sp, tp), device_id_type=MESH,
        ).wait_recv()
    total = (row_zero, row_zero)
    for s in range(n_sp - 1):
        moved = cmul(*block_decay, *total)
        use = s < me
        total = (
            jnp.where(use, moved[0] + ends[s, 0:1, :], total[0]),
            jnp.where(use, moved[1] + ends[s, 1:2, :], total[1]),
        )
    begin_real, begin_imag = zero, zero
    for j in range(CHUNKS):
        begin_real = jnp.where(which == j, total[0], begin_real)
        begin_imag = jnp.where(which == j, total[1], begin_imag)
        moved = cmul(*chunk_decay, *total)
        total = (moved[0] + end_real[j : j + 1], moved[1] + end_imag[j : j + 1])

    def add_carry(p, carry):
        cut = pl.ds(pl.multiple_of(p * CHUNKS, CHUNKS), CHUNKS)
        real, imag = cmul(decay_real, decay_imag, *carry)
        push[0, cut, :] = push[0, cut, :] + real
        push[1, cut, :] = push[1, cut, :] + imag
        return real, imag

    lax.fori_loop(0, span, add_carry, (begin_real, begin_imag))
    step()
    real_high, real_low = split(push[0])
    imag_high, imag_low = split(push[1])
    readout = dot(real_high, rmat[0, 0]) + dot(real_high, rmat[0, 1]) + dot(real_low, rmat[0, 0])
    step()
    readout -= dot(imag_high, rmat[1, 0]) + dot(imag_high, rmat[1, 1]) + dot(imag_low, rmat[1, 0])
    skip = skip_ref[:, pl.ds(pl.multiple_of(tp * width, width), width)]
    readout += skip * signal.astype(f32)
    shuffled = jax.nn.gelu(readout).astype(bf16)
    restore = (
        iota((rows, rows), 0)
        == (iota((rows, rows), 1) % CHUNKS) * span + iota((rows, rows), 1) // CHUNKS
    ).astype(bf16)
    mine_s[...] = dot(restore, shuffled).astype(bf16)
    for k in range(1, n_tp):
        act_copy(0, k, tp).start()
    act[0, tp] = mine_s[...]
    while turn[0] < len(turns):
        step()
    for which in (1, 0):
        for k in range(1, n_tp):
            act_copy(which, k, (tp - k + n_tp) % n_tp).wait_recv()
    owns[2].wait()
    owns[3].wait()
    result = None
    for t in range(n_tp):
        for which, full, size in ((1, wpo, pool_width), (0, wso, width)):
            term = dot(act[which, t], full[t * size : (t + 1) * size, :])
            result = term if result is None else result + term
    out_ref[...] = result.astype(bf16)

    for a in range(4):
        for d in range(2):
            for s in range(reach_of(a, d)):
                for h in range(PIECES):
                    sender(a, d, s, h).wait_send()
    for k in range(1, n_tp):
        token_copy(k).wait_send()
        act_copy(0, k, tp).wait_send()
        act_copy(1, k, tp).wait_send()
    halo_copy.wait_send()
    for k in range(1, n_sp):
        end_copy(k).wait_send()

LANES = 128
HALVES = 2


def slab_kernel(
    n_sp, n_tp, n_x, states,
    tok_ref, gain_ref, wsi_ref, wpi_ref, rr_ref, ri_ref, step_ref, inr_ref, ini_ref, outr_ref,
    outi_ref, skip_ref, pw_ref, pg_ref, wso_ref, wpo_ref,
    out_ref,
    tok, scaled, squares, w_in, w_out, dmat, rmat, pmat, push, order, halo, halo_out, ends, act,
    guest, partial, sums, made, rates, matrices, pool_own, dec_ref,
    own_sem, xw_send, xw_recv, z_send, z_recv, tok_send, tok_recv, act_send, act_recv, halo_sem, end_send, end_recv,
    out_send, out_recv, guest_send, guest_recv, guest_z_send, guest_z_recv, part_send, part_recv,
):
    me, tp = lax.axis_index("sp"), lax.axis_index("tp")
    n_z = n_sp // n_x
    z, x = me // n_x, me % n_x
    y, core = tp // 2, tp % 2
    rows = tok_ref.shape[0]
    slab = rows * n_x
    features = tok_ref.shape[1]
    in_rows = wsi_ref.shape[0]
    out_rows = wso_ref.shape[0]
    width = wsi_ref.shape[1] // n_x
    out_width = wso_ref.shape[1] // n_x
    chunk_count = out_width // LANES
    groups = width // SSM_GROUP
    columns = groups * states
    pool_groups = width // POOL_GROUP
    span = slab // CHUNKS
    q = tp * n_x + x

    across, pair, both = (1 - y) * 2 + core, y * 2 + 1 - core, (1 - y) * 2 + 1 - core
    beside = me + 1 - 2 * x
    to_x, to_y, to_pair = (beside, tp), (me, across), (me, pair)
    ways = (1, -1)

    def to_z(way):
        return (me + way * n_x, tp)

    def inside(at):
        return jnp.logical_and(at >= 0, at < n_z)

    def inner(at):
        return jnp.logical_and(at > 0, at < n_z - 1)

    middle, rim = inner(z), jnp.logical_not(inner(z))
    inward, outward = jnp.where(z == 0, 1, -1), jnp.where(z == 1, -1, 1)

    def aligned(index, size):
        return pl.ds(pl.multiple_of(index * size, size), size)

    barrier = pltpu.get_barrier_semaphore()
    for there in (to_x, to_y, to_pair):
        pl.semaphore_signal(barrier, inc=1, device_id=there, device_id_type=MESH)
    for way in ways:
        @pl.when(inside(z + way))
        def _():
            pl.semaphore_signal(barrier, inc=1, device_id=to_z(way), device_id_type=MESH)

    def remote(source, there, send, recv, target):
        return pltpu.make_async_remote_copy(
            source, there, send, recv, device_id=target, device_id_type=MESH
        )

    def in_part(ref, half):
        return ref.at[:, aligned(half, width)]

    def out_part(ref, half, j):
        return ref.at[:, pl.ds(pl.multiple_of(half * out_width + j * LANES, LANES), LANES)]

    own_in, own_out = (wpi_ref, wsi_ref), (wso_ref, wpo_ref)

    def in_at(m, sp):
        return w_in.at[m, aligned(sp, in_rows)]

    def out_at(m, sp):
        return w_out.at[m, :, aligned(sp, out_rows)]

    def weight_at(k, sp):
        return in_at(k, sp) if k < 2 else out_at(k - 2, sp)

    def parts(k, half, sp):
        if k < 2:
            return [(in_part(own_in[k], half), in_at(k, sp))]
        return [
            (out_part(own_out[k - 2], half, j), w_out.at[k - 2, j, aligned(sp, out_rows)])
            for j in range(chunk_count)
        ]

    def own_copy(k):
        return [pltpu.make_async_copy(source, there, own_sem.at[k]) for source, there in parts(k, x, me)]

    def own_wait(k):
        here = weight_at(k, me)
        pltpu.make_async_copy(here, here, own_sem.at[k]).wait()

    base = 4
    tok_copy = pltpu.make_async_copy(tok_ref, tok.at[tp, aligned(x, rows)], own_sem.at[base])

    def heads(ref, count):
        return ref.at[aligned(q, count)]

    loads = [
        pltpu.make_async_copy(heads(ref, count), there, own_sem.at[base + 1 + k])
        for ref, count, there, k in (
            (rr_ref, groups, rates.at[0], 0), (ri_ref, groups, rates.at[1], 0),
            (inr_ref, groups, matrices.at[0], 1), (ini_ref, groups, matrices.at[1], 1),
            (outr_ref, groups, matrices.at[2], 1), (outi_ref, groups, matrices.at[3], 1),
            (pw_ref, pool_groups, pool_own, 2),
        )
    ]
    for c in own_copy(0) + [tok_copy] + loads + [c for k in range(1, base) for c in own_copy(k)]:
        c.start()

    def x_send(k):
        for source, there in parts(k, 1 - x, me):
            remote(source, there, xw_send.at[0], xw_recv.at[k], to_x).start()

    @jax.named_scope("across_wait")
    def x_wait(k):
        here = weight_at(k, beside)
        remote(here, here, xw_send.at[0], xw_recv.at[k], to_x).wait_recv()

    def z_part(stage, h, at):
        return weight_at(stage, at * n_x + (x if h == 0 else 1 - x))

    def reach(way, stage):
        return inside(z + way) if stage < 3 else inner(z + way)

    def z_copy(d, stage, s, h):
        at = z - ways[d] * s
        there = z_part(stage, h, at)
        return remote(there, there, z_send.at[d, s], z_recv.at[stage, at, h], to_z(ways[d]))

    def toward(way, stage, inner_side):
        there = z + way
        if inner_side:
            return inner(there)
        return jnp.logical_and(reach(way, stage), jnp.logical_not(inner(there)))

    def z_own(stage, h, *sides):
        for inner_side in sides:
            for d in range(2):
                @pl.when(toward(ways[d], stage, inner_side))
                def _():
                    z_copy(d, stage, 0, h).start()

    def z_arrive(d, stage, s, h):
        at = z - ways[d] * (s + 1)
        here = z_part(stage, h, at)
        remote(here, here, z_send.at[d, s], z_recv.at[stage, at, h], to_z(ways[d])).wait_recv()

    def z_relay(stage, s, h, inner_side, flows):
        for d in flows:
            @pl.when(jnp.logical_and(inside(z - ways[d] * (s + 1)), toward(ways[d], stage, inner_side)))
            def _():
                z_arrive(d, stage, s, h)
                z_copy(d, stage, s + 1, h).start()

    @jax.named_scope("relay_in")
    def relay_in(stage, h):
        z_relay(stage, 0, h, True, range(2))

    @jax.named_scope("relay_out")
    def relay_out(stage, s, h, flows=(0, 1)):
        z_relay(stage, s, h, False, flows)

    @jax.named_scope("final_wait")
    def z_final(stage):
        here = rim if stage < 3 else middle
        for d in range(2):
            for s in range(n_z - 1):
                stays = jnp.logical_and(here, jnp.logical_not(reach(ways[d], stage)))
                @pl.when(jnp.logical_and(inside(z - ways[d] * (s + 1)), stays))
                def _():
                    for h in range(2):
                        z_arrive(d, stage, s, h)

    class Gather:
        def __init__(self, region, pair_region, send, recv, turned):
            self.region, self.pair_region, self.send, self.recv = region, pair_region, send, recv
            self.turned = turned

        def copy(self, slot, p):
            at_tp, at_x = (
                (tp, x), (tp, x), (across, x) if p == self.turned else (tp, 1 - x), (tp, x), (tp, 1 - x), (across, x), (across, 1 - x)
            )[slot]
            here = self.region(at_tp, at_x, p)
            recv = self.recv.at[2 * slot + p if slot < 3 else 6 if slot < 5 else 7]
            target = (to_x, to_y, to_x if p == self.turned else to_y, to_pair, to_pair, to_pair, to_pair)[slot]
            return remote(here, here, self.send, recv, target)

        def start(self, *slots, p):
            for slot in slots:
                self.copy(slot, p).start()

        @jax.named_scope("gather_wait")
        def wait(self, slot, p):
            here = self.region(*((tp, 1 - x), (across, x), (across, 1 - x))[slot], p)
            remote(here, here, self.send, self.recv.at[2 * slot + p], to_pair).wait_recv()

        @jax.named_scope("pair_wait")
        def wait_pair(self, at_tp, k):
            here = self.pair_region(at_tp)
            remote(here, here, self.send, self.recv.at[6 + k], to_pair).wait_recv()

        def relay_x(self, p):
            self.wait(0, p)
            self.start(*((4,) if p == self.turned else (2, 4)), p=p)

        def relay_y(self, p):
            self.wait(1, p)
            self.start(*((2, 5) if p == self.turned else (5,)), p=p)

        def relay_both(self, p):
            self.wait(2, p)
            self.start(6, p=p)

        def drain(self, sent):
            remote(sent, sent, self.send, self.recv.at[0], to_pair).wait_send()

    piece = rows // HALVES

    def tok_region(at_tp, at_x, p):
        return tok.at[at_tp, pl.ds(pl.multiple_of(at_x * rows + p * piece, piece), piece)]

    tokens = Gather(tok_region, lambda at_tp: tok.at[at_tp], tok_send.at[0], tok_recv, None)

    half_slab = slab // HALVES

    def act_gather(buffer, send, recv):
        def region(at_tp, at_x, p):
            return buffer.at[pl.ds(p * half_slab, half_slab), aligned(at_tp * n_x + at_x, width)]

        return Gather(region, lambda at_tp: buffer.at[:, aligned(at_tp, n_x * width)], send, recv, 1)

    acts = [act_gather(act.at[k], act_send.at[k], act_recv.at[k]) for k in range(2)]
    guests = act_gather(guest, guest_send.at[0], guest_recv)

    def guest_copy(p):
        cut = (pl.ds(p * half_slab, half_slab), aligned(q, width))
        return remote(
            act.at[(1, *cut)], guest.at[cut], guest_z_send.at[0], guest_z_recv.at[p], to_z(inward)
        )

    def part_rows(j, first):
        return partial.at[j, aligned(1 - x if first else x, rows)]

    def part_copy(j, first):
        here = part_rows(j, first)
        return remote(here, here, part_send.at[0], part_recv.at[j, 0 if first else 1], to_z(outward))

    pl.semaphore_wait(barrier, 3 + inside(z + 1).astype(jnp.int32) + inside(z - 1).astype(jnp.int32))

    both_sides = (True, False)
    x_send(0)
    own_wait(0)
    z_own(0, 0, *both_sides)
    own_wait(1)
    z_own(1, 0, *both_sides)
    tok_copy.wait()
    for p in range(HALVES):
        tokens.start(0, 1, 3, p=p)
    x_send(1)

    tile = iota((states, columns), 0) == iota((states, columns), 1) % states
    tile_exact, tile_half = tile.astype(f32), tile.astype(bf16)

    def exactly(a, b):
        return jnp.dot(a, b, precision=lax.Precision.HIGHEST, preferred_element_type=f32)

    factors = []

    @jax.named_scope("build_decay")
    def build_decay():
        for c in loads:
            c.wait()
        own_head = iota((groups, columns), 0) == iota((groups, columns), 1) // states

        def flat(a):
            return jnp.sum(jnp.where(own_head, exactly(a, tile_exact), 0.0), axis=0, keepdims=True)

        rate_real, rate_imag = flat(rates[0]), flat(rates[1])
        all_groups = step_ref.shape[1]
        head = iota((all_groups, columns), 0) == q * groups + iota((all_groups, columns), 1) // states
        log_step = exactly(jnp.broadcast_to(step_ref[...], (8, all_groups)), head.astype(f32))[0:1]
        step_size = jnp.exp(log_step) / (rows * n_sp)
        exponent, angle = rate_real * step_size, rate_imag * step_size
        magnitude = jnp.exp(exponent)
        cosine = jnp.cos(angle)
        decay_real, decay_imag = magnitude * cosine, magnitude * jnp.sin(angle)
        series = jnp.ones_like(exponent)
        for k in range(10, 1, -1):
            series = 1.0 + series * exponent * (1.0 / k)
        growth = jnp.where(jnp.abs(exponent) < 0.5, exponent * series, magnitude - 1.0)
        less_one = growth * cosine - 2.0 * jnp.square(jnp.sin(0.5 * angle))
        denominator = rate_real * rate_real + rate_imag * rate_imag
        factors.append((less_one * rate_real + decay_imag * rate_imag) / denominator)
        factors.append((decay_imag * rate_real - less_one * rate_imag) / denominator)
        dec_ref[0:1, :] = decay_real
        dec_ref[1:2, :] = decay_imag

    def spread(k):
        high, low = split(matrices[k].reshape(width, states))
        return dot(high, tile_half) + dot(low, tile_half)

    @jax.named_scope("build_drive")
    def build_drive(i):
        same = iota((width, columns), 0) // SSM_GROUP == iota((width, columns), 1) // states
        real, imag = spread(0), spread(1)
        if i == 0:
            drive = factors[0] * real - factors[1] * imag
        else:
            drive = factors[0] * imag + factors[1] * real
        for j, part in enumerate(split(jnp.where(same, drive, 0.0))):
            dmat[i, j] = part

    @jax.named_scope("build_read")
    def build_read(i):
        onto = (iota((columns, states), 0) % states == iota((columns, states), 1)).astype(bf16)
        same = iota((columns, width), 0) // states == iota((columns, width), 1) // SSM_GROUP
        for j, part in enumerate(split(matrices[2 + i].reshape(width, states))):
            rmat[i, j] = jnp.where(same, dot_nt(onto, part), 0.0).astype(bf16)

    @jax.named_scope("build_pool")
    def build_pool():
        onto = (iota((POOL_GROUP, width), 0) == iota((POOL_GROUP, width), 1) % POOL_GROUP).astype(bf16)
        same = iota((width, width), 0) // POOL_GROUP == iota((width, width), 1) // POOL_GROUP
        own = pool_own[...].reshape(width, POOL_GROUP)
        pmat[...] = jnp.where(same, dot(own, onto), 0.0).astype(bf16)

    @jax.named_scope("build_order")
    def build_order(i):
        a, b = iota((slab, slab), i), iota((slab, slab), 1 - i)
        order[i] = (b == (a % CHUNKS) * span + a // CHUNKS).astype(bf16)

    @jax.named_scope("take")
    def take(at_tp, first):
        cut = pl.ds(pl.multiple_of(at_tp * features, features), features)
        gain = gain_ref[:, cut]
        size = min(64, slab)

        def step(i, _):
            here = pl.ds(pl.multiple_of(i * size, size), size)
            block = tok[at_tp, here].astype(f32)
            total = jnp.broadcast_to(jnp.sum(block * block, axis=1, keepdims=True), (size, LANES))
            squares[here] = total if first else squares[here] + total
            scaled[here, cut] = (block * gain).astype(bf16)
            return 0

        lax.fori_loop(0, slab // size, step, 0)

    build_decay()
    build_drive(0)
    relay_in(0, 0)
    relay_out(0, 0, 0)
    x_wait(0)
    z_own(0, 1, *both_sides)
    relay_in(1, 0)
    tokens.relay_y(0)
    build_drive(1)
    relay_out(0, 1, 0)
    build_read(0)
    relay_in(0, 1)
    relay_out(0, 0, 1)
    tokens.relay_x(0)
    tokens.relay_y(1)
    own_wait(2)
    own_wait(3)
    z_own(2, 0, True)
    build_read(1)
    relay_out(1, 0, 0)
    build_order(0)
    build_order(1)
    build_pool()
    relay_out(0, 1, 1)
    tokens.relay_x(1)
    x_wait(1)
    z_own(1, 1, *both_sides)
    x_send(2)
    x_send(3)
    z_own(3, 0, True)
    relay_out(1, 1, 0)
    take(tp, True)
    tokens.relay_both(0)
    tokens.wait_pair(pair, 0)
    take(pair, False)
    relay_in(1, 1)
    tokens.relay_both(1)
    relay_in(2, 0)
    take(across, False)
    relay_out(1, 0, 1)
    tokens.wait_pair(both, 1)
    take(both, False)
    relay_out(1, 1, 1, (1,))
    inverse = lax.rsqrt(squares[...] / (features * n_tp) + epsilon)
    z_final(0)
    pool_in = (dot(scaled[...], w_in[0]) * inverse).astype(bf16)
    halo_out[...] = pool_in[slab - window_reach :]
    halo_copy = remote(halo_out, halo, halo_sem.at[0], halo_sem.at[1], to_z(1))

    @pl.when(inside(z + 1))
    def _():
        halo_copy.start()

    relay_out(1, 1, 1, (0,))
    relay_in(3, 0)

    @pl.when(rim)
    def _():
        x_wait(2)
        z_own(2, 1, True)


    @pl.when(z > 0)
    @jax.named_scope("halo_wait")
    def _():
        halo_copy.wait_recv()

    before = jnp.where(z == 0, jnp.zeros_like(halo), halo[...])
    whole = jnp.concatenate([before, pool_in], axis=0).astype(f32)
    window = jnp.left_shift(2, (q * pool_groups + iota((slab, width), 1) // POOL_GROUP) % 4)
    window_sums = jnp.zeros((slab, width), f32)
    running = whole
    for level in range(4):
        running = running + pltpu.roll(running, 2**level, 0)
        window_sums = jnp.where(window == 2 ** (level + 1), running[window_reach:], window_sums)
    position = z * slab + iota((slab, width), 0)
    divisor = jnp.minimum(position + 1, window).astype(f32)
    pooled = window_sums / divisor - whole[window_reach:]
    pooled_high, pooled_low = split(pooled)
    pool_gain = pg_ref[:, aligned(q, width)]
    projected = dot(pooled_high, pmat[...]) + dot(pooled_low, pmat[...])
    act[1, :, aligned(q, width)] = (projected * pool_gain).astype(bf16)

    @pl.when(rim)
    def _():
        for p in range(HALVES):
            guest_copy(p).start()

    @pl.when(middle)
    def _():
        for p in range(HALVES):
            acts[1].start(0, 1, 3, p=p)

    z_own(2, 0, False)

    @pl.when(middle)
    def _():
        x_wait(2)
        z_own(2, 1, *both_sides)

    x_wait(3)
    z_own(3, 1, True)
    relay_out(2, 0, 0)
    z_final(1)
    state_in = (dot(scaled[...], w_in[1]) * inverse).astype(bf16)
    relay_in(2, 1)
    signal = dot(order[0], state_in).astype(bf16)
    for i in range(2):
        push[i] = dot(signal, dmat[i, 0]) + dot(signal, dmat[i, 1])
    decay_real = jnp.broadcast_to(dec_ref[0:1, :], (CHUNKS, columns))
    decay_imag = jnp.broadcast_to(dec_ref[1:2, :], (CHUNKS, columns))

    def advance(p, carry):
        cut = pl.ds(pl.multiple_of(p * CHUNKS, CHUNKS), CHUNKS)
        real, imag = cmul(decay_real, decay_imag, *carry)
        real, imag = real + push[0, cut, :], imag + push[1, cut, :]
        push[0, cut, :] = real
        push[1, cut, :] = imag
        return real, imag

    zero = jnp.zeros((CHUNKS, columns), f32)
    end_real, end_imag = lax.fori_loop(0, span, advance, (zero, zero), unroll=4)

    def power(real, imag, count):
        out = None
        while count:
            if count % 2:
                out = (real, imag) if out is None else cmul(*out, real, imag)
            real, imag = cmul(real, imag, real, imag)
            count //= 2
        return out

    chunk_decay = power(dec_ref[0:1, :], dec_ref[1:2, :], span)
    block_decay = power(*chunk_decay, CHUNKS)
    row_zero = jnp.zeros((1, columns), f32)
    total = (row_zero, row_zero)
    for j in range(CHUNKS):
        moved = cmul(*chunk_decay, *total)
        total = (moved[0] + end_real[j : j + 1], moved[1] + end_imag[j : j + 1])
    which = iota((CHUNKS, columns), 0)
    ends[z] = jnp.where(which == 0, total[0], jnp.where(which == 1, total[1], 0.0))

    def end_copy(k):
        return remote(ends.at[z], ends.at[z], end_send.at[k - 1], end_recv.at[k - 1], (me + k * n_x, tp))

    for k in range(1, n_z):
        @pl.when(inside(z + k))
        def _():
            end_copy(k).start()

    @pl.when(middle)
    def _():
        for p in range(HALVES):
            here = guests.region(tp, x, p)
            with jax.named_scope("guest_wait"):
                remote(here, here, guest_z_send.at[0], guest_z_recv.at[p], to_pair).wait_recv()
            guests.start(0, 1, 3, p=p)

    relay_out(2, 1, 0)
    relay_out(2, 0, 1)

    @pl.when(middle)
    def _():
        for p in range(HALVES):
            acts[1].relay_x(p)
            acts[1].relay_y(p)

    @pl.when(middle)
    def _():
        for p in range(HALVES):
            acts[1].relay_both(p)

    relay_in(3, 1)

    @pl.when(middle)
    def _():
        for p in range(HALVES):
            guests.relay_x(p)
            guests.relay_y(p)

    relay_out(2, 1, 1)

    for k in range(1, n_z):
        @pl.when(inside(z - k))
        @jax.named_scope("ends_wait")
        def _():
            there = ends.at[z - k]
            remote(there, there, end_send.at[k - 1], end_recv.at[k - 1], to_z(1)).wait_recv()

    total = (row_zero, row_zero)
    for s in range(n_z - 1):
        moved = cmul(*block_decay, *total)
        use = s < z
        total = (
            jnp.where(use, moved[0] + ends[s, 0:1, :], total[0]),
            jnp.where(use, moved[1] + ends[s, 1:2, :], total[1]),
        )
    begin_real, begin_imag = zero, zero
    for j in range(CHUNKS):
        begin_real = jnp.where(which == j, total[0], begin_real)
        begin_imag = jnp.where(which == j, total[1], begin_imag)
        moved = cmul(*chunk_decay, *total)
        total = (moved[0] + end_real[j : j + 1], moved[1] + end_imag[j : j + 1])

    def add_carry(p, carry):
        cut = pl.ds(pl.multiple_of(p * CHUNKS, CHUNKS), CHUNKS)
        real, imag = cmul(decay_real, decay_imag, *carry)
        push[0, cut, :] = push[0, cut, :] + real
        push[1, cut, :] = push[1, cut, :] + imag
        return real, imag

    lax.fori_loop(0, span, add_carry, (begin_real, begin_imag), unroll=4)
    real_high, real_low = split(push[0])
    imag_high, imag_low = split(push[1])
    readout = dot(real_high, rmat[0, 0]) + dot(real_high, rmat[0, 1]) + dot(real_low, rmat[0, 0])
    readout -= dot(imag_high, rmat[1, 0]) + dot(imag_high, rmat[1, 1]) + dot(imag_low, rmat[1, 0])
    skip = skip_ref[:, aligned(q, width)]
    readout += skip * signal.astype(f32)
    shuffled = jax.nn.gelu(readout).astype(bf16)
    act[0, :, aligned(q, width)] = dot(order[1], shuffled).astype(bf16)
    for p in range(HALVES):
        acts[0].start(0, 1, 3, p=p)

    @pl.when(middle)
    def _():
        for p in range(HALVES):
            guests.relay_both(p)
        guests.wait_pair(pair, 0)
        guests.wait_pair(both, 1)

    z_final(3)

    @pl.when(middle)
    def _():
        for first in (True, False):
            cut = aligned(1 - x if first else x, rows)
            for j in range(chunk_count):
                partial[j, cut] = dot(guest[cut], w_out[1, j]).astype(bf16)
                part_copy(j, first).start()

    for p in range(HALVES):
        acts[0].relay_x(p)
        acts[0].relay_y(p)
    for p in range(HALVES):
        acts[0].relay_both(p)

    @pl.when(middle)
    def _():
        acts[1].wait_pair(pair, 0)
        acts[1].wait_pair(both, 1)

    acts[0].wait_pair(pair, 0)
    acts[0].wait_pair(both, 1)
    z_final(2)

    def out_columns(half, j):
        return pl.ds(pl.multiple_of(half * out_width + j * LANES, LANES), LANES)

    def out_copy(j):
        return remote(made.at[j], out_ref.at[:, out_columns(x, j)], out_send.at[0], out_recv.at[0], to_x)

    here, there = aligned(x, rows), aligned(1 - x, rows)

    @pl.when(middle)
    def _():
        for j in range(chunk_count):
            made[j] = (dot(act[0, there], w_out[0, j]) + dot(act[1, there], w_out[1, j])).astype(bf16)
            out_copy(j).start()
        for j in range(chunk_count):
            mine = dot(act[0, here], w_out[0, j]) + dot(act[1, here], w_out[1, j])
            out_ref[:, out_columns(x, j)] = mine.astype(bf16)

    @pl.when(rim)
    def _():
        for cut in (there, here):
            for j in range(chunk_count):
                sums[j, cut] = dot(act[0, cut], w_out[0, j])

        @jax.named_scope("partial_wait")
        def part_wait(j, first):
            part = part_rows(j, first)
            recv = part_recv.at[j, 0 if first else 1]
            remote(part, part, part_send.at[0], recv, to_pair).wait_recv()

        for j in range(chunk_count):
            part_wait(j, True)
            made[j] = (sums[j, there] + partial[j, there].astype(f32)).astype(bf16)
            out_copy(j).start()
        for j in range(chunk_count):
            part_wait(j, False)
            out_ref[:, out_columns(x, j)] = (sums[j, here] + partial[j, here].astype(f32)).astype(bf16)

    @jax.named_scope("drain")
    def drain():
        sent = w_in.at[0, pl.ds(0, 2 * in_rows + 2 * chunk_count * out_rows)]
        remote(sent, sent, xw_send.at[0], xw_recv.at[0], to_x).wait_send()
        few = n_x * (2 * in_rows + chunk_count * out_rows)
        many = few + n_x * chunk_count * out_rows
        for d in range(2):
            for s in range(n_z - 1):
                any_sent = jnp.logical_and(inside(z + ways[d]), inside(z - ways[d] * s))
                for count, case in ((many, inner(z + ways[d])), (few, jnp.logical_not(inner(z + ways[d])))):
                    @pl.when(jnp.logical_and(any_sent, case))
                    def _():
                        sent = w_in.at[0, pl.ds(0, count)]
                        remote(sent, sent, z_send.at[d, s], z_recv.at[0, 0, 0], to_z(ways[d])).wait_send()
        tokens.drain(scaled.at[pl.ds(0, 7 * rows // n_tp)])
        acts[0].drain(act.at[0, :, pl.ds(0, 7 * width)])

        @pl.when(middle)
        def _():
            acts[1].drain(act.at[1, :, pl.ds(0, 7 * width)])
            guests.drain(guest.at[:, pl.ds(0, 7 * width)])
            remote(partial, partial, part_send.at[0], part_recv.at[0, 0], to_pair).wait_send()

        @pl.when(rim)
        def _():
            sent = act.at[1, :, aligned(q, width)]
            remote(sent, sent, guest_z_send.at[0], guest_z_recv.at[0], to_pair).wait_send()

        @pl.when(inside(z + 1))
        def _():
            halo_copy.wait_send()

        for k in range(1, n_z):
            @pl.when(inside(z + k))
            def _():
                end_copy(k).wait_send()

        remote(made, made, out_send.at[0], out_recv.at[0], to_x).wait_send()

    drain()
    with jax.named_scope("out_wait"):
        here = out_ref.at[:, aligned(1 - x, out_width)]
        remote(here, here, out_send.at[0], out_recv.at[0], to_x).wait_recv()


def slab_call(n_sp, n_tp, n_x, arrays):
    tokens, state_in_weight, state_out_weight = arrays[0], arrays[2], arrays[14]
    rows, features = tokens.shape
    in_rows, width = state_in_weight.shape
    out_rows, out_columns = state_out_weight.shape
    width //= n_x
    n_z, slab, chunk_count = n_sp // n_x, rows * n_x, out_columns // n_x // LANES
    groups, states = width // SSM_GROUP, arrays[4].shape[1]
    columns, pool_groups = groups * states, width // POOL_GROUP
    vmem = pl.BlockSpec(memory_space=pltpu.VMEM)
    anywhere = pl.BlockSpec(memory_space=pl.ANY)
    dma = pltpu.SemaphoreType.DMA
    return pl.pallas_call(
        functools.partial(slab_kernel, n_sp, n_tp, n_x, states),
        out_shape=pltpu.VMEM((rows, out_columns), bf16),
        in_specs=[anywhere, vmem] + [anywhere] * 4 + [vmem] + [anywhere] * 4 + [vmem, anywhere, vmem]
        + [anywhere] * 2,
        out_specs=vmem,
        scratch_shapes=[
            pltpu.VMEM((n_tp, slab, features), bf16),
            pltpu.VMEM((slab, features * n_tp), bf16),
            pltpu.VMEM((slab, LANES), f32),
            pltpu.VMEM((2, n_sp * in_rows, width), bf16),
            pltpu.VMEM((2, chunk_count, n_sp * out_rows, LANES), bf16),
            pltpu.VMEM((2, 2, width, columns), bf16),
            pltpu.VMEM((2, 2, columns, width), bf16),
            pltpu.VMEM((width, width), bf16),
            pltpu.VMEM((2, slab, columns), f32),
            pltpu.VMEM((2, slab, slab), bf16),
            pltpu.VMEM((window_reach, width), bf16),
            pltpu.VMEM((window_reach, width), bf16),
            pltpu.VMEM((n_z, CHUNKS, columns), f32),
            pltpu.VMEM((2, slab, n_tp * n_x * width), bf16),
            pltpu.VMEM((slab, n_tp * n_x * width), bf16),
            pltpu.VMEM((chunk_count, slab, LANES), bf16),
            pltpu.VMEM((chunk_count, slab, LANES), f32),
            pltpu.VMEM((chunk_count, rows, LANES), bf16),
            pltpu.VMEM((2, groups, states), f32),
            pltpu.VMEM((4, groups, SSM_GROUP, states), f32),
            pltpu.VMEM((pool_groups, POOL_GROUP, POOL_GROUP), bf16),
            pltpu.VMEM((2, columns), f32),
            dma((8,)),
            dma((1,)),
            dma((4,)),
            dma((2, n_z - 1)),
            dma((4, n_z, 2)),
            dma((1,)),
            dma((8,)),
            dma((2,)),
            dma((2, 8)),
            dma((2,)),
            dma((n_z - 1,)),
            dma((n_z - 1,)),
            dma((1,)),
            dma((1,)),
            dma((1,)),
            dma((8,)),
            dma((1,)),
            dma((HALVES,)),
            dma((1,)),
            dma((chunk_count, 2)),
        ],
        compiler_params=pltpu.CompilerParams(
            collective_id=0, has_side_effects=True, vmem_limit_bytes=60 * 2**20
        ),
    )(*arrays)


def slab_fits(n_sp, n_tp, n_x, in_rows, width, pool_width, out_rows, out_columns):
    return (
        n_x == 2 and n_tp == 4 and n_sp // n_x == 4 and width == n_x * LANES
        and pool_width == width and out_columns % (n_x * LANES) == 0
        and n_x * (2 * in_rows + out_columns // (n_x * LANES) * 2 * out_rows) <= n_sp * in_rows
    )


def body(
    n_sp, n_tp, n_x,
    tokens, norm_gain, state_in_weight, pool_in_weight, rate_real, rate_imag, log_step,
    input_real, input_imag, output_real, output_imag, skip_gain, pool_weight, pool_gain,
    state_out_weight, pool_out_weight,
):
    rows, features = tokens.shape
    in_rows, width = state_in_weight.shape
    pool_width = pool_in_weight.shape[1]
    out_rows, out_columns = state_out_weight.shape
    groups = width // SSM_GROUP
    states = rate_real.shape[1]
    columns = groups * states
    pool_groups = pool_width // POOL_GROUP
    if slab_fits(n_sp, n_tp, n_x, in_rows, width, pool_width, out_rows, out_columns):
        return slab_call(n_sp, n_tp, n_x, (
            tokens, norm_gain[None], state_in_weight, pool_in_weight, rate_real, rate_imag, log_step[None],
            jnp.swapaxes(input_real, 1, 2), jnp.swapaxes(input_imag, 1, 2), output_real, output_imag,
            skip_gain[None], pool_weight, pool_gain[None], state_out_weight, pool_out_weight,
        ))
    vmem = pl.BlockSpec(memory_space=pltpu.VMEM)
    anywhere = pl.BlockSpec(memory_space=pl.ANY)
    dma = pltpu.SemaphoreType.DMA
    return pl.pallas_call(
        functools.partial(kernel, n_sp, n_tp, n_x, states),
        out_shape=jax.ShapeDtypeStruct((rows, out_columns), bf16),
        in_specs=[anywhere, vmem] + [anywhere] * 4 + [vmem] + [anywhere] * 4 + [vmem, anywhere, vmem]
        + [anywhere] * 2,
        out_specs=vmem,
        scratch_shapes=[
            pltpu.VMEM((n_tp, rows, features), bf16),
            pltpu.VMEM((n_sp * in_rows, width), bf16),
            pltpu.VMEM((n_sp * in_rows, pool_width), bf16),
            pltpu.VMEM((n_sp * out_rows, out_columns), bf16),
            pltpu.VMEM((n_sp * out_rows, out_columns), bf16),
            pltpu.VMEM((rows, features * n_tp), bf16),
            pltpu.VMEM((2, 2, width, columns), bf16),
            pltpu.VMEM((2, 2, columns, width), bf16),
            pltpu.VMEM((pool_width, pool_width), bf16),
            pltpu.VMEM((2, rows, columns), f32),
            pltpu.VMEM((rows + window_reach, pool_width), bf16),
            pltpu.VMEM((window_reach, pool_width), bf16),
            pltpu.VMEM((n_sp, CHUNKS, columns), f32),
            pltpu.VMEM((2, n_tp, rows, width), bf16),
            pltpu.VMEM((rows, width), bf16),
            pltpu.VMEM((rows, pool_width), bf16),
            pltpu.VMEM((window_reach, pool_width), bf16),
            pltpu.VMEM((2, groups, states), f32),
            pltpu.VMEM((4, groups, SSM_GROUP, states), f32),
            pltpu.VMEM((pool_groups, POOL_GROUP, POOL_GROUP), bf16),
            pltpu.VMEM((2, columns), f32),
            dma((12,)),
            dma((4, 2, n_sp // 2, PIECES)),
            dma((4, 2, n_sp // 2, PIECES)),
            dma((n_tp - 1,)),
            dma((n_tp - 1,)),
            dma((2, n_tp - 1)),
            dma((2, n_tp - 1)),
            dma((2,)),
            dma((n_sp - 1,)),
            dma((n_sp - 1,)),
        ],
        compiler_params=pltpu.CompilerParams(
            collective_id=0, has_side_effects=True, vmem_limit_bytes=60 * 2**20
        ),
    )(
        tokens, norm_gain[None], state_in_weight, pool_in_weight, rate_real, rate_imag, log_step[None],
        jnp.swapaxes(input_real, 1, 2), jnp.swapaxes(input_imag, 1, 2), output_real, output_imag,
        skip_gain[None], pool_weight, pool_gain[None], state_out_weight, pool_out_weight,
    )


def solution(mesh):
    n_sp, n_tp = mesh.shape["sp"], mesh.shape["tp"]
    n_x = 2 ** ((n_sp.bit_length() - 1) // 2)
    both, whole = P("sp", "tp"), P()
    return jax.shard_map(
        functools.partial(body, n_sp, n_tp, n_x),
        mesh=mesh,
        in_specs=(both, whole, both, both) + (whole,) * 10 + (both, both),
        out_specs=both,
        check_vma=False,
    )
```

```python
import functools

import jax
import jax.numpy as jnp
from jax import lax
from jax.experimental import pallas as pl
from jax.experimental.pallas import tpu as pltpu
from jax.sharding import PartitionSpec as P

SSM_GROUP = 16
POOL_GROUP = 64
CHUNKS = 8
PIECES = 2

epsilon = 1e-06
window_reach = 16
f32, bf16 = jnp.float32, jnp.bfloat16
MESH = pl.DeviceIdType.MESH


def discretize(rate_real, rate_imag, log_step, length):
    step_size = jnp.exp(log_step)[:, None] / length
    exponent = rate_real * step_size
    angle = rate_imag * step_size
    magnitude = jnp.exp(exponent)
    decay_real = magnitude * jnp.cos(angle)
    decay_imag = magnitude * jnp.sin(angle)
    less_one = jnp.expm1(exponent) * jnp.cos(angle) - 2.0 * jnp.square(jnp.sin(0.5 * angle))
    denominator = rate_real * rate_real + rate_imag * rate_imag
    factor_real = (less_one * rate_real + decay_imag * rate_imag) / denominator
    factor_imag = (decay_imag * rate_real - less_one * rate_imag) / denominator
    return decay_real, decay_imag, factor_real, factor_imag


def iota(shape, axis):
    return lax.broadcasted_iota(jnp.int32, shape, axis)


def dot(a, b):
    return jnp.dot(a, b, preferred_element_type=f32)


def dot_nt(a, b):
    return lax.dot_general(a, b, (((1,), (1,)), ((), ())), preferred_element_type=f32)


def split(a):
    high = a.astype(bf16)
    return high, (a - high.astype(f32)).astype(bf16)


def cmul(ar, ai, br, bi):
    return ar * br - ai * bi, ar * bi + ai * br


def kernel(
    n_sp, n_tp, n_x, states,
    tok_ref, gain_ref, wsi_ref, wpi_ref, rr_ref, ri_ref, step_ref, inr_ref, ini_ref, outr_ref,
    outi_ref, skip_ref, pw_ref, pg_ref, wso_ref, wpo_ref,
    out_ref,
    tok_full, wsi, wpi, wso, wpo, scaled, dmat, rmat, pmat, push, ext, halo, ends, act,
    mine_s, mine_p, halo_out, rates, matrices, pool_own, dec_ref,
    own_sem, ring_send, ring_recv, tok_send, tok_recv, act_send, act_recv, halo_sem, end_send, end_recv,
):
    me, tp = lax.axis_index("sp"), lax.axis_index("tp")
    n_z = n_sp // n_x
    rows = tok_ref.shape[0]
    features = tok_ref.shape[1]
    width = wsi_ref.shape[1]
    pool_width = wpi_ref.shape[1]
    groups = width // SSM_GROUP
    columns = groups * states
    pool_groups = pool_width // POOL_GROUP
    span = rows // CHUNKS

    def place(p):
        x, r = p // n_z, p % n_z
        return (r + (x % 2) * (n_z - 1 - 2 * r)) * n_x + x

    my_x, my_z = me % n_x, me // n_x
    at = my_x * n_z + my_z + (my_x % 2) * (n_z - 1 - 2 * my_z)

    barrier = pltpu.get_barrier_semaphore()
    for k in range(1, n_sp):
        pl.semaphore_signal(barrier, inc=1, device_id=((me + k) % n_sp, tp), device_id_type=MESH)
    for k in range(1, n_tp):
        pl.semaphore_signal(barrier, inc=1, device_id=(me, (tp + k) % n_tp), device_id_type=MESH)

    fulls = ((wsi_ref, wsi), (wpi_ref, wpi), (wso_ref, wso), (wpo_ref, wpo))
    owns = []
    for a, (own, full) in enumerate(fulls):
        count = own.shape[0]
        owns.append(
            pltpu.make_async_copy(
                own, full.at[pl.ds(pl.multiple_of(me * count, count), count)], own_sem.at[a]
            )
        )
    owns.append(pltpu.make_async_copy(tok_ref, tok_full.at[tp], own_sem.at[4]))
    def heads(ref, count):
        return ref.at[pl.ds(pl.multiple_of(tp * count, count), count)]

    loads = [
        pltpu.make_async_copy(heads(ref, groups), there, own_sem.at[5 + k])
        for k, (ref, there) in enumerate(
            (
                (rr_ref, rates.at[0]), (ri_ref, rates.at[1]), (inr_ref, matrices.at[0]),
                (ini_ref, matrices.at[1]), (outr_ref, matrices.at[2]), (outi_ref, matrices.at[3]),
            )
        )
    ]
    loads.append(pltpu.make_async_copy(heads(pw_ref, pool_groups), pool_own, own_sem.at[11]))
    for c in owns + loads:
        c.start()
    pl.semaphore_wait(barrier, n_sp - 1 + n_tp - 1)

    ways = (1, -1)

    def reach_of(a, d):
        return n_sp // 2 if a % 2 == d else n_sp - 1 - n_sp // 2

    def part(a, d, s, h):
        own, full = fulls[a]
        count = own.shape[0]
        size = count // PIECES
        way = ways[d]
        owner = place((at - way * s + n_sp) % n_sp)
        there = full.at[pl.ds(pl.multiple_of(owner * count + h * size, size), size)]
        source = own.at[pl.ds(h * size, size)] if s == 0 else there
        return source, there, (place((at + way + n_sp) % n_sp), tp)

    def sender(a, d, s, h):
        source, there, target = part(a, d, s, h)
        return pltpu.make_async_remote_copy(
            source, there, ring_send.at[a, d, s, h], ring_recv.at[a, d, s, h],
            device_id=target, device_id_type=MESH,
        )

    def arrive(a, d, s, h):
        _, there, target = part(a, d, s + 1, h)
        pltpu.make_async_remote_copy(
            there, there, ring_send.at[a, d, s, h], ring_recv.at[a, d, s, h],
            device_id=target, device_id_type=MESH,
        ).wait_recv()

    longest = n_sp // 2

    def ring(phase, s, h):
        streams = [
            (a, d) for a in (2 * phase, 2 * phase + 1) for d in range(2) if s < reach_of(a, d)
        ]
        for a, d in sorted(streams, key=lambda i: -reach_of(*i)):
            arrive(a, d, s, h)
            if s + 1 < reach_of(a, d):
                sender(a, d, s + 1, h).start()
        if phase == 0 and h == PIECES - 1:
            for a, d in streams:
                if s + 1 == reach_of(a, d):
                    for g in range(PIECES):
                        sender(a + 2, d, 0, g).start()

    turns = [(phase, s, h) for phase in range(2) for s in range(longest) for h in range(PIECES)]
    turn = [0]

    def step(stop=len(turns)):
        if turn[0] < stop:
            ring(*turns[turn[0]])
            turn[0] += 1

    def token_copy(k):
        return pltpu.make_async_remote_copy(
            tok_ref, tok_full.at[tp], tok_send.at[k - 1], tok_recv.at[k - 1],
            device_id=(me, (tp + k) % n_tp), device_id_type=MESH,
        )

    for h in range(PIECES):
        for a, d in ((0, 0), (1, 1), (0, 1), (1, 0)):
            sender(a, d, 0, h).start()
    for k in range(1, n_tp):
        token_copy(k).start()

    tile = iota((states, columns), 0) == iota((states, columns), 1) % states
    tile_exact, tile_half = tile.astype(f32), tile.astype(bf16)

    def exactly(a, b):
        return jnp.dot(a, b, precision=lax.Precision.HIGHEST, preferred_element_type=f32)

    factors = []

    def build_decay():
        for c in loads:
            c.wait()
        own_head = iota((groups, columns), 0) == iota((groups, columns), 1) // states

        def flat(a):
            return jnp.sum(jnp.where(own_head, exactly(a, tile_exact), 0.0), axis=0, keepdims=True)

        rate_real, rate_imag = flat(rates[0]), flat(rates[1])
        all_groups = step_ref.shape[1]
        head = iota((all_groups, columns), 0) == tp * groups + iota((all_groups, columns), 1) // states
        log_step = exactly(jnp.broadcast_to(step_ref[...], (8, all_groups)), head.astype(f32))[0:1]
        step_size = jnp.exp(log_step) / (rows * n_sp)
        exponent, angle = rate_real * step_size, rate_imag * step_size
        magnitude = jnp.exp(exponent)
        cosine = jnp.cos(angle)
        decay_real, decay_imag = magnitude * cosine, magnitude * jnp.sin(angle)
        series = jnp.ones_like(exponent)
        for k in range(10, 1, -1):
            series = 1.0 + series * exponent * (1.0 / k)
        growth = jnp.where(jnp.abs(exponent) < 0.5, exponent * series, magnitude - 1.0)
        less_one = growth * cosine - 2.0 * jnp.square(jnp.sin(0.5 * angle))
        denominator = rate_real * rate_real + rate_imag * rate_imag
        factors.append((less_one * rate_real + decay_imag * rate_imag) / denominator)
        factors.append((decay_imag * rate_real - less_one * rate_imag) / denominator)
        dec_ref[0:1, :] = decay_real
        dec_ref[1:2, :] = decay_imag

    def spread(k):
        high, low = split(matrices[k].reshape(width, states))
        return dot(high, tile_half) + dot(low, tile_half)

    def build_drive(i):
        same = iota((width, columns), 0) // SSM_GROUP == iota((width, columns), 1) // states
        real, imag = spread(0), spread(1)
        if i == 0:
            drive = factors[0] * real - factors[1] * imag
        else:
            drive = factors[0] * imag + factors[1] * real
        for j, piece in enumerate(split(jnp.where(same, drive, 0.0))):
            dmat[i, j] = piece

    def build_read(i):
        across = (iota((columns, states), 0) % states == iota((columns, states), 1)).astype(bf16)
        same = iota((columns, width), 0) // states == iota((columns, width), 1) // SSM_GROUP
        for j, piece in enumerate(split(matrices[2 + i].reshape(width, states))):
            rmat[i, j] = jnp.where(same, dot_nt(across, piece), 0.0).astype(bf16)

    def build_pool():
        across = (
            iota((POOL_GROUP, pool_width), 0) == iota((POOL_GROUP, pool_width), 1) % POOL_GROUP
        ).astype(bf16)
        same = iota((pool_width, pool_width), 0) // POOL_GROUP == iota((pool_width, pool_width), 1) // POOL_GROUP
        own = pool_own[...].reshape(pool_width, POOL_GROUP)
        pmat[...] = jnp.where(same, dot(own, across), 0.0).astype(bf16)

    squares = []

    def take(t):
        block = tok_full[t].astype(f32)
        squares.append(jnp.sum(block * block, axis=1, keepdims=True))
        cut = slice(t * features, (t + 1) * features)
        scaled[:, cut] = (block * gain_ref[:, cut]).astype(bf16)

    def tokens_in():
        owns[4].wait()
        for k in range(1, n_tp):
            pltpu.make_async_remote_copy(
                tok_ref, tok_full.at[(tp - k + n_tp) % n_tp], tok_send.at[k - 1], tok_recv.at[k - 1],
                device_id=(me, (tp + k) % n_tp), device_id_type=MESH,
            ).wait_recv()

    half = len(turns) // 2
    for at_work, work in enumerate(
        (
            build_decay, lambda: build_drive(0), lambda: build_drive(1), lambda: build_read(0),
            lambda: build_read(1), build_pool,
        )
    ):
        work()
        if at_work in (0, 1, 3, 5):
            step(half)
    while turn[0] < half - 3:
        step(half)
    tokens_in()
    for t in range(n_tp):
        take(t)
        if t == n_tp // 2 - 1:
            step(half)
    while turn[0] < half:
        step(half)
    owns[0].wait()
    owns[1].wait()
    inverse = lax.rsqrt(sum(squares) / (features * n_tp) + epsilon)
    state_in = (dot(scaled[...], wsi[...]) * inverse).astype(bf16)
    pool_in = (dot(scaled[...], wpi[...]) * inverse).astype(bf16)
    ext[window_reach:] = pool_in
    halo_out[...] = pool_in[rows - window_reach :]
    halo_copy = pltpu.make_async_remote_copy(
        halo_out, halo, halo_sem.at[0], halo_sem.at[1],
        device_id=((me + 1) % n_sp, tp), device_id_type=MESH,
    )
    shuffle = (
        iota((rows, rows), 1)
        == (iota((rows, rows), 0) % CHUNKS) * span + iota((rows, rows), 0) // CHUNKS
    ).astype(bf16)
    signal = dot(shuffle, state_in).astype(bf16)
    for i in range(2):
        push[i] = dot(signal, dmat[i, 0]) + dot(signal, dmat[i, 1])
        if i == 0:
            halo_copy.start()
        else:
            step()
    decay_real = jnp.broadcast_to(dec_ref[0:1, :], (CHUNKS, columns))
    decay_imag = jnp.broadcast_to(dec_ref[1:2, :], (CHUNKS, columns))

    def advance(p, carry):
        cut = pl.ds(pl.multiple_of(p * CHUNKS, CHUNKS), CHUNKS)
        real, imag = cmul(decay_real, decay_imag, *carry)
        real, imag = real + push[0, cut, :], imag + push[1, cut, :]
        push[0, cut, :] = real
        push[1, cut, :] = imag
        return real, imag

    zero = jnp.zeros((CHUNKS, columns), f32)
    end_real, end_imag = lax.fori_loop(0, span, advance, (zero, zero))

    def power(real, imag, count):
        out = None
        while count:
            if count % 2:
                out = (real, imag) if out is None else cmul(*out, real, imag)
            real, imag = cmul(real, imag, real, imag)
            count //= 2
        return out

    chunk_decay = power(dec_ref[0:1, :], dec_ref[1:2, :], span)
    block_decay = power(*chunk_decay, CHUNKS)
    row_zero = jnp.zeros((1, columns), f32)
    total = (row_zero, row_zero)
    for j in range(CHUNKS):
        moved = cmul(*chunk_decay, *total)
        total = (moved[0] + end_real[j : j + 1], moved[1] + end_imag[j : j + 1])
    which = iota((CHUNKS, columns), 0)
    ends[me] = jnp.where(which == 0, total[0], jnp.where(which == 1, total[1], 0.0))

    def end_copy(k):
        return pltpu.make_async_remote_copy(
            ends.at[me], ends.at[me], end_send.at[k - 1], end_recv.at[k - 1],
            device_id=((me + k) % n_sp, tp), device_id_type=MESH,
        )

    for k in range(1, n_sp):
        end_copy(k).start()

    halo_copy.wait_recv()
    ext[:window_reach] = jnp.where(me == 0, jnp.zeros_like(halo), halo[...])
    group = tp * (pool_width // POOL_GROUP) + iota((rows, pool_width), 1) // POOL_GROUP
    window = jnp.left_shift(jnp.ones_like(group), group % 4 + 1)
    targets = iota((rows, rows + window_reach), 0) + window_reach
    sources = iota((rows, rows + window_reach), 1)
    whole = ext[...]
    sums = jnp.zeros((rows, pool_width), f32)
    for power_index in range(1, 5):
        reach = 2**power_index
        band = ((sources <= targets) & (sources > targets - reach)).astype(bf16)
        sums = jnp.where(window == reach, dot(band, whole), sums)
        if power_index == 2:
            step()
    position = me * rows + iota((rows, pool_width), 0)
    divisor = jnp.minimum(position + 1, window).astype(f32)
    pooled = sums / divisor - ext[window_reach:].astype(f32)
    pooled_high, pooled_low = split(pooled)
    pool_gain = pg_ref[:, pl.ds(pl.multiple_of(tp * pool_width, pool_width), pool_width)]
    projected = dot(pooled_high, pmat[...]) + dot(pooled_low, pmat[...])
    mine_p[...] = (projected * pool_gain).astype(bf16)
    step()

    def act_copy(which, k, source):
        mine = mine_s if which == 0 else mine_p
        return pltpu.make_async_remote_copy(
            mine, act.at[which, source], act_send.at[which, k - 1], act_recv.at[which, k - 1],
            device_id=(me, (tp + k) % n_tp), device_id_type=MESH,
        )

    for k in range(1, n_tp):
        act_copy(1, k, tp).start()
    act[1, tp] = mine_p[...]

    for k in range(1, n_sp):
        there = ends.at[(me - k + n_sp) % n_sp]
        pltpu.make_async_remote_copy(
            there, there, end_send.at[k - 1], end_recv.at[k - 1],
            device_id=((me + k) % n_sp, tp), device_id_type=MESH,
        ).wait_recv()
    total = (row_zero, row_zero)
    for s in range(n_sp - 1):
        moved = cmul(*block_decay, *total)
        use = s < me
        total = (
            jnp.where(use, moved[0] + ends[s, 0:1, :], total[0]),
            jnp.where(use, moved[1] + ends[s, 1:2, :], total[1]),
        )
    begin_real, begin_imag = zero, zero
    for j in range(CHUNKS):
        begin_real = jnp.where(which == j, total[0], begin_real)
        begin_imag = jnp.where(which == j, total[1], begin_imag)
        moved = cmul(*chunk_decay, *total)
        total = (moved[0] + end_real[j : j + 1], moved[1] + end_imag[j : j + 1])

    def add_carry(p, carry):
        cut = pl.ds(pl.multiple_of(p * CHUNKS, CHUNKS), CHUNKS)
        real, imag = cmul(decay_real, decay_imag, *carry)
        push[0, cut, :] = push[0, cut, :] + real
        push[1, cut, :] = push[1, cut, :] + imag
        return real, imag

    lax.fori_loop(0, span, add_carry, (begin_real, begin_imag))
    step()
    real_high, real_low = split(push[0])
    imag_high, imag_low = split(push[1])
    readout = dot(real_high, rmat[0, 0]) + dot(real_high, rmat[0, 1]) + dot(real_low, rmat[0, 0])
    step()
    readout -= dot(imag_high, rmat[1, 0]) + dot(imag_high, rmat[1, 1]) + dot(imag_low, rmat[1, 0])
    skip = skip_ref[:, pl.ds(pl.multiple_of(tp * width, width), width)]
    readout += skip * signal.astype(f32)
    shuffled = jax.nn.gelu(readout).astype(bf16)
    restore = (
        iota((rows, rows), 0)
        == (iota((rows, rows), 1) % CHUNKS) * span + iota((rows, rows), 1) // CHUNKS
    ).astype(bf16)
    mine_s[...] = dot(restore, shuffled).astype(bf16)
    for k in range(1, n_tp):
        act_copy(0, k, tp).start()
    act[0, tp] = mine_s[...]
    while turn[0] < len(turns):
        step()
    for which in (1, 0):
        for k in range(1, n_tp):
            act_copy(which, k, (tp - k + n_tp) % n_tp).wait_recv()
    owns[2].wait()
    owns[3].wait()
    result = None
    for t in range(n_tp):
        for which, full, size in ((1, wpo, pool_width), (0, wso, width)):
            term = dot(act[which, t], full[t * size : (t + 1) * size, :])
            result = term if result is None else result + term
    out_ref[...] = result.astype(bf16)

    for a in range(4):
        for d in range(2):
            for s in range(reach_of(a, d)):
                for h in range(PIECES):
                    sender(a, d, s, h).wait_send()
    for k in range(1, n_tp):
        token_copy(k).wait_send()
        act_copy(0, k, tp).wait_send()
        act_copy(1, k, tp).wait_send()
    halo_copy.wait_send()
    for k in range(1, n_sp):
        end_copy(k).wait_send()

LANES = 128
HALVES = 2


def slab_kernel(
    n_sp, n_tp, n_x, states,
    tok_ref, gain_ref, wsi_ref, wpi_ref, rr_ref, ri_ref, step_ref, inr_ref, ini_ref, outr_ref,
    outi_ref, skip_ref, pw_ref, pg_ref, wso_ref, wpo_ref,
    out_ref,
    tok, scaled, squares, w_in, w_out, dmat, rmat, pmat, push, order, halo, halo_out, ends, act,
    guest, partial, sums, made, rates, matrices, pool_own, dec_ref,
    own_sem, xw_send, xw_recv, z_send, z_recv, tok_send, tok_recv, act_send, act_recv, halo_sem, end_send, end_recv,
    out_send, out_recv, guest_send, guest_recv, guest_z_send, guest_z_recv, part_send, part_recv,
):
    me, tp = lax.axis_index("sp"), lax.axis_index("tp")
    n_z = n_sp // n_x
    z, x = me // n_x, me % n_x
    y, core = tp // 2, tp % 2
    rows = tok_ref.shape[0]
    slab = rows * n_x
    features = tok_ref.shape[1]
    in_rows = wsi_ref.shape[0]
    out_rows = wso_ref.shape[0]
    width = wsi_ref.shape[1] // n_x
    out_width = wso_ref.shape[1] // n_x
    chunk_count = out_width // LANES
    groups = width // SSM_GROUP
    columns = groups * states
    pool_groups = width // POOL_GROUP
    span = slab // CHUNKS
    q = tp * n_x + x

    across, pair, both = (1 - y) * 2 + core, y * 2 + 1 - core, (1 - y) * 2 + 1 - core
    beside = me + 1 - 2 * x
    to_x, to_y, to_pair = (beside, tp), (me, across), (me, pair)
    ways = (1, -1)

    def to_z(way):
        return (me + way * n_x, tp)

    def inside(at):
        return jnp.logical_and(at >= 0, at < n_z)

    def inner(at):
        return jnp.logical_and(at > 0, at < n_z - 1)

    middle, rim = inner(z), jnp.logical_not(inner(z))
    inward, outward = jnp.where(z == 0, 1, -1), jnp.where(z == 1, -1, 1)

    def aligned(index, size):
        return pl.ds(pl.multiple_of(index * size, size), size)

    barrier = pltpu.get_barrier_semaphore()
    for there in (to_x, to_y, to_pair):
        pl.semaphore_signal(barrier, inc=1, device_id=there, device_id_type=MESH)
    for way in ways:
        @pl.when(inside(z + way))
        def _():
            pl.semaphore_signal(barrier, inc=1, device_id=to_z(way), device_id_type=MESH)

    def remote(source, there, send, recv, target):
        return pltpu.make_async_remote_copy(
            source, there, send, recv, device_id=target, device_id_type=MESH
        )

    def in_part(ref, half):
        return ref.at[:, aligned(half, width)]

    def out_part(ref, half, j):
        return ref.at[:, pl.ds(pl.multiple_of(half * out_width + j * LANES, LANES), LANES)]

    own_in, own_out = (wpi_ref, wsi_ref), (wso_ref, wpo_ref)

    def in_at(m, sp):
        return w_in.at[m, aligned(sp, in_rows)]

    def out_at(m, sp):
        return w_out.at[m, :, aligned(sp, out_rows)]

    def weight_at(k, sp):
        return in_at(k, sp) if k < 2 else out_at(k - 2, sp)

    def parts(k, half, sp):
        if k < 2:
            return [(in_part(own_in[k], half), in_at(k, sp))]
        return [
            (out_part(own_out[k - 2], half, j), w_out.at[k - 2, j, aligned(sp, out_rows)])
            for j in range(chunk_count)
        ]

    def own_copy(k):
        return [pltpu.make_async_copy(source, there, own_sem.at[k]) for source, there in parts(k, x, me)]

    def own_wait(k):
        here = weight_at(k, me)
        pltpu.make_async_copy(here, here, own_sem.at[k]).wait()

    base = 4
    tok_copy = pltpu.make_async_copy(tok_ref, tok.at[tp, aligned(x, rows)], own_sem.at[base])

    def heads(ref, count):
        return ref.at[aligned(q, count)]

    loads = [
        pltpu.make_async_copy(heads(ref, count), there, own_sem.at[base + 1 + k])
        for ref, count, there, k in (
            (rr_ref, groups, rates.at[0], 0), (ri_ref, groups, rates.at[1], 0),
            (inr_ref, groups, matrices.at[0], 1), (ini_ref, groups, matrices.at[1], 1),
            (outr_ref, groups, matrices.at[2], 1), (outi_ref, groups, matrices.at[3], 1),
            (pw_ref, pool_groups, pool_own, 2),
        )
    ]
    for c in own_copy(0) + [tok_copy] + loads + [c for k in range(1, base) for c in own_copy(k)]:
        c.start()

    def x_send(k):
        for source, there in parts(k, 1 - x, me):
            remote(source, there, xw_send.at[0], xw_recv.at[k], to_x).start()

    @jax.named_scope("across_wait")
    def x_wait(k):
        here = weight_at(k, beside)
        remote(here, here, xw_send.at[0], xw_recv.at[k], to_x).wait_recv()

    def z_part(stage, h, at):
        return weight_at(stage, at * n_x + (x if h == 0 else 1 - x))

    def reach(way, stage):
        return inside(z + way) if stage < 3 else inner(z + way)

    def z_copy(d, stage, s, h):
        at = z - ways[d] * s
        there = z_part(stage, h, at)
        return remote(there, there, z_send.at[d, s], z_recv.at[stage, at, h], to_z(ways[d]))

    def toward(way, stage, inner_side):
        there = z + way
        if inner_side:
            return inner(there)
        return jnp.logical_and(reach(way, stage), jnp.logical_not(inner(there)))

    def z_own(stage, h, *sides, flows=(0, 1)):
        for inner_side in sides:
            for d in flows:
                @pl.when(toward(ways[d], stage, inner_side))
                def _():
                    z_copy(d, stage, 0, h).start()

    def z_arrive(d, stage, s, h):
        at = z - ways[d] * (s + 1)
        here = z_part(stage, h, at)
        remote(here, here, z_send.at[d, s], z_recv.at[stage, at, h], to_z(ways[d])).wait_recv()

    def z_relay(stage, s, h, inner_side, flows):
        for d in flows:
            @pl.when(jnp.logical_and(inside(z - ways[d] * (s + 1)), toward(ways[d], stage, inner_side)))
            def _():
                z_arrive(d, stage, s, h)
                z_copy(d, stage, s + 1, h).start()

    @jax.named_scope("relay_in")
    def relay_in(stage, h, flows=(0, 1)):
        z_relay(stage, 0, h, True, flows)

    @jax.named_scope("relay_out")
    def relay_out(stage, s, h, flows=(0, 1)):
        z_relay(stage, s, h, False, flows)

    @jax.named_scope("final_wait")
    def z_final(stage):
        here = rim if stage < 3 else middle
        for d in range(2):
            for s in range(n_z - 1):
                stays = jnp.logical_and(here, jnp.logical_not(reach(ways[d], stage)))
                @pl.when(jnp.logical_and(inside(z - ways[d] * (s + 1)), stays))
                def _():
                    for h in range(2):
                        z_arrive(d, stage, s, h)

    class Gather:
        def __init__(self, region, pair_region, send, recv, turned):
            self.region, self.pair_region, self.send, self.recv = region, pair_region, send, recv
            self.turned = turned

        def copy(self, slot, p):
            at_tp, at_x = (
                (tp, x), (tp, x), (across, x) if p == self.turned else (tp, 1 - x), (tp, x), (tp, 1 - x), (across, x), (across, 1 - x)
            )[slot]
            here = self.region(at_tp, at_x, p)
            recv = self.recv.at[2 * slot + p if slot < 3 else 6 if slot < 5 else 7]
            target = (to_x, to_y, to_x if p == self.turned else to_y, to_pair, to_pair, to_pair, to_pair)[slot]
            return remote(here, here, self.send, recv, target)

        def start(self, *slots, p):
            for slot in slots:
                self.copy(slot, p).start()

        @jax.named_scope("gather_wait")
        def wait(self, slot, p):
            here = self.region(*((tp, 1 - x), (across, x), (across, 1 - x))[slot], p)
            remote(here, here, self.send, self.recv.at[2 * slot + p], to_pair).wait_recv()

        @jax.named_scope("pair_wait")
        def wait_pair(self, at_tp, k):
            here = self.pair_region(at_tp)
            remote(here, here, self.send, self.recv.at[6 + k], to_pair).wait_recv()

        def relay_x(self, p):
            self.wait(0, p)
            self.start(*((4,) if p == self.turned else (2, 4)), p=p)

        def relay_y(self, p):
            self.wait(1, p)
            self.start(*((2, 5) if p == self.turned else (5,)), p=p)

        def relay_both(self, p):
            self.wait(2, p)
            self.start(6, p=p)

        def drain(self, sent):
            remote(sent, sent, self.send, self.recv.at[0], to_pair).wait_send()

    piece = rows // HALVES

    def tok_region(at_tp, at_x, p):
        return tok.at[at_tp, pl.ds(pl.multiple_of(at_x * rows + p * piece, piece), piece)]

    tokens = Gather(tok_region, lambda at_tp: tok.at[at_tp], tok_send.at[0], tok_recv, None)

    half_slab = slab // HALVES

    def act_gather(buffer, send, recv):
        def region(at_tp, at_x, p):
            return buffer.at[pl.ds(p * half_slab, half_slab), aligned(at_tp * n_x + at_x, width)]

        return Gather(region, lambda at_tp: buffer.at[:, aligned(at_tp, n_x * width)], send, recv, 1)

    acts = [act_gather(act.at[k], act_send.at[k], act_recv.at[k]) for k in range(2)]
    guests = act_gather(guest, guest_send.at[0], guest_recv)

    def guest_copy(p):
        cut = (pl.ds(p * half_slab, half_slab), aligned(q, width))
        return remote(
            act.at[(1, *cut)], guest.at[cut], guest_z_send.at[0], guest_z_recv.at[p], to_z(inward)
        )

    def part_rows(j, first):
        return partial.at[j, aligned(1 - x if first else x, rows)]

    def part_copy(j, first):
        here = part_rows(j, first)
        return remote(here, here, part_send.at[0], part_recv.at[j, 0 if first else 1], to_z(outward))

    pl.semaphore_wait(barrier, 3 + inside(z + 1).astype(jnp.int32) + inside(z - 1).astype(jnp.int32))

    both_sides = (True, False)
    x_send(0)
    own_wait(0)
    z_own(0, 0, *both_sides)
    own_wait(1)
    z_own(1, 0, *both_sides)
    tok_copy.wait()
    for p in range(HALVES):
        tokens.start(0, 1, 3, p=p)
    x_send(1)

    tile = iota((states, columns), 0) == iota((states, columns), 1) % states
    tile_exact, tile_half = tile.astype(f32), tile.astype(bf16)

    def exactly(a, b):
        return jnp.dot(a, b, precision=lax.Precision.HIGHEST, preferred_element_type=f32)

    factors = []

    @jax.named_scope("build_decay")
    def build_decay():
        for c in loads:
            c.wait()
        own_head = iota((groups, columns), 0) == iota((groups, columns), 1) // states

        def flat(a):
            return jnp.sum(jnp.where(own_head, exactly(a, tile_exact), 0.0), axis=0, keepdims=True)

        rate_real, rate_imag = flat(rates[0]), flat(rates[1])
        all_groups = step_ref.shape[1]
        head = iota((all_groups, columns), 0) == q * groups + iota((all_groups, columns), 1) // states
        log_step = exactly(jnp.broadcast_to(step_ref[...], (8, all_groups)), head.astype(f32))[0:1]
        step_size = jnp.exp(log_step) / (rows * n_sp)
        exponent, angle = rate_real * step_size, rate_imag * step_size
        magnitude = jnp.exp(exponent)
        cosine = jnp.cos(angle)
        decay_real, decay_imag = magnitude * cosine, magnitude * jnp.sin(angle)
        series = jnp.ones_like(exponent)
        for k in range(10, 1, -1):
            series = 1.0 + series * exponent * (1.0 / k)
        growth = jnp.where(jnp.abs(exponent) < 0.5, exponent * series, magnitude - 1.0)
        less_one = growth * cosine - 2.0 * jnp.square(jnp.sin(0.5 * angle))
        denominator = rate_real * rate_real + rate_imag * rate_imag
        factors.append((less_one * rate_real + decay_imag * rate_imag) / denominator)
        factors.append((decay_imag * rate_real - less_one * rate_imag) / denominator)
        dec_ref[0:1, :] = decay_real
        dec_ref[1:2, :] = decay_imag

    def spread(k):
        high, low = split(matrices[k].reshape(width, states))
        return dot(high, tile_half) + dot(low, tile_half)

    @jax.named_scope("build_drive")
    def build_drive(i):
        same = iota((width, columns), 0) // SSM_GROUP == iota((width, columns), 1) // states
        real, imag = spread(0), spread(1)
        if i == 0:
            drive = factors[0] * real - factors[1] * imag
        else:
            drive = factors[0] * imag + factors[1] * real
        for j, part in enumerate(split(jnp.where(same, drive, 0.0))):
            dmat[i, j] = part

    @jax.named_scope("build_read")
    def build_read(i):
        onto = (iota((columns, states), 0) % states == iota((columns, states), 1)).astype(bf16)
        same = iota((columns, width), 0) // states == iota((columns, width), 1) // SSM_GROUP
        for j, part in enumerate(split(matrices[2 + i].reshape(width, states))):
            rmat[i, j] = jnp.where(same, dot_nt(onto, part), 0.0).astype(bf16)

    @jax.named_scope("build_pool")
    def build_pool():
        onto = (iota((POOL_GROUP, width), 0) == iota((POOL_GROUP, width), 1) % POOL_GROUP).astype(bf16)
        same = iota((width, width), 0) // POOL_GROUP == iota((width, width), 1) // POOL_GROUP
        own = pool_own[...].reshape(width, POOL_GROUP)
        pmat[...] = jnp.where(same, dot(own, onto), 0.0).astype(bf16)

    @jax.named_scope("build_order")
    def build_order(i):
        a, b = iota((slab, slab), i), iota((slab, slab), 1 - i)
        order[i] = (b == (a % CHUNKS) * span + a // CHUNKS).astype(bf16)

    @jax.named_scope("take")
    def take(at_tp, first):
        cut = pl.ds(pl.multiple_of(at_tp * features, features), features)
        gain = gain_ref[:, cut]
        size = min(64, slab)

        def step(i, _):
            here = pl.ds(pl.multiple_of(i * size, size), size)
            block = tok[at_tp, here].astype(f32)
            square = block * block
            total = sum(square[:, k : k + LANES] for k in range(0, features, LANES))
            squares[here] = total if first else squares[here] + total
            scaled[here, cut] = (block * gain).astype(bf16)
            return 0

        lax.fori_loop(0, slab // size, step, 0)

    build_decay()
    build_drive(0)
    relay_in(0, 0)
    relay_out(0, 0, 0)
    x_wait(0)
    z_own(0, 1, *both_sides)
    relay_in(1, 0)
    tokens.relay_y(0)
    build_drive(1)
    relay_out(0, 1, 0)
    build_read(0)
    relay_in(0, 1)
    relay_out(0, 0, 1)
    tokens.relay_x(0)
    tokens.relay_y(1)
    own_wait(2)
    own_wait(3)
    z_own(2, 0, True)
    build_read(1)
    relay_out(1, 0, 0)
    build_order(0)
    build_order(1)
    build_pool()
    relay_out(0, 1, 1)
    tokens.relay_x(1)
    x_wait(1)
    z_own(1, 1, *both_sides)
    x_send(3)
    x_send(2)
    z_own(3, 0, True)
    relay_out(1, 1, 0)
    take(tp, True)
    tokens.relay_both(0)
    tokens.wait_pair(pair, 0)
    take(pair, False)
    relay_in(1, 1)
    tokens.relay_both(1)
    relay_in(2, 0)
    take(across, False)
    relay_out(1, 0, 1)
    tokens.wait_pair(both, 1)
    take(both, False)
    inverse = lax.rsqrt(jnp.sum(squares[...], axis=1, keepdims=True) / (features * n_tp) + epsilon)
    z_final(0)
    pool_in = (dot(scaled[...], w_in[0]) * inverse).astype(bf16)
    halo_out[...] = pool_in[slab - window_reach :]
    halo_copy = remote(halo_out, halo, halo_sem.at[0], halo_sem.at[1], to_z(1))

    @pl.when(inside(z + 1))
    def _():
        halo_copy.start()

    relay_out(1, 1, 1)
    relay_in(3, 0)

    @pl.when(rim)
    def _():
        x_wait(3)
        z_own(3, 1, True)


    @pl.when(z > 0)
    @jax.named_scope("halo_wait")
    def _():
        halo_copy.wait_recv()

    before = jnp.where(z == 0, jnp.zeros_like(halo), halo[...])
    whole = jnp.concatenate([before, pool_in], axis=0).astype(f32)
    window = jnp.left_shift(2, (q * pool_groups + iota((slab, width), 1) // POOL_GROUP) % 4)
    window_sums = jnp.zeros((slab, width), f32)
    running = whole
    for level in range(4):
        running = running + pltpu.roll(running, 2**level, 0)
        window_sums = jnp.where(window == 2 ** (level + 1), running[window_reach:], window_sums)
    position = z * slab + iota((slab, width), 0)
    divisor = jnp.minimum(position + 1, window).astype(f32)
    pooled = window_sums / divisor - whole[window_reach:]
    pooled_high, pooled_low = split(pooled)
    pool_gain = pg_ref[:, aligned(q, width)]
    projected = dot(pooled_high, pmat[...]) + dot(pooled_low, pmat[...])
    act[1, :, aligned(q, width)] = (projected * pool_gain).astype(bf16)

    @pl.when(rim)
    def _():
        for p in range(HALVES):
            guest_copy(p).start()

    @pl.when(middle)
    def _():
        for p in range(HALVES):
            acts[1].start(0, 1, 3, p=p)

    z_own(2, 0, False)

    x_wait(2)

    @pl.when(rim)
    def _():
        z_own(2, 1, True)

    @pl.when(middle)
    def _():
        x_wait(3)
        z_own(2, 1, True, False, flows=(1,))
        z_own(3, 1, True, flows=(1,))

    relay_out(2, 0, 0, (1,))
    z_final(1)
    state_in = (dot(scaled[...], w_in[1]) * inverse).astype(bf16)
    relay_in(3, 1, (1,))
    signal = dot(order[0], state_in).astype(bf16)
    for i in range(2):
        push[i] = dot(signal, dmat[i, 0]) + dot(signal, dmat[i, 1])
    decay_real = jnp.broadcast_to(dec_ref[0:1, :], (CHUNKS, columns))
    decay_imag = jnp.broadcast_to(dec_ref[1:2, :], (CHUNKS, columns))

    def advance(p, carry):
        cut = pl.ds(pl.multiple_of(p * CHUNKS, CHUNKS), CHUNKS)
        real, imag = cmul(decay_real, decay_imag, *carry)
        real, imag = real + push[0, cut, :], imag + push[1, cut, :]
        push[0, cut, :] = real
        push[1, cut, :] = imag
        return real, imag

    zero = jnp.zeros((CHUNKS, columns), f32)
    end_real, end_imag = lax.fori_loop(0, span, advance, (zero, zero), unroll=4)

    def power(real, imag, count):
        out = None
        while count:
            if count % 2:
                out = (real, imag) if out is None else cmul(*out, real, imag)
            real, imag = cmul(real, imag, real, imag)
            count //= 2
        return out

    chunk_decay = power(dec_ref[0:1, :], dec_ref[1:2, :], span)
    block_decay = power(*chunk_decay, CHUNKS)
    row_zero = jnp.zeros((1, columns), f32)
    total = (row_zero, row_zero)
    for j in range(CHUNKS):
        moved = cmul(*chunk_decay, *total)
        total = (moved[0] + end_real[j : j + 1], moved[1] + end_imag[j : j + 1])
    which = iota((CHUNKS, columns), 0)
    ends[z] = jnp.where(which == 0, total[0], jnp.where(which == 1, total[1], 0.0))

    def end_copy(k):
        return remote(ends.at[z], ends.at[z], end_send.at[k - 1], end_recv.at[k - 1], (me + k * n_x, tp))

    for k in range(1, n_z):
        @pl.when(inside(z + k))
        def _():
            end_copy(k).start()

    @pl.when(middle)
    def _():
        for p in range(HALVES):
            here = guests.region(tp, x, p)
            with jax.named_scope("guest_wait"):
                remote(here, here, guest_z_send.at[0], guest_z_recv.at[p], to_pair).wait_recv()
            guests.start(0, 1, 3, p=p)

    @pl.when(middle)
    def _():
        z_own(2, 1, True, False, flows=(0,))
        z_own(3, 1, True, flows=(0,))

    relay_in(3, 1, (0,))
    relay_out(2, 0, 0, (0,))
    relay_out(2, 1, 0)

    @pl.when(middle)
    def _():
        for p in range(HALVES):
            acts[1].relay_x(p)
            acts[1].relay_y(p)

    relay_in(2, 1)
    relay_out(2, 0, 1, (1,))

    @pl.when(middle)
    def _():
        for p in range(HALVES):
            acts[1].relay_both(p)


    @pl.when(middle)
    def _():
        for p in range(HALVES):
            guests.relay_x(p)
            guests.relay_y(p)

    for k in range(1, n_z):
        @pl.when(inside(z - k))
        @jax.named_scope("ends_wait")
        def _():
            there = ends.at[z - k]
            remote(there, there, end_send.at[k - 1], end_recv.at[k - 1], to_z(1)).wait_recv()

    total = (row_zero, row_zero)
    for s in range(n_z - 1):
        moved = cmul(*block_decay, *total)
        use = s < z
        total = (
            jnp.where(use, moved[0] + ends[s, 0:1, :], total[0]),
            jnp.where(use, moved[1] + ends[s, 1:2, :], total[1]),
        )
    begin_real, begin_imag = zero, zero
    for j in range(CHUNKS):
        begin_real = jnp.where(which == j, total[0], begin_real)
        begin_imag = jnp.where(which == j, total[1], begin_imag)
        moved = cmul(*chunk_decay, *total)
        total = (moved[0] + end_real[j : j + 1], moved[1] + end_imag[j : j + 1])

    def add_carry(p, carry):
        cut = pl.ds(pl.multiple_of(p * CHUNKS, CHUNKS), CHUNKS)
        real, imag = cmul(decay_real, decay_imag, *carry)
        push[0, cut, :] = push[0, cut, :] + real
        push[1, cut, :] = push[1, cut, :] + imag
        return real, imag

    lax.fori_loop(0, span, add_carry, (begin_real, begin_imag), unroll=4)
    real_high, real_low = split(push[0])
    imag_high, imag_low = split(push[1])
    readout = dot(real_high, rmat[0, 0]) + dot(real_high, rmat[0, 1]) + dot(real_low, rmat[0, 0])
    readout -= dot(imag_high, rmat[1, 0]) + dot(imag_high, rmat[1, 1]) + dot(imag_low, rmat[1, 0])
    skip = skip_ref[:, aligned(q, width)]
    readout += skip * signal.astype(f32)
    shuffled = jax.nn.gelu(readout).astype(bf16)
    act[0, :, aligned(q, width)] = dot(order[1], shuffled).astype(bf16)
    for p in range(HALVES):
        acts[0].start(0, 1, 3, p=p)

    relay_out(2, 0, 1, (0,))
    relay_out(2, 1, 1)

    @pl.when(middle)
    def _():
        for p in range(HALVES):
            guests.relay_both(p)
        guests.wait_pair(pair, 0)
        guests.wait_pair(both, 1)

    z_final(3)

    @pl.when(middle)
    def _():
        for first in (True, False):
            cut = aligned(1 - x if first else x, rows)
            for j in range(chunk_count):
                partial[j, cut] = dot(guest[cut], w_out[1, j]).astype(bf16)
                part_copy(j, first).start()

    for p in range(HALVES):
        acts[0].relay_x(p)
        acts[0].relay_y(p)
    for p in range(HALVES):
        acts[0].relay_both(p)

    @pl.when(middle)
    def _():
        acts[1].wait_pair(pair, 0)
        acts[1].wait_pair(both, 1)

    acts[0].wait_pair(pair, 0)
    acts[0].wait_pair(both, 1)
    z_final(2)

    def out_columns(half, j):
        return pl.ds(pl.multiple_of(half * out_width + j * LANES, LANES), LANES)

    def out_copy(j):
        return remote(made.at[j], out_ref.at[:, out_columns(x, j)], out_send.at[0], out_recv.at[0], to_x)

    here, there = aligned(x, rows), aligned(1 - x, rows)

    @pl.when(middle)
    def _():
        for j in range(chunk_count):
            made[j] = (dot(act[0, there], w_out[0, j]) + dot(act[1, there], w_out[1, j])).astype(bf16)
            out_copy(j).start()
        for j in range(chunk_count):
            mine = dot(act[0, here], w_out[0, j]) + dot(act[1, here], w_out[1, j])
            out_ref[:, out_columns(x, j)] = mine.astype(bf16)

    @pl.when(rim)
    def _():
        for cut in (there, here):
            for j in range(chunk_count):
                sums[j, cut] = dot(act[0, cut], w_out[0, j])

        @jax.named_scope("partial_wait")
        def part_wait(j, first):
            part = part_rows(j, first)
            recv = part_recv.at[j, 0 if first else 1]
            remote(part, part, part_send.at[0], recv, to_pair).wait_recv()

        for j in range(chunk_count):
            part_wait(j, True)
            made[j] = (sums[j, there] + partial[j, there].astype(f32)).astype(bf16)
            out_copy(j).start()
        for j in range(chunk_count):
            part_wait(j, False)
            out_ref[:, out_columns(x, j)] = (sums[j, here] + partial[j, here].astype(f32)).astype(bf16)

    @jax.named_scope("drain")
    def drain():
        sent = w_in.at[0, pl.ds(0, 2 * in_rows + 2 * chunk_count * out_rows)]
        remote(sent, sent, xw_send.at[0], xw_recv.at[0], to_x).wait_send()
        few = n_x * (2 * in_rows + chunk_count * out_rows)
        many = few + n_x * chunk_count * out_rows
        for d in range(2):
            for s in range(n_z - 1):
                any_sent = jnp.logical_and(inside(z + ways[d]), inside(z - ways[d] * s))
                for count, case in ((many, inner(z + ways[d])), (few, jnp.logical_not(inner(z + ways[d])))):
                    @pl.when(jnp.logical_and(any_sent, case))
                    def _():
                        sent = w_in.at[0, pl.ds(0, count)]
                        remote(sent, sent, z_send.at[d, s], z_recv.at[0, 0, 0], to_z(ways[d])).wait_send()
        tokens.drain(scaled.at[pl.ds(0, 7 * rows // n_tp)])
        acts[0].drain(act.at[0, :, pl.ds(0, 7 * width)])

        @pl.when(middle)
        def _():
            acts[1].drain(act.at[1, :, pl.ds(0, 7 * width)])
            guests.drain(guest.at[:, pl.ds(0, 7 * width)])
            remote(partial, partial, part_send.at[0], part_recv.at[0, 0], to_pair).wait_send()

        @pl.when(rim)
        def _():
            sent = act.at[1, :, aligned(q, width)]
            remote(sent, sent, guest_z_send.at[0], guest_z_recv.at[0], to_pair).wait_send()

        @pl.when(inside(z + 1))
        def _():
            halo_copy.wait_send()

        for k in range(1, n_z):
            @pl.when(inside(z + k))
            def _():
                end_copy(k).wait_send()

        remote(made, made, out_send.at[0], out_recv.at[0], to_x).wait_send()

    drain()
    with jax.named_scope("out_wait"):
        here = out_ref.at[:, aligned(1 - x, out_width)]
        remote(here, here, out_send.at[0], out_recv.at[0], to_x).wait_recv()


def slab_call(n_sp, n_tp, n_x, arrays):
    tokens, state_in_weight, state_out_weight = arrays[0], arrays[2], arrays[14]
    rows, features = tokens.shape
    in_rows, width = state_in_weight.shape
    out_rows, out_columns = state_out_weight.shape
    width //= n_x
    n_z, slab, chunk_count = n_sp // n_x, rows * n_x, out_columns // n_x // LANES
    groups, states = width // SSM_GROUP, arrays[4].shape[1]
    columns, pool_groups = groups * states, width // POOL_GROUP
    vmem = pl.BlockSpec(memory_space=pltpu.VMEM)
    anywhere = pl.BlockSpec(memory_space=pl.ANY)
    dma = pltpu.SemaphoreType.DMA
    return pl.pallas_call(
        functools.partial(slab_kernel, n_sp, n_tp, n_x, states),
        out_shape=pltpu.VMEM((rows, out_columns), bf16),
        in_specs=[anywhere, vmem] + [anywhere] * 4 + [vmem] + [anywhere] * 4 + [vmem, anywhere, vmem]
        + [anywhere] * 2,
        out_specs=vmem,
        scratch_shapes=[
            pltpu.VMEM((n_tp, slab, features), bf16),
            pltpu.VMEM((slab, features * n_tp), bf16),
            pltpu.VMEM((slab, LANES), f32),
            pltpu.VMEM((2, n_sp * in_rows, width), bf16),
            pltpu.VMEM((2, chunk_count, n_sp * out_rows, LANES), bf16),
            pltpu.VMEM((2, 2, width, columns), bf16),
            pltpu.VMEM((2, 2, columns, width), bf16),
            pltpu.VMEM((width, width), bf16),
            pltpu.VMEM((2, slab, columns), f32),
            pltpu.VMEM((2, slab, slab), bf16),
            pltpu.VMEM((window_reach, width), bf16),
            pltpu.VMEM((window_reach, width), bf16),
            pltpu.VMEM((n_z, CHUNKS, columns), f32),
            pltpu.VMEM((2, slab, n_tp * n_x * width), bf16),
            pltpu.VMEM((slab, n_tp * n_x * width), bf16),
            pltpu.VMEM((chunk_count, slab, LANES), bf16),
            pltpu.VMEM((chunk_count, slab, LANES), f32),
            pltpu.VMEM((chunk_count, rows, LANES), bf16),
            pltpu.VMEM((2, groups, states), f32),
            pltpu.VMEM((4, groups, SSM_GROUP, states), f32),
            pltpu.VMEM((pool_groups, POOL_GROUP, POOL_GROUP), bf16),
            pltpu.VMEM((2, columns), f32),
            dma((8,)),
            dma((1,)),
            dma((4,)),
            dma((2, n_z - 1)),
            dma((4, n_z, 2)),
            dma((1,)),
            dma((8,)),
            dma((2,)),
            dma((2, 8)),
            dma((2,)),
            dma((n_z - 1,)),
            dma((n_z - 1,)),
            dma((1,)),
            dma((1,)),
            dma((1,)),
            dma((8,)),
            dma((1,)),
            dma((HALVES,)),
            dma((1,)),
            dma((chunk_count, 2)),
        ],
        compiler_params=pltpu.CompilerParams(
            collective_id=0, has_side_effects=True, vmem_limit_bytes=60 * 2**20
        ),
    )(*arrays)


def slab_fits(n_sp, n_tp, n_x, features, in_rows, width, pool_width, out_rows, out_columns):
    return (
        n_x == 2 and n_tp == 4 and n_sp // n_x == 4 and features % LANES == 0 and width == n_x * LANES
        and pool_width == width and out_columns % (n_x * LANES) == 0
        and n_x * (2 * in_rows + out_columns // (n_x * LANES) * 2 * out_rows) <= n_sp * in_rows
    )


def body(
    n_sp, n_tp, n_x,
    tokens, norm_gain, state_in_weight, pool_in_weight, rate_real, rate_imag, log_step,
    input_real, input_imag, output_real, output_imag, skip_gain, pool_weight, pool_gain,
    state_out_weight, pool_out_weight,
):
    rows, features = tokens.shape
    in_rows, width = state_in_weight.shape
    pool_width = pool_in_weight.shape[1]
    out_rows, out_columns = state_out_weight.shape
    groups = width // SSM_GROUP
    states = rate_real.shape[1]
    columns = groups * states
    pool_groups = pool_width // POOL_GROUP
    if slab_fits(n_sp, n_tp, n_x, features, in_rows, width, pool_width, out_rows, out_columns):
        return slab_call(n_sp, n_tp, n_x, (
            tokens, norm_gain[None], state_in_weight, pool_in_weight, rate_real, rate_imag, log_step[None],
            jnp.swapaxes(input_real, 1, 2), jnp.swapaxes(input_imag, 1, 2), output_real, output_imag,
            skip_gain[None], pool_weight, pool_gain[None], state_out_weight, pool_out_weight,
        ))
    vmem = pl.BlockSpec(memory_space=pltpu.VMEM)
    anywhere = pl.BlockSpec(memory_space=pl.ANY)
    dma = pltpu.SemaphoreType.DMA
    return pl.pallas_call(
        functools.partial(kernel, n_sp, n_tp, n_x, states),
        out_shape=jax.ShapeDtypeStruct((rows, out_columns), bf16),
        in_specs=[anywhere, vmem] + [anywhere] * 4 + [vmem] + [anywhere] * 4 + [vmem, anywhere, vmem]
        + [anywhere] * 2,
        out_specs=vmem,
        scratch_shapes=[
            pltpu.VMEM((n_tp, rows, features), bf16),
            pltpu.VMEM((n_sp * in_rows, width), bf16),
            pltpu.VMEM((n_sp * in_rows, pool_width), bf16),
            pltpu.VMEM((n_sp * out_rows, out_columns), bf16),
            pltpu.VMEM((n_sp * out_rows, out_columns), bf16),
            pltpu.VMEM((rows, features * n_tp), bf16),
            pltpu.VMEM((2, 2, width, columns), bf16),
            pltpu.VMEM((2, 2, columns, width), bf16),
            pltpu.VMEM((pool_width, pool_width), bf16),
            pltpu.VMEM((2, rows, columns), f32),
            pltpu.VMEM((rows + window_reach, pool_width), bf16),
            pltpu.VMEM((window_reach, pool_width), bf16),
            pltpu.VMEM((n_sp, CHUNKS, columns), f32),
            pltpu.VMEM((2, n_tp, rows, width), bf16),
            pltpu.VMEM((rows, width), bf16),
            pltpu.VMEM((rows, pool_width), bf16),
            pltpu.VMEM((window_reach, pool_width), bf16),
            pltpu.VMEM((2, groups, states), f32),
            pltpu.VMEM((4, groups, SSM_GROUP, states), f32),
            pltpu.VMEM((pool_groups, POOL_GROUP, POOL_GROUP), bf16),
            pltpu.VMEM((2, columns), f32),
            dma((12,)),
            dma((4, 2, n_sp // 2, PIECES)),
            dma((4, 2, n_sp // 2, PIECES)),
            dma((n_tp - 1,)),
            dma((n_tp - 1,)),
            dma((2, n_tp - 1)),
            dma((2, n_tp - 1)),
            dma((2,)),
            dma((n_sp - 1,)),
            dma((n_sp - 1,)),
        ],
        compiler_params=pltpu.CompilerParams(
            collective_id=0, has_side_effects=True, vmem_limit_bytes=60 * 2**20
        ),
    )(
        tokens, norm_gain[None], state_in_weight, pool_in_weight, rate_real, rate_imag, log_step[None],
        jnp.swapaxes(input_real, 1, 2), jnp.swapaxes(input_imag, 1, 2), output_real, output_imag,
        skip_gain[None], pool_weight, pool_gain[None], state_out_weight, pool_out_weight,
    )


def solution(mesh):
    n_sp, n_tp = mesh.shape["sp"], mesh.shape["tp"]
    n_x = 2 ** ((n_sp.bit_length() - 1) // 2)
    both, whole = P("sp", "tp"), P()
    return jax.shard_map(
        functools.partial(body, n_sp, n_tp, n_x),
        mesh=mesh,
        in_specs=(both, whole, both, both) + (whole,) * 10 + (both, both),
        out_specs=both,
        check_vma=False,
    )
```

```python
import functools

import jax
import jax.numpy as jnp
from jax import lax
from jax.experimental import pallas as pl
from jax.experimental.pallas import tpu as pltpu
from jax.sharding import PartitionSpec as P

SSM_GROUP = 16
POOL_GROUP = 64
CHUNKS = 8
PIECES = 2

epsilon = 1e-06
window_reach = 16
f32, bf16 = jnp.float32, jnp.bfloat16
MESH = pl.DeviceIdType.MESH


def discretize(rate_real, rate_imag, log_step, length):
    step_size = jnp.exp(log_step)[:, None] / length
    exponent = rate_real * step_size
    angle = rate_imag * step_size
    magnitude = jnp.exp(exponent)
    decay_real = magnitude * jnp.cos(angle)
    decay_imag = magnitude * jnp.sin(angle)
    less_one = jnp.expm1(exponent) * jnp.cos(angle) - 2.0 * jnp.square(jnp.sin(0.5 * angle))
    denominator = rate_real * rate_real + rate_imag * rate_imag
    factor_real = (less_one * rate_real + decay_imag * rate_imag) / denominator
    factor_imag = (decay_imag * rate_real - less_one * rate_imag) / denominator
    return decay_real, decay_imag, factor_real, factor_imag


def iota(shape, axis):
    return lax.broadcasted_iota(jnp.int32, shape, axis)


def dot(a, b):
    return jnp.dot(a, b, preferred_element_type=f32)


def dot_nt(a, b):
    return lax.dot_general(a, b, (((1,), (1,)), ((), ())), preferred_element_type=f32)


def split(a):
    high = a.astype(bf16)
    return high, (a - high.astype(f32)).astype(bf16)


def cmul(ar, ai, br, bi):
    return ar * br - ai * bi, ar * bi + ai * br


def kernel(
    n_sp, n_tp, n_x, states,
    tok_ref, gain_ref, wsi_ref, wpi_ref, rr_ref, ri_ref, step_ref, inr_ref, ini_ref, outr_ref,
    outi_ref, skip_ref, pw_ref, pg_ref, wso_ref, wpo_ref,
    out_ref,
    tok_full, wsi, wpi, wso, wpo, scaled, dmat, rmat, pmat, push, ext, halo, ends, act,
    mine_s, mine_p, halo_out, rates, matrices, pool_own, dec_ref,
    own_sem, ring_send, ring_recv, tok_send, tok_recv, act_send, act_recv, halo_sem, end_send, end_recv,
):
    me, tp = lax.axis_index("sp"), lax.axis_index("tp")
    n_z = n_sp // n_x
    rows = tok_ref.shape[0]
    features = tok_ref.shape[1]
    width = wsi_ref.shape[1]
    pool_width = wpi_ref.shape[1]
    groups = width // SSM_GROUP
    columns = groups * states
    pool_groups = pool_width // POOL_GROUP
    span = rows // CHUNKS

    def place(p):
        x, r = p // n_z, p % n_z
        return (r + (x % 2) * (n_z - 1 - 2 * r)) * n_x + x

    my_x, my_z = me % n_x, me // n_x
    at = my_x * n_z + my_z + (my_x % 2) * (n_z - 1 - 2 * my_z)

    barrier = pltpu.get_barrier_semaphore()
    for k in range(1, n_sp):
        pl.semaphore_signal(barrier, inc=1, device_id=((me + k) % n_sp, tp), device_id_type=MESH)
    for k in range(1, n_tp):
        pl.semaphore_signal(barrier, inc=1, device_id=(me, (tp + k) % n_tp), device_id_type=MESH)

    fulls = ((wsi_ref, wsi), (wpi_ref, wpi), (wso_ref, wso), (wpo_ref, wpo))
    owns = []
    for a, (own, full) in enumerate(fulls):
        count = own.shape[0]
        owns.append(
            pltpu.make_async_copy(
                own, full.at[pl.ds(pl.multiple_of(me * count, count), count)], own_sem.at[a]
            )
        )
    owns.append(pltpu.make_async_copy(tok_ref, tok_full.at[tp], own_sem.at[4]))
    def heads(ref, count):
        return ref.at[pl.ds(pl.multiple_of(tp * count, count), count)]

    loads = [
        pltpu.make_async_copy(heads(ref, groups), there, own_sem.at[5 + k])
        for k, (ref, there) in enumerate(
            (
                (rr_ref, rates.at[0]), (ri_ref, rates.at[1]), (inr_ref, matrices.at[0]),
                (ini_ref, matrices.at[1]), (outr_ref, matrices.at[2]), (outi_ref, matrices.at[3]),
            )
        )
    ]
    loads.append(pltpu.make_async_copy(heads(pw_ref, pool_groups), pool_own, own_sem.at[11]))
    for c in owns + loads:
        c.start()
    pl.semaphore_wait(barrier, n_sp - 1 + n_tp - 1)

    ways = (1, -1)

    def reach_of(a, d):
        return n_sp // 2 if a % 2 == d else n_sp - 1 - n_sp // 2

    def part(a, d, s, h):
        own, full = fulls[a]
        count = own.shape[0]
        size = count // PIECES
        way = ways[d]
        owner = place((at - way * s + n_sp) % n_sp)
        there = full.at[pl.ds(pl.multiple_of(owner * count + h * size, size), size)]
        source = own.at[pl.ds(h * size, size)] if s == 0 else there
        return source, there, (place((at + way + n_sp) % n_sp), tp)

    def sender(a, d, s, h):
        source, there, target = part(a, d, s, h)
        return pltpu.make_async_remote_copy(
            source, there, ring_send.at[a, d, s, h], ring_recv.at[a, d, s, h],
            device_id=target, device_id_type=MESH,
        )

    def arrive(a, d, s, h):
        _, there, target = part(a, d, s + 1, h)
        pltpu.make_async_remote_copy(
            there, there, ring_send.at[a, d, s, h], ring_recv.at[a, d, s, h],
            device_id=target, device_id_type=MESH,
        ).wait_recv()

    longest = n_sp // 2

    def ring(phase, s, h):
        streams = [
            (a, d) for a in (2 * phase, 2 * phase + 1) for d in range(2) if s < reach_of(a, d)
        ]
        for a, d in sorted(streams, key=lambda i: -reach_of(*i)):
            arrive(a, d, s, h)
            if s + 1 < reach_of(a, d):
                sender(a, d, s + 1, h).start()
        if phase == 0 and h == PIECES - 1:
            for a, d in streams:
                if s + 1 == reach_of(a, d):
                    for g in range(PIECES):
                        sender(a + 2, d, 0, g).start()

    turns = [(phase, s, h) for phase in range(2) for s in range(longest) for h in range(PIECES)]
    turn = [0]

    def step(stop=len(turns)):
        if turn[0] < stop:
            ring(*turns[turn[0]])
            turn[0] += 1

    def token_copy(k):
        return pltpu.make_async_remote_copy(
            tok_ref, tok_full.at[tp], tok_send.at[k - 1], tok_recv.at[k - 1],
            device_id=(me, (tp + k) % n_tp), device_id_type=MESH,
        )

    for h in range(PIECES):
        for a, d in ((0, 0), (1, 1), (0, 1), (1, 0)):
            sender(a, d, 0, h).start()
    for k in range(1, n_tp):
        token_copy(k).start()

    tile = iota((states, columns), 0) == iota((states, columns), 1) % states
    tile_exact, tile_half = tile.astype(f32), tile.astype(bf16)

    def exactly(a, b):
        return jnp.dot(a, b, precision=lax.Precision.HIGHEST, preferred_element_type=f32)

    factors = []

    def build_decay():
        for c in loads:
            c.wait()
        own_head = iota((groups, columns), 0) == iota((groups, columns), 1) // states

        def flat(a):
            return jnp.sum(jnp.where(own_head, exactly(a, tile_exact), 0.0), axis=0, keepdims=True)

        rate_real, rate_imag = flat(rates[0]), flat(rates[1])
        all_groups = step_ref.shape[1]
        head = iota((all_groups, columns), 0) == tp * groups + iota((all_groups, columns), 1) // states
        log_step = exactly(jnp.broadcast_to(step_ref[...], (8, all_groups)), head.astype(f32))[0:1]
        step_size = jnp.exp(log_step) / (rows * n_sp)
        exponent, angle = rate_real * step_size, rate_imag * step_size
        magnitude = jnp.exp(exponent)
        cosine = jnp.cos(angle)
        decay_real, decay_imag = magnitude * cosine, magnitude * jnp.sin(angle)
        series = jnp.ones_like(exponent)
        for k in range(10, 1, -1):
            series = 1.0 + series * exponent * (1.0 / k)
        growth = jnp.where(jnp.abs(exponent) < 0.5, exponent * series, magnitude - 1.0)
        less_one = growth * cosine - 2.0 * jnp.square(jnp.sin(0.5 * angle))
        denominator = rate_real * rate_real + rate_imag * rate_imag
        factors.append((less_one * rate_real + decay_imag * rate_imag) / denominator)
        factors.append((decay_imag * rate_real - less_one * rate_imag) / denominator)
        dec_ref[0:1, :] = decay_real
        dec_ref[1:2, :] = decay_imag

    def spread(k):
        high, low = split(matrices[k].reshape(width, states))
        return dot(high, tile_half) + dot(low, tile_half)

    def build_drive(i):
        same = iota((width, columns), 0) // SSM_GROUP == iota((width, columns), 1) // states
        real, imag = spread(0), spread(1)
        if i == 0:
            drive = factors[0] * real - factors[1] * imag
        else:
            drive = factors[0] * imag + factors[1] * real
        for j, piece in enumerate(split(jnp.where(same, drive, 0.0))):
            dmat[i, j] = piece

    def build_read(i):
        across = (iota((columns, states), 0) % states == iota((columns, states), 1)).astype(bf16)
        same = iota((columns, width), 0) // states == iota((columns, width), 1) // SSM_GROUP
        for j, piece in enumerate(split(matrices[2 + i].reshape(width, states))):
            rmat[i, j] = jnp.where(same, dot_nt(across, piece), 0.0).astype(bf16)

    def build_pool():
        across = (
            iota((POOL_GROUP, pool_width), 0) == iota((POOL_GROUP, pool_width), 1) % POOL_GROUP
        ).astype(bf16)
        same = iota((pool_width, pool_width), 0) // POOL_GROUP == iota((pool_width, pool_width), 1) // POOL_GROUP
        own = pool_own[...].reshape(pool_width, POOL_GROUP)
        pmat[...] = jnp.where(same, dot(own, across), 0.0).astype(bf16)

    squares = []

    def take(t):
        block = tok_full[t].astype(f32)
        squares.append(jnp.sum(block * block, axis=1, keepdims=True))
        cut = slice(t * features, (t + 1) * features)
        scaled[:, cut] = (block * gain_ref[:, cut]).astype(bf16)

    def tokens_in():
        owns[4].wait()
        for k in range(1, n_tp):
            pltpu.make_async_remote_copy(
                tok_ref, tok_full.at[(tp - k + n_tp) % n_tp], tok_send.at[k - 1], tok_recv.at[k - 1],
                device_id=(me, (tp + k) % n_tp), device_id_type=MESH,
            ).wait_recv()

    half = len(turns) // 2
    for at_work, work in enumerate(
        (
            build_decay, lambda: build_drive(0), lambda: build_drive(1), lambda: build_read(0),
            lambda: build_read(1), build_pool,
        )
    ):
        work()
        if at_work in (0, 1, 3, 5):
            step(half)
    while turn[0] < half - 3:
        step(half)
    tokens_in()
    for t in range(n_tp):
        take(t)
        if t == n_tp // 2 - 1:
            step(half)
    while turn[0] < half:
        step(half)
    owns[0].wait()
    owns[1].wait()
    inverse = lax.rsqrt(sum(squares) / (features * n_tp) + epsilon)
    state_in = (dot(scaled[...], wsi[...]) * inverse).astype(bf16)
    pool_in = (dot(scaled[...], wpi[...]) * inverse).astype(bf16)
    ext[window_reach:] = pool_in
    halo_out[...] = pool_in[rows - window_reach :]
    halo_copy = pltpu.make_async_remote_copy(
        halo_out, halo, halo_sem.at[0], halo_sem.at[1],
        device_id=((me + 1) % n_sp, tp), device_id_type=MESH,
    )
    shuffle = (
        iota((rows, rows), 1)
        == (iota((rows, rows), 0) % CHUNKS) * span + iota((rows, rows), 0) // CHUNKS
    ).astype(bf16)
    signal = dot(shuffle, state_in).astype(bf16)
    for i in range(2):
        push[i] = dot(signal, dmat[i, 0]) + dot(signal, dmat[i, 1])
        if i == 0:
            halo_copy.start()
        else:
            step()
    decay_real = jnp.broadcast_to(dec_ref[0:1, :], (CHUNKS, columns))
    decay_imag = jnp.broadcast_to(dec_ref[1:2, :], (CHUNKS, columns))

    def advance(p, carry):
        cut = pl.ds(pl.multiple_of(p * CHUNKS, CHUNKS), CHUNKS)
        real, imag = cmul(decay_real, decay_imag, *carry)
        real, imag = real + push[0, cut, :], imag + push[1, cut, :]
        push[0, cut, :] = real
        push[1, cut, :] = imag
        return real, imag

    zero = jnp.zeros((CHUNKS, columns), f32)
    end_real, end_imag = lax.fori_loop(0, span, advance, (zero, zero))

    def power(real, imag, count):
        out = None
        while count:
            if count % 2:
                out = (real, imag) if out is None else cmul(*out, real, imag)
            real, imag = cmul(real, imag, real, imag)
            count //= 2
        return out

    chunk_decay = power(dec_ref[0:1, :], dec_ref[1:2, :], span)
    block_decay = power(*chunk_decay, CHUNKS)
    row_zero = jnp.zeros((1, columns), f32)
    total = (row_zero, row_zero)
    for j in range(CHUNKS):
        moved = cmul(*chunk_decay, *total)
        total = (moved[0] + end_real[j : j + 1], moved[1] + end_imag[j : j + 1])
    which = iota((CHUNKS, columns), 0)
    ends[me] = jnp.where(which == 0, total[0], jnp.where(which == 1, total[1], 0.0))

    def end_copy(k):
        return pltpu.make_async_remote_copy(
            ends.at[me], ends.at[me], end_send.at[k - 1], end_recv.at[k - 1],
            device_id=((me + k) % n_sp, tp), device_id_type=MESH,
        )

    for k in range(1, n_sp):
        end_copy(k).start()

    halo_copy.wait_recv()
    ext[:window_reach] = jnp.where(me == 0, jnp.zeros_like(halo), halo[...])
    group = tp * (pool_width // POOL_GROUP) + iota((rows, pool_width), 1) // POOL_GROUP
    window = jnp.left_shift(jnp.ones_like(group), group % 4 + 1)
    targets = iota((rows, rows + window_reach), 0) + window_reach
    sources = iota((rows, rows + window_reach), 1)
    whole = ext[...]
    sums = jnp.zeros((rows, pool_width), f32)
    for power_index in range(1, 5):
        reach = 2**power_index
        band = ((sources <= targets) & (sources > targets - reach)).astype(bf16)
        sums = jnp.where(window == reach, dot(band, whole), sums)
        if power_index == 2:
            step()
    position = me * rows + iota((rows, pool_width), 0)
    divisor = jnp.minimum(position + 1, window).astype(f32)
    pooled = sums / divisor - ext[window_reach:].astype(f32)
    pooled_high, pooled_low = split(pooled)
    pool_gain = pg_ref[:, pl.ds(pl.multiple_of(tp * pool_width, pool_width), pool_width)]
    projected = dot(pooled_high, pmat[...]) + dot(pooled_low, pmat[...])
    mine_p[...] = (projected * pool_gain).astype(bf16)
    step()

    def act_copy(which, k, source):
        mine = mine_s if which == 0 else mine_p
        return pltpu.make_async_remote_copy(
            mine, act.at[which, source], act_send.at[which, k - 1], act_recv.at[which, k - 1],
            device_id=(me, (tp + k) % n_tp), device_id_type=MESH,
        )

    for k in range(1, n_tp):
        act_copy(1, k, tp).start()
    act[1, tp] = mine_p[...]

    for k in range(1, n_sp):
        there = ends.at[(me - k + n_sp) % n_sp]
        pltpu.make_async_remote_copy(
            there, there, end_send.at[k - 1], end_recv.at[k - 1],
            device_id=((me + k) % n_sp, tp), device_id_type=MESH,
        ).wait_recv()
    total = (row_zero, row_zero)
    for s in range(n_sp - 1):
        moved = cmul(*block_decay, *total)
        use = s < me
        total = (
            jnp.where(use, moved[0] + ends[s, 0:1, :], total[0]),
            jnp.where(use, moved[1] + ends[s, 1:2, :], total[1]),
        )
    begin_real, begin_imag = zero, zero
    for j in range(CHUNKS):
        begin_real = jnp.where(which == j, total[0], begin_real)
        begin_imag = jnp.where(which == j, total[1], begin_imag)
        moved = cmul(*chunk_decay, *total)
        total = (moved[0] + end_real[j : j + 1], moved[1] + end_imag[j : j + 1])

    def add_carry(p, carry):
        cut = pl.ds(pl.multiple_of(p * CHUNKS, CHUNKS), CHUNKS)
        real, imag = cmul(decay_real, decay_imag, *carry)
        push[0, cut, :] = push[0, cut, :] + real
        push[1, cut, :] = push[1, cut, :] + imag
        return real, imag

    lax.fori_loop(0, span, add_carry, (begin_real, begin_imag))
    step()
    real_high, real_low = split(push[0])
    imag_high, imag_low = split(push[1])
    readout = dot(real_high, rmat[0, 0]) + dot(real_high, rmat[0, 1]) + dot(real_low, rmat[0, 0])
    step()
    readout -= dot(imag_high, rmat[1, 0]) + dot(imag_high, rmat[1, 1]) + dot(imag_low, rmat[1, 0])
    skip = skip_ref[:, pl.ds(pl.multiple_of(tp * width, width), width)]
    readout += skip * signal.astype(f32)
    shuffled = jax.nn.gelu(readout).astype(bf16)
    restore = (
        iota((rows, rows), 0)
        == (iota((rows, rows), 1) % CHUNKS) * span + iota((rows, rows), 1) // CHUNKS
    ).astype(bf16)
    mine_s[...] = dot(restore, shuffled).astype(bf16)
    for k in range(1, n_tp):
        act_copy(0, k, tp).start()
    act[0, tp] = mine_s[...]
    while turn[0] < len(turns):
        step()
    for which in (1, 0):
        for k in range(1, n_tp):
            act_copy(which, k, (tp - k + n_tp) % n_tp).wait_recv()
    owns[2].wait()
    owns[3].wait()
    result = None
    for t in range(n_tp):
        for which, full, size in ((1, wpo, pool_width), (0, wso, width)):
            term = dot(act[which, t], full[t * size : (t + 1) * size, :])
            result = term if result is None else result + term
    out_ref[...] = result.astype(bf16)

    for a in range(4):
        for d in range(2):
            for s in range(reach_of(a, d)):
                for h in range(PIECES):
                    sender(a, d, s, h).wait_send()
    for k in range(1, n_tp):
        token_copy(k).wait_send()
        act_copy(0, k, tp).wait_send()
        act_copy(1, k, tp).wait_send()
    halo_copy.wait_send()
    for k in range(1, n_sp):
        end_copy(k).wait_send()

LANES = 128
HALVES = 2


def slab_kernel(
    n_sp, n_tp, n_x, states,
    tok_ref, gain_ref, wsi_ref, wpi_ref, rr_ref, ri_ref, step_ref, inr_ref, ini_ref, outr_ref,
    outi_ref, skip_ref, pw_ref, pg_ref, wso_ref, wpo_ref,
    out_ref,
    tok, scaled, squares, w_in, w_out, dmat, rmat, pmat, push, order, halo, halo_out, ends, act,
    guest, partial, sums, made, rates, matrices, pool_own, dec_ref,
    own_sem, xw_send, xw_recv, z_send, z_recv, tok_send, tok_recv, act_send, act_recv, halo_sem, end_send, end_recv,
    out_send, out_recv, guest_send, guest_recv, guest_z_send, guest_z_recv, part_send, part_recv,
):
    me, tp = lax.axis_index("sp"), lax.axis_index("tp")
    n_z = n_sp // n_x
    z, x = me // n_x, me % n_x
    y, core = tp // 2, tp % 2
    rows = tok_ref.shape[0]
    slab = rows * n_x
    features = tok_ref.shape[1]
    in_rows = wsi_ref.shape[0]
    out_rows = wso_ref.shape[0]
    width = wsi_ref.shape[1] // n_x
    out_width = wso_ref.shape[1] // n_x
    chunk_count = out_width // LANES
    groups = width // SSM_GROUP
    columns = groups * states
    pool_groups = width // POOL_GROUP
    span = slab // CHUNKS
    q = tp * n_x + x

    across, pair, both = (1 - y) * 2 + core, y * 2 + 1 - core, (1 - y) * 2 + 1 - core
    beside = me + 1 - 2 * x
    to_x, to_y, to_pair = (beside, tp), (me, across), (me, pair)
    ways = (1, -1)

    def to_z(way):
        return (me + way * n_x, tp)

    def inside(at):
        return jnp.logical_and(at >= 0, at < n_z)

    def inner(at):
        return jnp.logical_and(at > 0, at < n_z - 1)

    middle, rim = inner(z), jnp.logical_not(inner(z))
    inward, outward = jnp.where(z == 0, 1, -1), jnp.where(z == 1, -1, 1)

    def aligned(index, size):
        return pl.ds(pl.multiple_of(index * size, size), size)

    barrier = pltpu.get_barrier_semaphore()
    for there in (to_x, to_y, to_pair):
        pl.semaphore_signal(barrier, inc=1, device_id=there, device_id_type=MESH)
    for way in ways:
        @pl.when(inside(z + way))
        def _():
            pl.semaphore_signal(barrier, inc=1, device_id=to_z(way), device_id_type=MESH)

    def remote(source, there, send, recv, target):
        return pltpu.make_async_remote_copy(
            source, there, send, recv, device_id=target, device_id_type=MESH
        )

    def in_part(ref, half):
        return ref.at[:, aligned(half, width)]

    def out_part(ref, half, j):
        return ref.at[:, pl.ds(pl.multiple_of(half * out_width + j * LANES, LANES), LANES)]

    own_in, own_out = (wpi_ref, wsi_ref), (wso_ref, wpo_ref)

    def in_at(m, sp):
        return w_in.at[m, aligned(sp, in_rows)]

    def out_at(m, sp):
        return w_out.at[m, :, aligned(sp, out_rows)]

    def weight_at(k, sp):
        return in_at(k, sp) if k < 2 else out_at(k - 2, sp)

    def parts(k, half, sp):
        if k < 2:
            return [(in_part(own_in[k], half), in_at(k, sp))]
        return [
            (out_part(own_out[k - 2], half, j), w_out.at[k - 2, j, aligned(sp, out_rows)])
            for j in range(chunk_count)
        ]

    def own_copy(k):
        return [pltpu.make_async_copy(source, there, own_sem.at[k]) for source, there in parts(k, x, me)]

    def own_wait(k):
        here = weight_at(k, me)
        pltpu.make_async_copy(here, here, own_sem.at[k]).wait()

    base = 4
    tok_copy = pltpu.make_async_copy(tok_ref, tok.at[tp, aligned(x, rows)], own_sem.at[base])

    def heads(ref, count):
        return ref.at[aligned(q, count)]

    loads = [
        pltpu.make_async_copy(heads(ref, count), there, own_sem.at[base + 1 + k])
        for ref, count, there, k in (
            (rr_ref, groups, rates.at[0], 0), (ri_ref, groups, rates.at[1], 0),
            (inr_ref, groups, matrices.at[0], 1), (ini_ref, groups, matrices.at[1], 1),
            (outr_ref, groups, matrices.at[2], 1), (outi_ref, groups, matrices.at[3], 1),
            (pw_ref, pool_groups, pool_own, 2),
        )
    ]
    for c in own_copy(0) + [tok_copy] + loads + [c for k in range(1, base) for c in own_copy(k)]:
        c.start()

    def x_send(k):
        for source, there in parts(k, 1 - x, me):
            remote(source, there, xw_send.at[0], xw_recv.at[k], to_x).start()

    @jax.named_scope("across_wait")
    def x_wait(k):
        here = weight_at(k, beside)
        remote(here, here, xw_send.at[0], xw_recv.at[k], to_x).wait_recv()

    def z_part(stage, h, at):
        return weight_at(stage, at * n_x + (x if h == 0 else 1 - x))

    def reach(way, stage):
        return inside(z + way) if stage < 3 else inner(z + way)

    def z_copy(d, stage, s, h):
        at = z - ways[d] * s
        there = z_part(stage, h, at)
        return remote(there, there, z_send.at[d, s], z_recv.at[stage, at, h], to_z(ways[d]))

    def toward(way, stage, inner_side):
        there = z + way
        if inner_side:
            return inner(there)
        return jnp.logical_and(reach(way, stage), jnp.logical_not(inner(there)))

    def z_own(stage, h, *sides, flows=(0, 1)):
        for inner_side in sides:
            for d in flows:
                @pl.when(toward(ways[d], stage, inner_side))
                def _():
                    z_copy(d, stage, 0, h).start()

    def z_arrive(d, stage, s, h):
        at = z - ways[d] * (s + 1)
        here = z_part(stage, h, at)
        remote(here, here, z_send.at[d, s], z_recv.at[stage, at, h], to_z(ways[d])).wait_recv()

    def z_relay(stage, s, h, inner_side, flows):
        for d in flows:
            @pl.when(jnp.logical_and(inside(z - ways[d] * (s + 1)), toward(ways[d], stage, inner_side)))
            def _():
                z_arrive(d, stage, s, h)
                z_copy(d, stage, s + 1, h).start()

    @jax.named_scope("relay_in")
    def relay_in(stage, h, flows=(0, 1)):
        z_relay(stage, 0, h, True, flows)

    @jax.named_scope("relay_out")
    def relay_out(stage, s, h, flows=(0, 1)):
        z_relay(stage, s, h, False, flows)

    @jax.named_scope("final_wait")
    def z_final(stage):
        here = rim if stage < 3 else middle
        for d in range(2):
            for s in range(n_z - 1):
                stays = jnp.logical_and(here, jnp.logical_not(reach(ways[d], stage)))
                @pl.when(jnp.logical_and(inside(z - ways[d] * (s + 1)), stays))
                def _():
                    for h in range(2):
                        z_arrive(d, stage, s, h)

    class Gather:
        def __init__(self, region, pair_region, send, recv, turned):
            self.region, self.pair_region, self.send, self.recv = region, pair_region, send, recv
            self.turned = turned

        def copy(self, slot, p):
            at_tp, at_x = (
                (tp, x), (tp, x), (across, x) if p == self.turned else (tp, 1 - x), (tp, x), (tp, 1 - x), (across, x), (across, 1 - x)
            )[slot]
            here = self.region(at_tp, at_x, p)
            recv = self.recv.at[2 * slot + p if slot < 3 else 6 if slot < 5 else 7]
            target = (to_x, to_y, to_x if p == self.turned else to_y, to_pair, to_pair, to_pair, to_pair)[slot]
            return remote(here, here, self.send, recv, target)

        def start(self, *slots, p):
            for slot in slots:
                self.copy(slot, p).start()

        @jax.named_scope("gather_wait")
        def wait(self, slot, p):
            here = self.region(*((tp, 1 - x), (across, x), (across, 1 - x))[slot], p)
            remote(here, here, self.send, self.recv.at[2 * slot + p], to_pair).wait_recv()

        @jax.named_scope("pair_wait")
        def wait_pair(self, at_tp, k):
            here = self.pair_region(at_tp)
            remote(here, here, self.send, self.recv.at[6 + k], to_pair).wait_recv()

        def relay_x(self, p):
            self.wait(0, p)
            self.start(*((4,) if p == self.turned else (2, 4)), p=p)

        def relay_y(self, p):
            self.wait(1, p)
            self.start(*((2, 5) if p == self.turned else (5,)), p=p)

        def relay_both(self, p):
            self.wait(2, p)
            self.start(6, p=p)

        def drain(self, sent):
            remote(sent, sent, self.send, self.recv.at[0], to_pair).wait_send()

    piece = rows // HALVES

    def tok_region(at_tp, at_x, p):
        return tok.at[at_tp, pl.ds(pl.multiple_of(at_x * rows + p * piece, piece), piece)]

    tokens = Gather(tok_region, lambda at_tp: tok.at[at_tp], tok_send.at[0], tok_recv, None)

    half_slab = slab // HALVES

    def act_gather(buffer, send, recv):
        def region(at_tp, at_x, p):
            return buffer.at[pl.ds(p * half_slab, half_slab), aligned(at_tp * n_x + at_x, width)]

        return Gather(region, lambda at_tp: buffer.at[:, aligned(at_tp, n_x * width)], send, recv, 1)

    acts = [act_gather(act.at[k], act_send.at[k], act_recv.at[k]) for k in range(2)]
    guests = act_gather(guest, guest_send.at[0], guest_recv)

    def guest_copy(p):
        cut = (pl.ds(p * half_slab, half_slab), aligned(q, width))
        return remote(
            act.at[(1, *cut)], guest.at[cut], guest_z_send.at[0], guest_z_recv.at[p], to_z(inward)
        )

    def part_rows(j, first):
        return partial.at[j, aligned(1 - x if first else x, rows)]

    def part_copy(j, first):
        here = part_rows(j, first)
        return remote(here, here, part_send.at[0], part_recv.at[j, 0 if first else 1], to_z(outward))

    pl.semaphore_wait(barrier, 3 + inside(z + 1).astype(jnp.int32) + inside(z - 1).astype(jnp.int32))

    both_sides = (True, False)
    x_send(0)
    own_wait(0)
    z_own(0, 0, *both_sides)
    own_wait(1)
    z_own(1, 0, *both_sides)
    tok_copy.wait()
    for p in range(HALVES):
        tokens.start(0, 1, 3, p=p)
    x_send(1)

    tile = iota((states, columns), 0) == iota((states, columns), 1) % states
    tile_exact, tile_half = tile.astype(f32), tile.astype(bf16)

    def exactly(a, b):
        return jnp.dot(a, b, precision=lax.Precision.HIGHEST, preferred_element_type=f32)

    factors = []

    @jax.named_scope("build_decay")
    def build_decay():
        for c in loads:
            c.wait()
        own_head = iota((groups, columns), 0) == iota((groups, columns), 1) // states

        def flat(a):
            return jnp.sum(jnp.where(own_head, exactly(a, tile_exact), 0.0), axis=0, keepdims=True)

        rate_real, rate_imag = flat(rates[0]), flat(rates[1])
        all_groups = step_ref.shape[1]
        head = iota((all_groups, columns), 0) == q * groups + iota((all_groups, columns), 1) // states
        log_step = exactly(jnp.broadcast_to(step_ref[...], (8, all_groups)), head.astype(f32))[0:1]
        step_size = jnp.exp(log_step) / (rows * n_sp)
        exponent, angle = rate_real * step_size, rate_imag * step_size
        magnitude = jnp.exp(exponent)
        cosine = jnp.cos(angle)
        decay_real, decay_imag = magnitude * cosine, magnitude * jnp.sin(angle)
        series = jnp.ones_like(exponent)
        for k in range(10, 1, -1):
            series = 1.0 + series * exponent * (1.0 / k)
        growth = jnp.where(jnp.abs(exponent) < 0.5, exponent * series, magnitude - 1.0)
        less_one = growth * cosine - 2.0 * jnp.square(jnp.sin(0.5 * angle))
        denominator = rate_real * rate_real + rate_imag * rate_imag
        factors.append((less_one * rate_real + decay_imag * rate_imag) / denominator)
        factors.append((decay_imag * rate_real - less_one * rate_imag) / denominator)
        dec_ref[0:1, :] = decay_real
        dec_ref[1:2, :] = decay_imag

    def spread(k):
        high, low = split(matrices[k].reshape(width, states))
        return dot(high, tile_half) + dot(low, tile_half)

    @jax.named_scope("build_drive")
    def build_drive(i):
        same = iota((width, columns), 0) // SSM_GROUP == iota((width, columns), 1) // states
        real, imag = spread(0), spread(1)
        if i == 0:
            drive = factors[0] * real - factors[1] * imag
        else:
            drive = factors[0] * imag + factors[1] * real
        for j, part in enumerate(split(jnp.where(same, drive, 0.0))):
            dmat[i, j] = part

    @jax.named_scope("build_read")
    def build_read(i):
        onto = (iota((columns, states), 0) % states == iota((columns, states), 1)).astype(bf16)
        same = iota((columns, width), 0) // states == iota((columns, width), 1) // SSM_GROUP
        for j, part in enumerate(split(matrices[2 + i].reshape(width, states))):
            rmat[i, j] = jnp.where(same, dot_nt(onto, part), 0.0).astype(bf16)

    @jax.named_scope("build_pool")
    def build_pool():
        onto = (iota((POOL_GROUP, width), 0) == iota((POOL_GROUP, width), 1) % POOL_GROUP).astype(bf16)
        same = iota((width, width), 0) // POOL_GROUP == iota((width, width), 1) // POOL_GROUP
        own = pool_own[...].reshape(width, POOL_GROUP)
        pmat[...] = jnp.where(same, dot(own, onto), 0.0).astype(bf16)

    @jax.named_scope("build_order")
    def build_order(i):
        a, b = iota((slab, slab), i), iota((slab, slab), 1 - i)
        order[i] = (b == (a % CHUNKS) * span + a // CHUNKS).astype(bf16)

    @jax.named_scope("take")
    def take(at_tp, first):
        cut = pl.ds(pl.multiple_of(at_tp * features, features), features)
        gain = gain_ref[:, cut]
        size = min(64, slab)

        def step(i, _):
            here = pl.ds(pl.multiple_of(i * size, size), size)
            block = tok[at_tp, here].astype(f32)
            square = block * block
            total = sum(square[:, k : k + LANES] for k in range(0, features, LANES))
            squares[here] = total if first else squares[here] + total
            scaled[here, cut] = (block * gain).astype(bf16)
            return 0

        lax.fori_loop(0, slab // size, step, 0)

    build_decay()
    build_drive(0)
    relay_in(0, 0)
    relay_out(0, 0, 0)
    x_wait(0)
    z_own(0, 1, *both_sides)
    relay_in(1, 0)
    tokens.relay_y(0)
    build_drive(1)
    relay_out(0, 1, 0)
    build_read(0)
    relay_in(0, 1)
    relay_out(0, 0, 1)
    tokens.relay_x(0)
    tokens.relay_y(1)
    own_wait(2)
    own_wait(3)
    z_own(2, 0, True)
    build_read(1)
    relay_out(1, 0, 0)
    build_order(0)
    build_order(1)
    build_pool()
    relay_out(0, 1, 1)
    tokens.relay_x(1)
    x_wait(1)
    z_own(1, 1, *both_sides)
    x_send(3)
    x_send(2)
    z_own(3, 0, True)
    relay_out(1, 1, 0)
    take(tp, True)
    tokens.relay_both(0)
    tokens.wait_pair(pair, 0)
    take(pair, False)
    relay_in(1, 1)
    tokens.relay_both(1)
    relay_in(2, 0)
    take(across, False)
    relay_out(1, 0, 1)
    tokens.wait_pair(both, 1)
    take(both, False)
    inverse = lax.rsqrt(jnp.sum(squares[...], axis=1, keepdims=True) / (features * n_tp) + epsilon)
    z_final(0)
    pool_in = (dot(scaled[...], w_in[0]) * inverse).astype(bf16)
    halo_out[...] = pool_in[slab - window_reach :]
    halo_copy = remote(halo_out, halo, halo_sem.at[0], halo_sem.at[1], to_z(1))

    @pl.when(inside(z + 1))
    def _():
        halo_copy.start()

    relay_out(1, 1, 1)
    relay_in(3, 0)

    @pl.when(rim)
    def _():
        x_wait(3)
        z_own(3, 1, True)


    def project_state():
        sums[0] = (dot(scaled[...], w_in[1]) * inverse).astype(bf16).astype(f32)

    @pl.when(middle)
    def _():
        project_state()

    @pl.when(z > 0)
    @jax.named_scope("halo_wait")
    def _():
        halo_copy.wait_recv()

    before = jnp.where(z == 0, jnp.zeros_like(halo), halo[...])
    whole = jnp.concatenate([before, pool_in], axis=0).astype(f32)
    window = jnp.left_shift(2, (q * pool_groups + iota((slab, width), 1) // POOL_GROUP) % 4)
    window_sums = jnp.zeros((slab, width), f32)
    running = whole
    for level in range(4):
        running = running + pltpu.roll(running, 2**level, 0)
        window_sums = jnp.where(window == 2 ** (level + 1), running[window_reach:], window_sums)
    position = z * slab + iota((slab, width), 0)
    divisor = jnp.minimum(position + 1, window).astype(f32)
    pooled = window_sums / divisor - whole[window_reach:]
    pooled_high, pooled_low = split(pooled)
    pool_gain = pg_ref[:, aligned(q, width)]
    projected = dot(pooled_high, pmat[...]) + dot(pooled_low, pmat[...])
    act[1, :, aligned(q, width)] = (projected * pool_gain).astype(bf16)

    @pl.when(rim)
    def _():
        for p in range(HALVES):
            guest_copy(p).start()

    @pl.when(middle)
    def _():
        for p in range(HALVES):
            acts[1].start(0, 1, 3, p=p)

    z_own(2, 0, False)

    x_wait(2)

    @pl.when(rim)
    def _():
        z_own(2, 1, True)

    @pl.when(middle)
    def _():
        x_wait(3)
        z_own(2, 1, True, False, flows=(1,))
        z_own(3, 1, True, flows=(1,))

    relay_out(2, 0, 0, (1,))
    z_final(1)

    @pl.when(rim)
    def _():
        project_state()

    state_in = sums[0].astype(bf16)
    relay_in(3, 1, (1,))
    signal = dot(order[0], state_in).astype(bf16)
    for i in range(2):
        push[i] = dot(signal, dmat[i, 0]) + dot(signal, dmat[i, 1])
    decay_real = jnp.broadcast_to(dec_ref[0:1, :], (CHUNKS, columns))
    decay_imag = jnp.broadcast_to(dec_ref[1:2, :], (CHUNKS, columns))

    def advance(p, carry):
        cut = pl.ds(pl.multiple_of(p * CHUNKS, CHUNKS), CHUNKS)
        real, imag = cmul(decay_real, decay_imag, *carry)
        real, imag = real + push[0, cut, :], imag + push[1, cut, :]
        push[0, cut, :] = real
        push[1, cut, :] = imag
        return real, imag

    zero = jnp.zeros((CHUNKS, columns), f32)
    end_real, end_imag = lax.fori_loop(0, span, advance, (zero, zero), unroll=4)

    def power(real, imag, count):
        out = None
        while count:
            if count % 2:
                out = (real, imag) if out is None else cmul(*out, real, imag)
            real, imag = cmul(real, imag, real, imag)
            count //= 2
        return out

    chunk_decay = power(dec_ref[0:1, :], dec_ref[1:2, :], span)
    block_decay = power(*chunk_decay, CHUNKS)
    row_zero = jnp.zeros((1, columns), f32)
    total = (row_zero, row_zero)
    for j in range(CHUNKS):
        moved = cmul(*chunk_decay, *total)
        total = (moved[0] + end_real[j : j + 1], moved[1] + end_imag[j : j + 1])
    which = iota((CHUNKS, columns), 0)
    ends[z] = jnp.where(which == 0, total[0], jnp.where(which == 1, total[1], 0.0))

    def end_copy(k):
        return remote(ends.at[z], ends.at[z], end_send.at[k - 1], end_recv.at[k - 1], (me + k * n_x, tp))

    for k in range(1, n_z):
        @pl.when(inside(z + k))
        def _():
            end_copy(k).start()

    @pl.when(middle)
    def _():
        for p in range(HALVES):
            here = guests.region(tp, x, p)
            with jax.named_scope("guest_wait"):
                remote(here, here, guest_z_send.at[0], guest_z_recv.at[p], to_pair).wait_recv()
            guests.start(0, 1, 3, p=p)

    @pl.when(middle)
    def _():
        z_own(2, 1, True, False, flows=(0,))
        z_own(3, 1, True, flows=(0,))

    relay_in(3, 1, (0,))
    relay_out(2, 0, 0, (0,))
    relay_out(2, 1, 0)

    @pl.when(middle)
    def _():
        for p in range(HALVES):
            acts[1].relay_x(p)
            acts[1].relay_y(p)

    relay_in(2, 1)
    relay_out(2, 0, 1, (1,))

    @pl.when(middle)
    def _():
        for p in range(HALVES):
            acts[1].relay_both(p)


    @pl.when(middle)
    def _():
        for p in range(HALVES):
            guests.relay_x(p)
            guests.relay_y(p)

    for k in range(1, n_z):
        @pl.when(inside(z - k))
        @jax.named_scope("ends_wait")
        def _():
            there = ends.at[z - k]
            remote(there, there, end_send.at[k - 1], end_recv.at[k - 1], to_z(1)).wait_recv()

    total = (row_zero, row_zero)
    for s in range(n_z - 1):
        moved = cmul(*block_decay, *total)
        use = s < z
        total = (
            jnp.where(use, moved[0] + ends[s, 0:1, :], total[0]),
            jnp.where(use, moved[1] + ends[s, 1:2, :], total[1]),
        )
    begin_real, begin_imag = zero, zero
    for j in range(CHUNKS):
        begin_real = jnp.where(which == j, total[0], begin_real)
        begin_imag = jnp.where(which == j, total[1], begin_imag)
        moved = cmul(*chunk_decay, *total)
        total = (moved[0] + end_real[j : j + 1], moved[1] + end_imag[j : j + 1])

    def add_carry(p, carry):
        cut = pl.ds(pl.multiple_of(p * CHUNKS, CHUNKS), CHUNKS)
        real, imag = cmul(decay_real, decay_imag, *carry)
        push[0, cut, :] = push[0, cut, :] + real
        push[1, cut, :] = push[1, cut, :] + imag
        return real, imag

    lax.fori_loop(0, span, add_carry, (begin_real, begin_imag), unroll=4)
    real_high, real_low = split(push[0])
    imag_high, imag_low = split(push[1])
    readout = dot(real_high, rmat[0, 0]) + dot(real_high, rmat[0, 1]) + dot(real_low, rmat[0, 0])
    readout -= dot(imag_high, rmat[1, 0]) + dot(imag_high, rmat[1, 1]) + dot(imag_low, rmat[1, 0])
    skip = skip_ref[:, aligned(q, width)]
    readout += skip * signal.astype(f32)
    shuffled = jax.nn.gelu(readout).astype(bf16)
    act[0, :, aligned(q, width)] = dot(order[1], shuffled).astype(bf16)
    for p in range(HALVES):
        acts[0].start(0, 1, 3, p=p)

    relay_out(2, 0, 1, (0,))
    relay_out(2, 1, 1)

    @pl.when(middle)
    def _():
        for p in range(HALVES):
            guests.relay_both(p)
        guests.wait_pair(pair, 0)
        guests.wait_pair(both, 1)

    z_final(3)

    @pl.when(middle)
    def _():
        for first in (True, False):
            cut = aligned(1 - x if first else x, rows)
            for j in range(chunk_count):
                partial[j, cut] = dot(guest[cut], w_out[1, j]).astype(bf16)
                part_copy(j, first).start()

    for p in range(HALVES):
        acts[0].relay_x(p)
        acts[0].relay_y(p)
        if p == 0:
            @pl.when(middle)
            def _():
                acts[1].wait_pair(pair, 0)
                acts[1].wait_pair(both, 1)
                for j in range(chunk_count):
                    sums[j] = dot(act[1], w_out[1, j])
    for p in range(HALVES):
        acts[0].relay_both(p)

    acts[0].wait_pair(pair, 0)
    acts[0].wait_pair(both, 1)
    z_final(2)

    def out_columns(half, j):
        return pl.ds(pl.multiple_of(half * out_width + j * LANES, LANES), LANES)

    def out_copy(j):
        return remote(made.at[j], out_ref.at[:, out_columns(x, j)], out_send.at[0], out_recv.at[0], to_x)

    here, there = aligned(x, rows), aligned(1 - x, rows)

    @pl.when(middle)
    def _():
        for j in range(chunk_count):
            made[j] = (dot(act[0, there], w_out[0, j]) + sums[j, there]).astype(bf16)
            out_copy(j).start()
        for j in range(chunk_count):
            mine = dot(act[0, here], w_out[0, j]) + sums[j, here]
            out_ref[:, out_columns(x, j)] = mine.astype(bf16)

    @pl.when(rim)
    def _():
        for cut in (there, here):
            for j in range(chunk_count):
                sums[j, cut] = dot(act[0, cut], w_out[0, j])

        @jax.named_scope("partial_wait")
        def part_wait(j, first):
            part = part_rows(j, first)
            recv = part_recv.at[j, 0 if first else 1]
            remote(part, part, part_send.at[0], recv, to_pair).wait_recv()

        for j in range(chunk_count):
            part_wait(j, True)
            made[j] = (sums[j, there] + partial[j, there].astype(f32)).astype(bf16)
            out_copy(j).start()
        for j in range(chunk_count):
            part_wait(j, False)
            out_ref[:, out_columns(x, j)] = (sums[j, here] + partial[j, here].astype(f32)).astype(bf16)

    @jax.named_scope("drain")
    def drain():
        sent = w_in.at[0, pl.ds(0, 2 * in_rows + 2 * chunk_count * out_rows)]
        remote(sent, sent, xw_send.at[0], xw_recv.at[0], to_x).wait_send()
        few = n_x * (2 * in_rows + chunk_count * out_rows)
        many = few + n_x * chunk_count * out_rows
        for d in range(2):
            for s in range(n_z - 1):
                any_sent = jnp.logical_and(inside(z + ways[d]), inside(z - ways[d] * s))
                for count, case in ((many, inner(z + ways[d])), (few, jnp.logical_not(inner(z + ways[d])))):
                    @pl.when(jnp.logical_and(any_sent, case))
                    def _():
                        sent = w_in.at[0, pl.ds(0, count)]
                        remote(sent, sent, z_send.at[d, s], z_recv.at[0, 0, 0], to_z(ways[d])).wait_send()
        tokens.drain(scaled.at[pl.ds(0, 7 * rows // n_tp)])
        acts[0].drain(act.at[0, :, pl.ds(0, 7 * width)])

        @pl.when(middle)
        def _():
            acts[1].drain(act.at[1, :, pl.ds(0, 7 * width)])
            guests.drain(guest.at[:, pl.ds(0, 7 * width)])
            remote(partial, partial, part_send.at[0], part_recv.at[0, 0], to_pair).wait_send()

        @pl.when(rim)
        def _():
            sent = act.at[1, :, aligned(q, width)]
            remote(sent, sent, guest_z_send.at[0], guest_z_recv.at[0], to_pair).wait_send()

        @pl.when(inside(z + 1))
        def _():
            halo_copy.wait_send()

        for k in range(1, n_z):
            @pl.when(inside(z + k))
            def _():
                end_copy(k).wait_send()

        remote(made, made, out_send.at[0], out_recv.at[0], to_x).wait_send()

    drain()
    with jax.named_scope("out_wait"):
        here = out_ref.at[:, aligned(1 - x, out_width)]
        remote(here, here, out_send.at[0], out_recv.at[0], to_x).wait_recv()


def slab_call(n_sp, n_tp, n_x, arrays):
    tokens, state_in_weight, state_out_weight = arrays[0], arrays[2], arrays[14]
    rows, features = tokens.shape
    in_rows, width = state_in_weight.shape
    out_rows, out_columns = state_out_weight.shape
    width //= n_x
    n_z, slab, chunk_count = n_sp // n_x, rows * n_x, out_columns // n_x // LANES
    groups, states = width // SSM_GROUP, arrays[4].shape[1]
    columns, pool_groups = groups * states, width // POOL_GROUP
    vmem = pl.BlockSpec(memory_space=pltpu.VMEM)
    anywhere = pl.BlockSpec(memory_space=pl.ANY)
    dma = pltpu.SemaphoreType.DMA
    return pl.pallas_call(
        functools.partial(slab_kernel, n_sp, n_tp, n_x, states),
        out_shape=pltpu.VMEM((rows, out_columns), bf16),
        in_specs=[anywhere, vmem] + [anywhere] * 4 + [vmem] + [anywhere] * 4 + [vmem, anywhere, vmem]
        + [anywhere] * 2,
        out_specs=vmem,
        scratch_shapes=[
            pltpu.VMEM((n_tp, slab, features), bf16),
            pltpu.VMEM((slab, features * n_tp), bf16),
            pltpu.VMEM((slab, LANES), f32),
            pltpu.VMEM((2, n_sp * in_rows, width), bf16),
            pltpu.VMEM((2, chunk_count, n_sp * out_rows, LANES), bf16),
            pltpu.VMEM((2, 2, width, columns), bf16),
            pltpu.VMEM((2, 2, columns, width), bf16),
            pltpu.VMEM((width, width), bf16),
            pltpu.VMEM((2, slab, columns), f32),
            pltpu.VMEM((2, slab, slab), bf16),
            pltpu.VMEM((window_reach, width), bf16),
            pltpu.VMEM((window_reach, width), bf16),
            pltpu.VMEM((n_z, CHUNKS, columns), f32),
            pltpu.VMEM((2, slab, n_tp * n_x * width), bf16),
            pltpu.VMEM((slab, n_tp * n_x * width), bf16),
            pltpu.VMEM((chunk_count, slab, LANES), bf16),
            pltpu.VMEM((chunk_count, slab, LANES), f32),
            pltpu.VMEM((chunk_count, rows, LANES), bf16),
            pltpu.VMEM((2, groups, states), f32),
            pltpu.VMEM((4, groups, SSM_GROUP, states), f32),
            pltpu.VMEM((pool_groups, POOL_GROUP, POOL_GROUP), bf16),
            pltpu.VMEM((2, columns), f32),
            dma((8,)),
            dma((1,)),
            dma((4,)),
            dma((2, n_z - 1)),
            dma((4, n_z, 2)),
            dma((1,)),
            dma((8,)),
            dma((2,)),
            dma((2, 8)),
            dma((2,)),
            dma((n_z - 1,)),
            dma((n_z - 1,)),
            dma((1,)),
            dma((1,)),
            dma((1,)),
            dma((8,)),
            dma((1,)),
            dma((HALVES,)),
            dma((1,)),
            dma((chunk_count, 2)),
        ],
        compiler_params=pltpu.CompilerParams(
            collective_id=0, has_side_effects=True, vmem_limit_bytes=60 * 2**20
        ),
    )(*arrays)


def slab_fits(n_sp, n_tp, n_x, features, in_rows, width, pool_width, out_rows, out_columns):
    return (
        n_x == 2 and n_tp == 4 and n_sp // n_x == 4 and features % LANES == 0 and width == n_x * LANES
        and pool_width == width and out_columns % (n_x * LANES) == 0
        and n_x * (2 * in_rows + out_columns // (n_x * LANES) * 2 * out_rows) <= n_sp * in_rows
    )


def body(
    n_sp, n_tp, n_x,
    tokens, norm_gain, state_in_weight, pool_in_weight, rate_real, rate_imag, log_step,
    input_real, input_imag, output_real, output_imag, skip_gain, pool_weight, pool_gain,
    state_out_weight, pool_out_weight,
):
    rows, features = tokens.shape
    in_rows, width = state_in_weight.shape
    pool_width = pool_in_weight.shape[1]
    out_rows, out_columns = state_out_weight.shape
    groups = width // SSM_GROUP
    states = rate_real.shape[1]
    columns = groups * states
    pool_groups = pool_width // POOL_GROUP
    if slab_fits(n_sp, n_tp, n_x, features, in_rows, width, pool_width, out_rows, out_columns):
        return slab_call(n_sp, n_tp, n_x, (
            tokens, norm_gain[None], state_in_weight, pool_in_weight, rate_real, rate_imag, log_step[None],
            jnp.swapaxes(input_real, 1, 2), jnp.swapaxes(input_imag, 1, 2), output_real, output_imag,
            skip_gain[None], pool_weight, pool_gain[None], state_out_weight, pool_out_weight,
        ))
    vmem = pl.BlockSpec(memory_space=pltpu.VMEM)
    anywhere = pl.BlockSpec(memory_space=pl.ANY)
    dma = pltpu.SemaphoreType.DMA
    return pl.pallas_call(
        functools.partial(kernel, n_sp, n_tp, n_x, states),
        out_shape=jax.ShapeDtypeStruct((rows, out_columns), bf16),
        in_specs=[anywhere, vmem] + [anywhere] * 4 + [vmem] + [anywhere] * 4 + [vmem, anywhere, vmem]
        + [anywhere] * 2,
        out_specs=vmem,
        scratch_shapes=[
            pltpu.VMEM((n_tp, rows, features), bf16),
            pltpu.VMEM((n_sp * in_rows, width), bf16),
            pltpu.VMEM((n_sp * in_rows, pool_width), bf16),
            pltpu.VMEM((n_sp * out_rows, out_columns), bf16),
            pltpu.VMEM((n_sp * out_rows, out_columns), bf16),
            pltpu.VMEM((rows, features * n_tp), bf16),
            pltpu.VMEM((2, 2, width, columns), bf16),
            pltpu.VMEM((2, 2, columns, width), bf16),
            pltpu.VMEM((pool_width, pool_width), bf16),
            pltpu.VMEM((2, rows, columns), f32),
            pltpu.VMEM((rows + window_reach, pool_width), bf16),
            pltpu.VMEM((window_reach, pool_width), bf16),
            pltpu.VMEM((n_sp, CHUNKS, columns), f32),
            pltpu.VMEM((2, n_tp, rows, width), bf16),
            pltpu.VMEM((rows, width), bf16),
            pltpu.VMEM((rows, pool_width), bf16),
            pltpu.VMEM((window_reach, pool_width), bf16),
            pltpu.VMEM((2, groups, states), f32),
            pltpu.VMEM((4, groups, SSM_GROUP, states), f32),
            pltpu.VMEM((pool_groups, POOL_GROUP, POOL_GROUP), bf16),
            pltpu.VMEM((2, columns), f32),
            dma((12,)),
            dma((4, 2, n_sp // 2, PIECES)),
            dma((4, 2, n_sp // 2, PIECES)),
            dma((n_tp - 1,)),
            dma((n_tp - 1,)),
            dma((2, n_tp - 1)),
            dma((2, n_tp - 1)),
            dma((2,)),
            dma((n_sp - 1,)),
            dma((n_sp - 1,)),
        ],
        compiler_params=pltpu.CompilerParams(
            collective_id=0, has_side_effects=True, vmem_limit_bytes=60 * 2**20
        ),
    )(
        tokens, norm_gain[None], state_in_weight, pool_in_weight, rate_real, rate_imag, log_step[None],
        jnp.swapaxes(input_real, 1, 2), jnp.swapaxes(input_imag, 1, 2), output_real, output_imag,
        skip_gain[None], pool_weight, pool_gain[None], state_out_weight, pool_out_weight,
    )


def solution(mesh):
    n_sp, n_tp = mesh.shape["sp"], mesh.shape["tp"]
    n_x = 2 ** ((n_sp.bit_length() - 1) // 2)
    both, whole = P("sp", "tp"), P()
    return jax.shard_map(
        functools.partial(body, n_sp, n_tp, n_x),
        mesh=mesh,
        in_specs=(both, whole, both, both) + (whole,) * 10 + (both, both),
        out_specs=both,
        check_vma=False,
    )
```

```python
import functools

import jax
import jax.numpy as jnp
from jax import lax
from jax.experimental import pallas as pl
from jax.experimental.pallas import tpu as pltpu
from jax.sharding import PartitionSpec as P

SSM_GROUP = 16
POOL_GROUP = 64
CHUNKS = 8
PIECES = 2

epsilon = 1e-06
window_reach = 16
f32, bf16 = jnp.float32, jnp.bfloat16
MESH = pl.DeviceIdType.MESH


def discretize(rate_real, rate_imag, log_step, length):
    step_size = jnp.exp(log_step)[:, None] / length
    exponent = rate_real * step_size
    angle = rate_imag * step_size
    magnitude = jnp.exp(exponent)
    decay_real = magnitude * jnp.cos(angle)
    decay_imag = magnitude * jnp.sin(angle)
    less_one = jnp.expm1(exponent) * jnp.cos(angle) - 2.0 * jnp.square(jnp.sin(0.5 * angle))
    denominator = rate_real * rate_real + rate_imag * rate_imag
    factor_real = (less_one * rate_real + decay_imag * rate_imag) / denominator
    factor_imag = (decay_imag * rate_real - less_one * rate_imag) / denominator
    return decay_real, decay_imag, factor_real, factor_imag


def iota(shape, axis):
    return lax.broadcasted_iota(jnp.int32, shape, axis)


def dot(a, b):
    return jnp.dot(a, b, preferred_element_type=f32)


def dot_nt(a, b):
    return lax.dot_general(a, b, (((1,), (1,)), ((), ())), preferred_element_type=f32)


def split(a):
    high = a.astype(bf16)
    return high, (a - high.astype(f32)).astype(bf16)


def cmul(ar, ai, br, bi):
    return ar * br - ai * bi, ar * bi + ai * br


def kernel(
    n_sp, n_tp, n_x, states,
    tok_ref, gain_ref, wsi_ref, wpi_ref, rr_ref, ri_ref, step_ref, inr_ref, ini_ref, outr_ref,
    outi_ref, skip_ref, pw_ref, pg_ref, wso_ref, wpo_ref,
    out_ref,
    tok_full, wsi, wpi, wso, wpo, scaled, dmat, rmat, pmat, push, ext, halo, ends, act,
    mine_s, mine_p, halo_out, rates, matrices, pool_own, dec_ref,
    own_sem, ring_send, ring_recv, tok_send, tok_recv, act_send, act_recv, halo_sem, end_send, end_recv,
):
    me, tp = lax.axis_index("sp"), lax.axis_index("tp")
    n_z = n_sp // n_x
    rows = tok_ref.shape[0]
    features = tok_ref.shape[1]
    width = wsi_ref.shape[1]
    pool_width = wpi_ref.shape[1]
    groups = width // SSM_GROUP
    columns = groups * states
    pool_groups = pool_width // POOL_GROUP
    span = rows // CHUNKS

    def place(p):
        x, r = p // n_z, p % n_z
        return (r + (x % 2) * (n_z - 1 - 2 * r)) * n_x + x

    my_x, my_z = me % n_x, me // n_x
    at = my_x * n_z + my_z + (my_x % 2) * (n_z - 1 - 2 * my_z)

    barrier = pltpu.get_barrier_semaphore()
    for k in range(1, n_sp):
        pl.semaphore_signal(barrier, inc=1, device_id=((me + k) % n_sp, tp), device_id_type=MESH)
    for k in range(1, n_tp):
        pl.semaphore_signal(barrier, inc=1, device_id=(me, (tp + k) % n_tp), device_id_type=MESH)

    fulls = ((wsi_ref, wsi), (wpi_ref, wpi), (wso_ref, wso), (wpo_ref, wpo))
    owns = []
    for a, (own, full) in enumerate(fulls):
        count = own.shape[0]
        owns.append(
            pltpu.make_async_copy(
                own, full.at[pl.ds(pl.multiple_of(me * count, count), count)], own_sem.at[a]
            )
        )
    owns.append(pltpu.make_async_copy(tok_ref, tok_full.at[tp], own_sem.at[4]))
    def heads(ref, count):
        return ref.at[pl.ds(pl.multiple_of(tp * count, count), count)]

    loads = [
        pltpu.make_async_copy(heads(ref, groups), there, own_sem.at[5 + k])
        for k, (ref, there) in enumerate(
            (
                (rr_ref, rates.at[0]), (ri_ref, rates.at[1]), (inr_ref, matrices.at[0]),
                (ini_ref, matrices.at[1]), (outr_ref, matrices.at[2]), (outi_ref, matrices.at[3]),
            )
        )
    ]
    loads.append(pltpu.make_async_copy(heads(pw_ref, pool_groups), pool_own, own_sem.at[11]))
    for c in owns + loads:
        c.start()
    pl.semaphore_wait(barrier, n_sp - 1 + n_tp - 1)

    ways = (1, -1)

    def reach_of(a, d):
        return n_sp // 2 if a % 2 == d else n_sp - 1 - n_sp // 2

    def part(a, d, s, h):
        own, full = fulls[a]
        count = own.shape[0]
        size = count // PIECES
        way = ways[d]
        owner = place((at - way * s + n_sp) % n_sp)
        there = full.at[pl.ds(pl.multiple_of(owner * count + h * size, size), size)]
        source = own.at[pl.ds(h * size, size)] if s == 0 else there
        return source, there, (place((at + way + n_sp) % n_sp), tp)

    def sender(a, d, s, h):
        source, there, target = part(a, d, s, h)
        return pltpu.make_async_remote_copy(
            source, there, ring_send.at[a, d, s, h], ring_recv.at[a, d, s, h],
            device_id=target, device_id_type=MESH,
        )

    def arrive(a, d, s, h):
        _, there, target = part(a, d, s + 1, h)
        pltpu.make_async_remote_copy(
            there, there, ring_send.at[a, d, s, h], ring_recv.at[a, d, s, h],
            device_id=target, device_id_type=MESH,
        ).wait_recv()

    longest = n_sp // 2

    def ring(phase, s, h):
        streams = [
            (a, d) for a in (2 * phase, 2 * phase + 1) for d in range(2) if s < reach_of(a, d)
        ]
        for a, d in sorted(streams, key=lambda i: -reach_of(*i)):
            arrive(a, d, s, h)
            if s + 1 < reach_of(a, d):
                sender(a, d, s + 1, h).start()
        if phase == 0 and h == PIECES - 1:
            for a, d in streams:
                if s + 1 == reach_of(a, d):
                    for g in range(PIECES):
                        sender(a + 2, d, 0, g).start()

    turns = [(phase, s, h) for phase in range(2) for s in range(longest) for h in range(PIECES)]
    turn = [0]

    def step(stop=len(turns)):
        if turn[0] < stop:
            ring(*turns[turn[0]])
            turn[0] += 1

    def token_copy(k):
        return pltpu.make_async_remote_copy(
            tok_ref, tok_full.at[tp], tok_send.at[k - 1], tok_recv.at[k - 1],
            device_id=(me, (tp + k) % n_tp), device_id_type=MESH,
        )

    for h in range(PIECES):
        for a, d in ((0, 0), (1, 1), (0, 1), (1, 0)):
            sender(a, d, 0, h).start()
    for k in range(1, n_tp):
        token_copy(k).start()

    tile = iota((states, columns), 0) == iota((states, columns), 1) % states
    tile_exact, tile_half = tile.astype(f32), tile.astype(bf16)

    def exactly(a, b):
        return jnp.dot(a, b, precision=lax.Precision.HIGHEST, preferred_element_type=f32)

    factors = []

    def build_decay():
        for c in loads:
            c.wait()
        own_head = iota((groups, columns), 0) == iota((groups, columns), 1) // states

        def flat(a):
            return jnp.sum(jnp.where(own_head, exactly(a, tile_exact), 0.0), axis=0, keepdims=True)

        rate_real, rate_imag = flat(rates[0]), flat(rates[1])
        all_groups = step_ref.shape[1]
        head = iota((all_groups, columns), 0) == tp * groups + iota((all_groups, columns), 1) // states
        log_step = exactly(jnp.broadcast_to(step_ref[...], (8, all_groups)), head.astype(f32))[0:1]
        step_size = jnp.exp(log_step) / (rows * n_sp)
        exponent, angle = rate_real * step_size, rate_imag * step_size
        magnitude = jnp.exp(exponent)
        cosine = jnp.cos(angle)
        decay_real, decay_imag = magnitude * cosine, magnitude * jnp.sin(angle)
        series = jnp.ones_like(exponent)
        for k in range(10, 1, -1):
            series = 1.0 + series * exponent * (1.0 / k)
        growth = jnp.where(jnp.abs(exponent) < 0.5, exponent * series, magnitude - 1.0)
        less_one = growth * cosine - 2.0 * jnp.square(jnp.sin(0.5 * angle))
        denominator = rate_real * rate_real + rate_imag * rate_imag
        factors.append((less_one * rate_real + decay_imag * rate_imag) / denominator)
        factors.append((decay_imag * rate_real - less_one * rate_imag) / denominator)
        dec_ref[0:1, :] = decay_real
        dec_ref[1:2, :] = decay_imag

    def spread(k):
        high, low = split(matrices[k].reshape(width, states))
        return dot(high, tile_half) + dot(low, tile_half)

    def build_drive(i):
        same = iota((width, columns), 0) // SSM_GROUP == iota((width, columns), 1) // states
        real, imag = spread(0), spread(1)
        if i == 0:
            drive = factors[0] * real - factors[1] * imag
        else:
            drive = factors[0] * imag + factors[1] * real
        for j, piece in enumerate(split(jnp.where(same, drive, 0.0))):
            dmat[i, j] = piece

    def build_read(i):
        across = (iota((columns, states), 0) % states == iota((columns, states), 1)).astype(bf16)
        same = iota((columns, width), 0) // states == iota((columns, width), 1) // SSM_GROUP
        for j, piece in enumerate(split(matrices[2 + i].reshape(width, states))):
            rmat[i, j] = jnp.where(same, dot_nt(across, piece), 0.0).astype(bf16)

    def build_pool():
        across = (
            iota((POOL_GROUP, pool_width), 0) == iota((POOL_GROUP, pool_width), 1) % POOL_GROUP
        ).astype(bf16)
        same = iota((pool_width, pool_width), 0) // POOL_GROUP == iota((pool_width, pool_width), 1) // POOL_GROUP
        own = pool_own[...].reshape(pool_width, POOL_GROUP)
        pmat[...] = jnp.where(same, dot(own, across), 0.0).astype(bf16)

    squares = []

    def take(t):
        block = tok_full[t].astype(f32)
        squares.append(jnp.sum(block * block, axis=1, keepdims=True))
        cut = slice(t * features, (t + 1) * features)
        scaled[:, cut] = (block * gain_ref[:, cut]).astype(bf16)

    def tokens_in():
        owns[4].wait()
        for k in range(1, n_tp):
            pltpu.make_async_remote_copy(
                tok_ref, tok_full.at[(tp - k + n_tp) % n_tp], tok_send.at[k - 1], tok_recv.at[k - 1],
                device_id=(me, (tp + k) % n_tp), device_id_type=MESH,
            ).wait_recv()

    half = len(turns) // 2
    for at_work, work in enumerate(
        (
            build_decay, lambda: build_drive(0), lambda: build_drive(1), lambda: build_read(0),
            lambda: build_read(1), build_pool,
        )
    ):
        work()
        if at_work in (0, 1, 3, 5):
            step(half)
    while turn[0] < half - 3:
        step(half)
    tokens_in()
    for t in range(n_tp):
        take(t)
        if t == n_tp // 2 - 1:
            step(half)
    while turn[0] < half:
        step(half)
    owns[0].wait()
    owns[1].wait()
    inverse = lax.rsqrt(sum(squares) / (features * n_tp) + epsilon)
    state_in = (dot(scaled[...], wsi[...]) * inverse).astype(bf16)
    pool_in = (dot(scaled[...], wpi[...]) * inverse).astype(bf16)
    ext[window_reach:] = pool_in
    halo_out[...] = pool_in[rows - window_reach :]
    halo_copy = pltpu.make_async_remote_copy(
        halo_out, halo, halo_sem.at[0], halo_sem.at[1],
        device_id=((me + 1) % n_sp, tp), device_id_type=MESH,
    )
    shuffle = (
        iota((rows, rows), 1)
        == (iota((rows, rows), 0) % CHUNKS) * span + iota((rows, rows), 0) // CHUNKS
    ).astype(bf16)
    signal = dot(shuffle, state_in).astype(bf16)
    for i in range(2):
        push[i] = dot(signal, dmat[i, 0]) + dot(signal, dmat[i, 1])
        if i == 0:
            halo_copy.start()
        else:
            step()
    decay_real = jnp.broadcast_to(dec_ref[0:1, :], (CHUNKS, columns))
    decay_imag = jnp.broadcast_to(dec_ref[1:2, :], (CHUNKS, columns))

    def advance(p, carry):
        cut = pl.ds(pl.multiple_of(p * CHUNKS, CHUNKS), CHUNKS)
        real, imag = cmul(decay_real, decay_imag, *carry)
        real, imag = real + push[0, cut, :], imag + push[1, cut, :]
        push[0, cut, :] = real
        push[1, cut, :] = imag
        return real, imag

    zero = jnp.zeros((CHUNKS, columns), f32)
    end_real, end_imag = lax.fori_loop(0, span, advance, (zero, zero))

    def power(real, imag, count):
        out = None
        while count:
            if count % 2:
                out = (real, imag) if out is None else cmul(*out, real, imag)
            real, imag = cmul(real, imag, real, imag)
            count //= 2
        return out

    chunk_decay = power(dec_ref[0:1, :], dec_ref[1:2, :], span)
    block_decay = power(*chunk_decay, CHUNKS)
    row_zero = jnp.zeros((1, columns), f32)
    total = (row_zero, row_zero)
    for j in range(CHUNKS):
        moved = cmul(*chunk_decay, *total)
        total = (moved[0] + end_real[j : j + 1], moved[1] + end_imag[j : j + 1])
    which = iota((CHUNKS, columns), 0)
    ends[me] = jnp.where(which == 0, total[0], jnp.where(which == 1, total[1], 0.0))

    def end_copy(k):
        return pltpu.make_async_remote_copy(
            ends.at[me], ends.at[me], end_send.at[k - 1], end_recv.at[k - 1],
            device_id=((me + k) % n_sp, tp), device_id_type=MESH,
        )

    for k in range(1, n_sp):
        end_copy(k).start()

    halo_copy.wait_recv()
    ext[:window_reach] = jnp.where(me == 0, jnp.zeros_like(halo), halo[...])
    group = tp * (pool_width // POOL_GROUP) + iota((rows, pool_width), 1) // POOL_GROUP
    window = jnp.left_shift(jnp.ones_like(group), group % 4 + 1)
    targets = iota((rows, rows + window_reach), 0) + window_reach
    sources = iota((rows, rows + window_reach), 1)
    whole = ext[...]
    sums = jnp.zeros((rows, pool_width), f32)
    for power_index in range(1, 5):
        reach = 2**power_index
        band = ((sources <= targets) & (sources > targets - reach)).astype(bf16)
        sums = jnp.where(window == reach, dot(band, whole), sums)
        if power_index == 2:
            step()
    position = me * rows + iota((rows, pool_width), 0)
    divisor = jnp.minimum(position + 1, window).astype(f32)
    pooled = sums / divisor - ext[window_reach:].astype(f32)
    pooled_high, pooled_low = split(pooled)
    pool_gain = pg_ref[:, pl.ds(pl.multiple_of(tp * pool_width, pool_width), pool_width)]
    projected = dot(pooled_high, pmat[...]) + dot(pooled_low, pmat[...])
    mine_p[...] = (projected * pool_gain).astype(bf16)
    step()

    def act_copy(which, k, source):
        mine = mine_s if which == 0 else mine_p
        return pltpu.make_async_remote_copy(
            mine, act.at[which, source], act_send.at[which, k - 1], act_recv.at[which, k - 1],
            device_id=(me, (tp + k) % n_tp), device_id_type=MESH,
        )

    for k in range(1, n_tp):
        act_copy(1, k, tp).start()
    act[1, tp] = mine_p[...]

    for k in range(1, n_sp):
        there = ends.at[(me - k + n_sp) % n_sp]
        pltpu.make_async_remote_copy(
            there, there, end_send.at[k - 1], end_recv.at[k - 1],
            device_id=((me + k) % n_sp, tp), device_id_type=MESH,
        ).wait_recv()
    total = (row_zero, row_zero)
    for s in range(n_sp - 1):
        moved = cmul(*block_decay, *total)
        use = s < me
        total = (
            jnp.where(use, moved[0] + ends[s, 0:1, :], total[0]),
            jnp.where(use, moved[1] + ends[s, 1:2, :], total[1]),
        )
    begin_real, begin_imag = zero, zero
    for j in range(CHUNKS):
        begin_real = jnp.where(which == j, total[0], begin_real)
        begin_imag = jnp.where(which == j, total[1], begin_imag)
        moved = cmul(*chunk_decay, *total)
        total = (moved[0] + end_real[j : j + 1], moved[1] + end_imag[j : j + 1])

    def add_carry(p, carry):
        cut = pl.ds(pl.multiple_of(p * CHUNKS, CHUNKS), CHUNKS)
        real, imag = cmul(decay_real, decay_imag, *carry)
        push[0, cut, :] = push[0, cut, :] + real
        push[1, cut, :] = push[1, cut, :] + imag
        return real, imag

    lax.fori_loop(0, span, add_carry, (begin_real, begin_imag))
    step()
    real_high, real_low = split(push[0])
    imag_high, imag_low = split(push[1])
    readout = dot(real_high, rmat[0, 0]) + dot(real_high, rmat[0, 1]) + dot(real_low, rmat[0, 0])
    step()
    readout -= dot(imag_high, rmat[1, 0]) + dot(imag_high, rmat[1, 1]) + dot(imag_low, rmat[1, 0])
    skip = skip_ref[:, pl.ds(pl.multiple_of(tp * width, width), width)]
    readout += skip * signal.astype(f32)
    shuffled = jax.nn.gelu(readout).astype(bf16)
    restore = (
        iota((rows, rows), 0)
        == (iota((rows, rows), 1) % CHUNKS) * span + iota((rows, rows), 1) // CHUNKS
    ).astype(bf16)
    mine_s[...] = dot(restore, shuffled).astype(bf16)
    for k in range(1, n_tp):
        act_copy(0, k, tp).start()
    act[0, tp] = mine_s[...]
    while turn[0] < len(turns):
        step()
    for which in (1, 0):
        for k in range(1, n_tp):
            act_copy(which, k, (tp - k + n_tp) % n_tp).wait_recv()
    owns[2].wait()
    owns[3].wait()
    result = None
    for t in range(n_tp):
        for which, full, size in ((1, wpo, pool_width), (0, wso, width)):
            term = dot(act[which, t], full[t * size : (t + 1) * size, :])
            result = term if result is None else result + term
    out_ref[...] = result.astype(bf16)

    for a in range(4):
        for d in range(2):
            for s in range(reach_of(a, d)):
                for h in range(PIECES):
                    sender(a, d, s, h).wait_send()
    for k in range(1, n_tp):
        token_copy(k).wait_send()
        act_copy(0, k, tp).wait_send()
        act_copy(1, k, tp).wait_send()
    halo_copy.wait_send()
    for k in range(1, n_sp):
        end_copy(k).wait_send()

LANES = 128
HALVES = 2


def slab_kernel(
    n_sp, n_tp, n_x, states,
    tok_ref, gain_ref, wsi_ref, wpi_ref, rr_ref, ri_ref, step_ref, inr_ref, ini_ref, outr_ref,
    outi_ref, skip_ref, pw_ref, pg_ref, wso_ref, wpo_ref,
    out_ref,
    tok, scaled, squares, w_in, w_out, dmat, rmat, pmat, push, order, halo, halo_out, ends, act,
    guest, partial, sums, made, rates, matrices, pool_own, dec_ref,
    own_sem, xw_send, xw_recv, z_send, z_recv, tok_send, tok_recv, act_send, act_recv, halo_sem, end_send, end_recv,
    out_send, out_recv, guest_send, guest_recv, guest_z_send, guest_z_recv, part_send, part_recv,
):
    me, tp = lax.axis_index("sp"), lax.axis_index("tp")
    n_z = n_sp // n_x
    z, x = me // n_x, me % n_x
    y, core = tp // 2, tp % 2
    rows = tok_ref.shape[0]
    slab = rows * n_x
    features = tok_ref.shape[1]
    in_rows = wsi_ref.shape[0]
    out_rows = wso_ref.shape[0]
    width = wsi_ref.shape[1] // n_x
    out_width = wso_ref.shape[1] // n_x
    chunk_count = out_width // LANES
    groups = width // SSM_GROUP
    columns = groups * states
    pool_groups = width // POOL_GROUP
    span = slab // CHUNKS
    q = tp * n_x + x

    across, pair, both = (1 - y) * 2 + core, y * 2 + 1 - core, (1 - y) * 2 + 1 - core
    beside = me + 1 - 2 * x
    to_x, to_y, to_pair = (beside, tp), (me, across), (me, pair)
    ways = (1, -1)

    def to_z(way):
        return (me + way * n_x, tp)

    def inside(at):
        return jnp.logical_and(at >= 0, at < n_z)

    def inner(at):
        return jnp.logical_and(at > 0, at < n_z - 1)

    middle, rim = inner(z), jnp.logical_not(inner(z))
    inward, outward = jnp.where(z == 0, 1, -1), jnp.where(z == 1, -1, 1)

    def aligned(index, size):
        return pl.ds(pl.multiple_of(index * size, size), size)

    barrier = pltpu.get_barrier_semaphore()
    for there in (to_x, to_y, to_pair):
        pl.semaphore_signal(barrier, inc=1, device_id=there, device_id_type=MESH)
    for way in ways:
        @pl.when(inside(z + way))
        def _():
            pl.semaphore_signal(barrier, inc=1, device_id=to_z(way), device_id_type=MESH)

    def remote(source, there, send, recv, target):
        return pltpu.make_async_remote_copy(
            source, there, send, recv, device_id=target, device_id_type=MESH
        )

    def in_part(ref, half):
        return ref.at[:, aligned(half, width)]

    def out_part(ref, half, j):
        return ref.at[:, pl.ds(pl.multiple_of(half * out_width + j * LANES, LANES), LANES)]

    own_in, own_out = (wpi_ref, wsi_ref), (wso_ref, wpo_ref)

    def in_at(m, sp):
        return w_in.at[m, aligned(sp, in_rows)]

    def out_at(m, sp):
        return w_out.at[m, :, aligned(sp, out_rows)]

    def weight_at(k, sp):
        return in_at(k, sp) if k < 2 else out_at(k - 2, sp)

    def parts(k, half, sp):
        if k < 2:
            return [(in_part(own_in[k], half), in_at(k, sp))]
        return [
            (out_part(own_out[k - 2], half, j), w_out.at[k - 2, j, aligned(sp, out_rows)])
            for j in range(chunk_count)
        ]

    def own_copy(k):
        return [pltpu.make_async_copy(source, there, own_sem.at[k]) for source, there in parts(k, x, me)]

    def own_wait(k):
        here = weight_at(k, me)
        pltpu.make_async_copy(here, here, own_sem.at[k]).wait()

    base = 4
    tok_copy = pltpu.make_async_copy(tok_ref, tok.at[tp, aligned(x, rows)], own_sem.at[base])

    def heads(ref, count):
        return ref.at[aligned(q, count)]

    loads = [
        pltpu.make_async_copy(heads(ref, count), there, own_sem.at[base + 1 + k])
        for ref, count, there, k in (
            (rr_ref, groups, rates.at[0], 0), (ri_ref, groups, rates.at[1], 0),
            (inr_ref, groups, matrices.at[0], 1), (ini_ref, groups, matrices.at[1], 1),
            (outr_ref, groups, matrices.at[2], 1), (outi_ref, groups, matrices.at[3], 1),
            (pw_ref, pool_groups, pool_own, 2),
        )
    ]
    for c in own_copy(0) + [tok_copy] + loads + [c for k in range(1, base) for c in own_copy(k)]:
        c.start()

    def x_send(k):
        for source, there in parts(k, 1 - x, me):
            remote(source, there, xw_send.at[0], xw_recv.at[k], to_x).start()

    @jax.named_scope("across_wait")
    def x_wait(k):
        here = weight_at(k, beside)
        remote(here, here, xw_send.at[0], xw_recv.at[k], to_x).wait_recv()

    def z_part(stage, h, at):
        return weight_at(stage, at * n_x + (x if h == 0 else 1 - x))

    def reach(way, stage):
        return inside(z + way) if stage < 3 else inner(z + way)

    def z_copy(d, stage, s, h):
        at = z - ways[d] * s
        there = z_part(stage, h, at)
        return remote(there, there, z_send.at[d, s], z_recv.at[stage, at, h], to_z(ways[d]))

    def toward(way, stage, inner_side):
        there = z + way
        if inner_side:
            return inner(there)
        return jnp.logical_and(reach(way, stage), jnp.logical_not(inner(there)))

    def z_own(stage, h, *sides, flows=(0, 1)):
        for inner_side in sides:
            for d in flows:
                @pl.when(toward(ways[d], stage, inner_side))
                def _():
                    z_copy(d, stage, 0, h).start()

    def z_arrive(d, stage, s, h):
        at = z - ways[d] * (s + 1)
        here = z_part(stage, h, at)
        remote(here, here, z_send.at[d, s], z_recv.at[stage, at, h], to_z(ways[d])).wait_recv()

    def z_relay(stage, s, h, inner_side, flows):
        for d in flows:
            @pl.when(jnp.logical_and(inside(z - ways[d] * (s + 1)), toward(ways[d], stage, inner_side)))
            def _():
                z_arrive(d, stage, s, h)
                z_copy(d, stage, s + 1, h).start()

    @jax.named_scope("relay_in")
    def relay_in(stage, h, flows=(0, 1)):
        z_relay(stage, 0, h, True, flows)

    @jax.named_scope("relay_out")
    def relay_out(stage, s, h, flows=(0, 1)):
        z_relay(stage, s, h, False, flows)

    @jax.named_scope("final_wait")
    def z_final(stage):
        here = rim if stage < 3 else middle
        for d in range(2):
            for s in range(n_z - 1):
                stays = jnp.logical_and(here, jnp.logical_not(reach(ways[d], stage)))
                @pl.when(jnp.logical_and(inside(z - ways[d] * (s + 1)), stays))
                def _():
                    for h in range(2):
                        z_arrive(d, stage, s, h)

    class Gather:
        def __init__(self, region, pair_region, send, recv, turned):
            self.region, self.pair_region, self.send, self.recv = region, pair_region, send, recv
            self.turned = turned

        def copy(self, slot, p):
            at_tp, at_x = (
                (tp, x), (tp, x), (across, x) if p == self.turned else (tp, 1 - x), (tp, x), (tp, 1 - x), (across, x), (across, 1 - x)
            )[slot]
            here = self.region(at_tp, at_x, p)
            recv = self.recv.at[2 * slot + p if slot < 3 else 6 if slot < 5 else 7]
            target = (to_x, to_y, to_x if p == self.turned else to_y, to_pair, to_pair, to_pair, to_pair)[slot]
            return remote(here, here, self.send, recv, target)

        def start(self, *slots, p):
            for slot in slots:
                self.copy(slot, p).start()

        @jax.named_scope("gather_wait")
        def wait(self, slot, p):
            here = self.region(*((tp, 1 - x), (across, x), (across, 1 - x))[slot], p)
            remote(here, here, self.send, self.recv.at[2 * slot + p], to_pair).wait_recv()

        @jax.named_scope("pair_wait")
        def wait_pair(self, at_tp, k):
            here = self.pair_region(at_tp)
            remote(here, here, self.send, self.recv.at[6 + k], to_pair).wait_recv()

        def relay_x(self, p):
            self.wait(0, p)
            self.start(*((4,) if p == self.turned else (2, 4)), p=p)

        def relay_y(self, p):
            self.wait(1, p)
            self.start(*((2, 5) if p == self.turned else (5,)), p=p)

        def relay_both(self, p):
            self.wait(2, p)
            self.start(6, p=p)

        def drain(self, sent):
            remote(sent, sent, self.send, self.recv.at[0], to_pair).wait_send()

    piece = rows // HALVES

    def tok_region(at_tp, at_x, p):
        return tok.at[at_tp, pl.ds(pl.multiple_of(at_x * rows + p * piece, piece), piece)]

    tokens = Gather(tok_region, lambda at_tp: tok.at[at_tp], tok_send.at[0], tok_recv, None)

    half_slab = slab // HALVES

    def act_gather(buffer, send, recv):
        def region(at_tp, at_x, p):
            return buffer.at[pl.ds(p * half_slab, half_slab), aligned(at_tp * n_x + at_x, width)]

        return Gather(region, lambda at_tp: buffer.at[:, aligned(at_tp, n_x * width)], send, recv, 1)

    acts = [act_gather(act.at[k], act_send.at[k], act_recv.at[k]) for k in range(2)]
    guests = act_gather(guest, guest_send.at[0], guest_recv)

    def guest_copy(p):
        cut = (pl.ds(p * half_slab, half_slab), aligned(q, width))
        return remote(
            act.at[(1, *cut)], guest.at[cut], guest_z_send.at[0], guest_z_recv.at[p], to_z(inward)
        )

    def part_rows(j, first):
        return partial.at[j, aligned(1 - x if first else x, rows)]

    def part_copy(j, first):
        here = part_rows(j, first)
        return remote(here, here, part_send.at[0], part_recv.at[j, 0 if first else 1], to_z(outward))

    pl.semaphore_wait(barrier, 3 + inside(z + 1).astype(jnp.int32) + inside(z - 1).astype(jnp.int32))

    both_sides = (True, False)
    x_send(0)
    own_wait(0)
    z_own(0, 0, *both_sides)
    own_wait(1)
    z_own(1, 0, *both_sides)
    tok_copy.wait()
    for p in range(HALVES):
        tokens.start(0, 1, 3, p=p)
    x_send(1)

    tile = iota((states, columns), 0) == iota((states, columns), 1) % states
    tile_exact, tile_half = tile.astype(f32), tile.astype(bf16)

    def exactly(a, b):
        return jnp.dot(a, b, precision=lax.Precision.HIGHEST, preferred_element_type=f32)

    factors = []

    @jax.named_scope("build_decay")
    def build_decay():
        for c in loads:
            c.wait()
        own_head = iota((groups, columns), 0) == iota((groups, columns), 1) // states

        def flat(a):
            return jnp.sum(jnp.where(own_head, exactly(a, tile_exact), 0.0), axis=0, keepdims=True)

        rate_real, rate_imag = flat(rates[0]), flat(rates[1])
        all_groups = step_ref.shape[1]
        head = iota((all_groups, columns), 0) == q * groups + iota((all_groups, columns), 1) // states
        log_step = exactly(jnp.broadcast_to(step_ref[...], (8, all_groups)), head.astype(f32))[0:1]
        step_size = jnp.exp(log_step) / (rows * n_sp)
        exponent, angle = rate_real * step_size, rate_imag * step_size
        magnitude = jnp.exp(exponent)
        cosine = jnp.cos(angle)
        decay_real, decay_imag = magnitude * cosine, magnitude * jnp.sin(angle)
        series = jnp.ones_like(exponent)
        for k in range(10, 1, -1):
            series = 1.0 + series * exponent * (1.0 / k)
        growth = jnp.where(jnp.abs(exponent) < 0.5, exponent * series, magnitude - 1.0)
        less_one = growth * cosine - 2.0 * jnp.square(jnp.sin(0.5 * angle))
        denominator = rate_real * rate_real + rate_imag * rate_imag
        factors.append((less_one * rate_real + decay_imag * rate_imag) / denominator)
        factors.append((decay_imag * rate_real - less_one * rate_imag) / denominator)
        dec_ref[0:1, :] = decay_real
        dec_ref[1:2, :] = decay_imag

    def spread(k):
        high, low = split(matrices[k].reshape(width, states))
        return dot(high, tile_half) + dot(low, tile_half)

    @jax.named_scope("build_drive")
    def build_drive(i):
        same = iota((width, columns), 0) // SSM_GROUP == iota((width, columns), 1) // states
        real, imag = spread(0), spread(1)
        if i == 0:
            drive = factors[0] * real - factors[1] * imag
        else:
            drive = factors[0] * imag + factors[1] * real
        for j, part in enumerate(split(jnp.where(same, drive, 0.0))):
            dmat[i, j] = part

    @jax.named_scope("build_read")
    def build_read(i):
        onto = (iota((columns, states), 0) % states == iota((columns, states), 1)).astype(bf16)
        same = iota((columns, width), 0) // states == iota((columns, width), 1) // SSM_GROUP
        for j, part in enumerate(split(matrices[2 + i].reshape(width, states))):
            rmat[i, j] = jnp.where(same, dot_nt(onto, part), 0.0).astype(bf16)

    @jax.named_scope("build_pool")
    def build_pool():
        onto = (iota((POOL_GROUP, width), 0) == iota((POOL_GROUP, width), 1) % POOL_GROUP).astype(bf16)
        same = iota((width, width), 0) // POOL_GROUP == iota((width, width), 1) // POOL_GROUP
        own = pool_own[...].reshape(width, POOL_GROUP)
        pmat[...] = jnp.where(same, dot(own, onto), 0.0).astype(bf16)

    @jax.named_scope("build_order")
    def build_order(i):
        a, b = iota((slab, slab), i), iota((slab, slab), 1 - i)
        order[i] = (b == (a % CHUNKS) * span + a // CHUNKS).astype(bf16)

    @jax.named_scope("take")
    def take(at_tp, first):
        cut = pl.ds(pl.multiple_of(at_tp * features, features), features)
        gain = gain_ref[:, cut]
        size = min(64, slab)

        def step(i, _):
            here = pl.ds(pl.multiple_of(i * size, size), size)
            block = tok[at_tp, here].astype(f32)
            square = block * block
            total = sum(square[:, k : k + LANES] for k in range(0, features, LANES))
            squares[here] = total if first else squares[here] + total
            scaled[here, cut] = (block * gain).astype(bf16)
            return 0

        lax.fori_loop(0, slab // size, step, 0)

    build_decay()
    build_drive(0)
    relay_in(0, 0)
    relay_out(0, 0, 0)
    x_wait(0)
    z_own(0, 1, *both_sides)
    relay_in(1, 0)
    tokens.relay_y(0)
    build_drive(1)
    relay_out(1, 0, 0)
    relay_out(0, 1, 0)
    build_read(0)
    relay_in(0, 1)
    relay_out(0, 0, 1)
    tokens.relay_x(0)
    tokens.relay_y(1)
    own_wait(2)
    own_wait(3)
    z_own(2, 0, True)
    build_read(1)
    build_order(0)
    build_order(1)
    build_pool()
    relay_out(0, 1, 1)
    tokens.relay_x(1)
    x_wait(1)
    z_own(1, 1, *both_sides)
    x_send(3)
    x_send(2)
    z_own(3, 0, True)
    relay_out(1, 1, 0)
    take(tp, True)
    tokens.relay_both(0)
    tokens.wait_pair(pair, 0)
    take(pair, False)
    relay_in(1, 1)
    tokens.relay_both(1)
    relay_in(2, 0)
    take(across, False)
    relay_out(1, 0, 1)
    tokens.wait_pair(both, 1)
    take(both, False)
    inverse = lax.rsqrt(jnp.sum(squares[...], axis=1, keepdims=True) / (features * n_tp) + epsilon)
    z_final(0)
    pool_in = (dot(scaled[...], w_in[0]) * inverse).astype(bf16)
    halo_out[...] = pool_in[slab - window_reach :]
    halo_copy = remote(halo_out, halo, halo_sem.at[0], halo_sem.at[1], to_z(1))

    @pl.when(inside(z + 1))
    def _():
        halo_copy.start()

    relay_out(1, 1, 1)
    relay_in(3, 0)

    @pl.when(rim)
    def _():
        x_wait(3)
        z_own(3, 1, True)


    def project_state():
        sums[0] = (dot(scaled[...], w_in[1]) * inverse).astype(bf16).astype(f32)

    @pl.when(middle)
    def _():
        project_state()

    @pl.when(z > 0)
    @jax.named_scope("halo_wait")
    def _():
        halo_copy.wait_recv()

    before = jnp.where(z == 0, jnp.zeros_like(halo), halo[...])
    whole = jnp.concatenate([before, pool_in], axis=0).astype(f32)
    window = jnp.left_shift(2, (q * pool_groups + iota((slab, width), 1) // POOL_GROUP) % 4)
    window_sums = jnp.zeros((slab, width), f32)
    running = whole
    for level in range(4):
        running = running + pltpu.roll(running, 2**level, 0)
        window_sums = jnp.where(window == 2 ** (level + 1), running[window_reach:], window_sums)
    position = z * slab + iota((slab, width), 0)
    divisor = jnp.minimum(position + 1, window).astype(f32)
    pooled = window_sums / divisor - whole[window_reach:]
    pooled_high, pooled_low = split(pooled)
    pool_gain = pg_ref[:, aligned(q, width)]
    projected = dot(pooled_high, pmat[...]) + dot(pooled_low, pmat[...])
    act[1, :, aligned(q, width)] = (projected * pool_gain).astype(bf16)

    @pl.when(rim)
    def _():
        for p in range(HALVES):
            guest_copy(p).start()

    @pl.when(middle)
    def _():
        for p in range(HALVES):
            acts[1].start(0, 1, 3, p=p)

    z_own(2, 0, False)

    x_wait(2)

    @pl.when(rim)
    def _():
        z_own(2, 1, True)

    @pl.when(middle)
    def _():
        x_wait(3)
        z_own(2, 1, True, False, flows=(1,))
        z_own(3, 1, True, flows=(1,))

    relay_out(2, 0, 0, (1,))
    z_final(1)

    @pl.when(rim)
    def _():
        project_state()

    state_in = sums[0].astype(bf16)
    relay_in(3, 1, (1,))
    signal = dot(order[0], state_in).astype(bf16)
    for i in range(2):
        push[i] = dot(signal, dmat[i, 0]) + dot(signal, dmat[i, 1])
    decay_real = jnp.broadcast_to(dec_ref[0:1, :], (CHUNKS, columns))
    decay_imag = jnp.broadcast_to(dec_ref[1:2, :], (CHUNKS, columns))

    def advance(p, carry):
        cut = pl.ds(pl.multiple_of(p * CHUNKS, CHUNKS), CHUNKS)
        real, imag = cmul(decay_real, decay_imag, *carry)
        real, imag = real + push[0, cut, :], imag + push[1, cut, :]
        push[0, cut, :] = real
        push[1, cut, :] = imag
        return real, imag

    zero = jnp.zeros((CHUNKS, columns), f32)
    end_real, end_imag = lax.fori_loop(0, span, advance, (zero, zero), unroll=4)

    def power(real, imag, count):
        out = None
        while count:
            if count % 2:
                out = (real, imag) if out is None else cmul(*out, real, imag)
            real, imag = cmul(real, imag, real, imag)
            count //= 2
        return out

    chunk_decay = power(dec_ref[0:1, :], dec_ref[1:2, :], span)
    block_decay = power(*chunk_decay, CHUNKS)
    row_zero = jnp.zeros((1, columns), f32)
    total = (row_zero, row_zero)
    for j in range(CHUNKS):
        moved = cmul(*chunk_decay, *total)
        total = (moved[0] + end_real[j : j + 1], moved[1] + end_imag[j : j + 1])
    which = iota((CHUNKS, columns), 0)
    ends[z] = jnp.where(which == 0, total[0], jnp.where(which == 1, total[1], 0.0))

    def end_copy(k):
        return remote(ends.at[z], ends.at[z], end_send.at[k - 1], end_recv.at[k - 1], (me + k * n_x, tp))

    for k in range(1, n_z):
        @pl.when(inside(z + k))
        def _():
            end_copy(k).start()

    @pl.when(middle)
    def _():
        for p in range(HALVES):
            here = guests.region(tp, x, p)
            with jax.named_scope("guest_wait"):
                remote(here, here, guest_z_send.at[0], guest_z_recv.at[p], to_pair).wait_recv()
            guests.start(0, 1, 3, p=p)

    @pl.when(middle)
    def _():
        z_own(2, 1, True, False, flows=(0,))
        z_own(3, 1, True, flows=(0,))

    relay_in(3, 1, (0,))
    relay_out(2, 0, 0, (0,))
    relay_out(2, 1, 0)

    @pl.when(middle)
    def _():
        for p in range(HALVES):
            acts[1].relay_x(p)
            acts[1].relay_y(p)

    relay_in(2, 1)
    relay_out(2, 0, 1, (1,))

    @pl.when(middle)
    def _():
        for p in range(HALVES):
            acts[1].relay_both(p)


    @pl.when(middle)
    def _():
        for p in range(HALVES):
            guests.relay_x(p)
            guests.relay_y(p)

    for k in range(1, n_z):
        @pl.when(inside(z - k))
        @jax.named_scope("ends_wait")
        def _():
            there = ends.at[z - k]
            remote(there, there, end_send.at[k - 1], end_recv.at[k - 1], to_z(1)).wait_recv()

    total = (row_zero, row_zero)
    for s in range(n_z - 1):
        moved = cmul(*block_decay, *total)
        use = s < z
        total = (
            jnp.where(use, moved[0] + ends[s, 0:1, :], total[0]),
            jnp.where(use, moved[1] + ends[s, 1:2, :], total[1]),
        )
    begin_real, begin_imag = zero, zero
    for j in range(CHUNKS):
        begin_real = jnp.where(which == j, total[0], begin_real)
        begin_imag = jnp.where(which == j, total[1], begin_imag)
        moved = cmul(*chunk_decay, *total)
        total = (moved[0] + end_real[j : j + 1], moved[1] + end_imag[j : j + 1])

    def add_carry(p, carry):
        cut = pl.ds(pl.multiple_of(p * CHUNKS, CHUNKS), CHUNKS)
        real, imag = cmul(decay_real, decay_imag, *carry)
        push[0, cut, :] = push[0, cut, :] + real
        push[1, cut, :] = push[1, cut, :] + imag
        return real, imag

    lax.fori_loop(0, span, add_carry, (begin_real, begin_imag), unroll=4)
    real_high, real_low = split(push[0])
    imag_high, imag_low = split(push[1])
    readout = dot(real_high, rmat[0, 0]) + dot(real_high, rmat[0, 1]) + dot(real_low, rmat[0, 0])
    readout -= dot(imag_high, rmat[1, 0]) + dot(imag_high, rmat[1, 1]) + dot(imag_low, rmat[1, 0])
    skip = skip_ref[:, aligned(q, width)]
    readout += skip * signal.astype(f32)
    shuffled = jax.nn.gelu(readout).astype(bf16)
    act[0, :, aligned(q, width)] = dot(order[1], shuffled).astype(bf16)
    for p in range(HALVES):
        acts[0].start(0, 1, 3, p=p)

    relay_out(2, 0, 1, (0,))
    relay_out(2, 1, 1)

    @pl.when(middle)
    def _():
        for p in range(HALVES):
            guests.relay_both(p)
        guests.wait_pair(pair, 0)
        guests.wait_pair(both, 1)

    z_final(3)

    @pl.when(middle)
    def _():
        for first in (True, False):
            cut = aligned(1 - x if first else x, rows)
            for j in range(chunk_count):
                partial[j, cut] = dot(guest[cut], w_out[1, j]).astype(bf16)
                part_copy(j, first).start()

    for p in range(HALVES):
        acts[0].relay_x(p)
        acts[0].relay_y(p)
        if p == 0:
            @pl.when(middle)
            def _():
                acts[1].wait_pair(pair, 0)
                acts[1].wait_pair(both, 1)
                for j in range(chunk_count):
                    sums[j] = dot(act[1], w_out[1, j])
    for p in range(HALVES):
        acts[0].relay_both(p)

    acts[0].wait_pair(pair, 0)
    acts[0].wait_pair(both, 1)
    z_final(2)

    def out_columns(half, j):
        return pl.ds(pl.multiple_of(half * out_width + j * LANES, LANES), LANES)

    def out_copy(j):
        return remote(made.at[j], out_ref.at[:, out_columns(x, j)], out_send.at[0], out_recv.at[0], to_x)

    here, there = aligned(x, rows), aligned(1 - x, rows)

    @pl.when(middle)
    def _():
        for j in range(chunk_count):
            made[j] = (dot(act[0, there], w_out[0, j]) + sums[j, there]).astype(bf16)
            out_copy(j).start()
        for j in range(chunk_count):
            mine = dot(act[0, here], w_out[0, j]) + sums[j, here]
            out_ref[:, out_columns(x, j)] = mine.astype(bf16)

    @pl.when(rim)
    def _():
        for cut in (there, here):
            for j in range(chunk_count):
                sums[j, cut] = dot(act[0, cut], w_out[0, j])

        @jax.named_scope("partial_wait")
        def part_wait(j, first):
            part = part_rows(j, first)
            recv = part_recv.at[j, 0 if first else 1]
            remote(part, part, part_send.at[0], recv, to_pair).wait_recv()

        for j in range(chunk_count):
            part_wait(j, True)
            made[j] = (sums[j, there] + partial[j, there].astype(f32)).astype(bf16)
            out_copy(j).start()
        for j in range(chunk_count):
            part_wait(j, False)
            out_ref[:, out_columns(x, j)] = (sums[j, here] + partial[j, here].astype(f32)).astype(bf16)

    @jax.named_scope("drain")
    def drain():
        sent = w_in.at[0, pl.ds(0, 2 * in_rows + 2 * chunk_count * out_rows)]
        remote(sent, sent, xw_send.at[0], xw_recv.at[0], to_x).wait_send()
        few = n_x * (2 * in_rows + chunk_count * out_rows)
        many = few + n_x * chunk_count * out_rows
        for d in range(2):
            for s in range(n_z - 1):
                any_sent = jnp.logical_and(inside(z + ways[d]), inside(z - ways[d] * s))
                for count, case in ((many, inner(z + ways[d])), (few, jnp.logical_not(inner(z + ways[d])))):
                    @pl.when(jnp.logical_and(any_sent, case))
                    def _():
                        sent = w_in.at[0, pl.ds(0, count)]
                        remote(sent, sent, z_send.at[d, s], z_recv.at[0, 0, 0], to_z(ways[d])).wait_send()
        tokens.drain(scaled.at[pl.ds(0, 7 * rows // n_tp)])
        acts[0].drain(act.at[0, :, pl.ds(0, 7 * width)])

        @pl.when(middle)
        def _():
            acts[1].drain(act.at[1, :, pl.ds(0, 7 * width)])
            guests.drain(guest.at[:, pl.ds(0, 7 * width)])
            remote(partial, partial, part_send.at[0], part_recv.at[0, 0], to_pair).wait_send()

        @pl.when(rim)
        def _():
            sent = act.at[1, :, aligned(q, width)]
            remote(sent, sent, guest_z_send.at[0], guest_z_recv.at[0], to_pair).wait_send()

        @pl.when(inside(z + 1))
        def _():
            halo_copy.wait_send()

        for k in range(1, n_z):
            @pl.when(inside(z + k))
            def _():
                end_copy(k).wait_send()

        remote(made, made, out_send.at[0], out_recv.at[0], to_x).wait_send()

    drain()
    with jax.named_scope("out_wait"):
        here = out_ref.at[:, aligned(1 - x, out_width)]
        remote(here, here, out_send.at[0], out_recv.at[0], to_x).wait_recv()


def slab_call(n_sp, n_tp, n_x, arrays):
    tokens, state_in_weight, state_out_weight = arrays[0], arrays[2], arrays[14]
    rows, features = tokens.shape
    in_rows, width = state_in_weight.shape
    out_rows, out_columns = state_out_weight.shape
    width //= n_x
    n_z, slab, chunk_count = n_sp // n_x, rows * n_x, out_columns // n_x // LANES
    groups, states = width // SSM_GROUP, arrays[4].shape[1]
    columns, pool_groups = groups * states, width // POOL_GROUP
    vmem = pl.BlockSpec(memory_space=pltpu.VMEM)
    anywhere = pl.BlockSpec(memory_space=pl.ANY)
    dma = pltpu.SemaphoreType.DMA
    return pl.pallas_call(
        functools.partial(slab_kernel, n_sp, n_tp, n_x, states),
        out_shape=pltpu.VMEM((rows, out_columns), bf16),
        in_specs=[anywhere, vmem] + [anywhere] * 4 + [vmem] + [anywhere] * 4 + [vmem, anywhere, vmem]
        + [anywhere] * 2,
        out_specs=vmem,
        scratch_shapes=[
            pltpu.VMEM((n_tp, slab, features), bf16),
            pltpu.VMEM((slab, features * n_tp), bf16),
            pltpu.VMEM((slab, LANES), f32),
            pltpu.VMEM((2, n_sp * in_rows, width), bf16),
            pltpu.VMEM((2, chunk_count, n_sp * out_rows, LANES), bf16),
            pltpu.VMEM((2, 2, width, columns), bf16),
            pltpu.VMEM((2, 2, columns, width), bf16),
            pltpu.VMEM((width, width), bf16),
            pltpu.VMEM((2, slab, columns), f32),
            pltpu.VMEM((2, slab, slab), bf16),
            pltpu.VMEM((window_reach, width), bf16),
            pltpu.VMEM((window_reach, width), bf16),
            pltpu.VMEM((n_z, CHUNKS, columns), f32),
            pltpu.VMEM((2, slab, n_tp * n_x * width), bf16),
            pltpu.VMEM((slab, n_tp * n_x * width), bf16),
            pltpu.VMEM((chunk_count, slab, LANES), bf16),
            pltpu.VMEM((chunk_count, slab, LANES), f32),
            pltpu.VMEM((chunk_count, rows, LANES), bf16),
            pltpu.VMEM((2, groups, states), f32),
            pltpu.VMEM((4, groups, SSM_GROUP, states), f32),
            pltpu.VMEM((pool_groups, POOL_GROUP, POOL_GROUP), bf16),
            pltpu.VMEM((2, columns), f32),
            dma((8,)),
            dma((1,)),
            dma((4,)),
            dma((2, n_z - 1)),
            dma((4, n_z, 2)),
            dma((1,)),
            dma((8,)),
            dma((2,)),
            dma((2, 8)),
            dma((2,)),
            dma((n_z - 1,)),
            dma((n_z - 1,)),
            dma((1,)),
            dma((1,)),
            dma((1,)),
            dma((8,)),
            dma((1,)),
            dma((HALVES,)),
            dma((1,)),
            dma((chunk_count, 2)),
        ],
        compiler_params=pltpu.CompilerParams(
            collective_id=0, has_side_effects=True, vmem_limit_bytes=60 * 2**20
        ),
    )(*arrays)


def slab_fits(n_sp, n_tp, n_x, features, in_rows, width, pool_width, out_rows, out_columns):
    return (
        n_x == 2 and n_tp == 4 and n_sp // n_x == 4 and features % LANES == 0 and width == n_x * LANES
        and pool_width == width and out_columns % (n_x * LANES) == 0
        and n_x * (2 * in_rows + out_columns // (n_x * LANES) * 2 * out_rows) <= n_sp * in_rows
    )


def body(
    n_sp, n_tp, n_x,
    tokens, norm_gain, state_in_weight, pool_in_weight, rate_real, rate_imag, log_step,
    input_real, input_imag, output_real, output_imag, skip_gain, pool_weight, pool_gain,
    state_out_weight, pool_out_weight,
):
    rows, features = tokens.shape
    in_rows, width = state_in_weight.shape
    pool_width = pool_in_weight.shape[1]
    out_rows, out_columns = state_out_weight.shape
    groups = width // SSM_GROUP
    states = rate_real.shape[1]
    columns = groups * states
    pool_groups = pool_width // POOL_GROUP
    if slab_fits(n_sp, n_tp, n_x, features, in_rows, width, pool_width, out_rows, out_columns):
        return slab_call(n_sp, n_tp, n_x, (
            tokens, norm_gain[None], state_in_weight, pool_in_weight, rate_real, rate_imag, log_step[None],
            jnp.swapaxes(input_real, 1, 2), jnp.swapaxes(input_imag, 1, 2), output_real, output_imag,
            skip_gain[None], pool_weight, pool_gain[None], state_out_weight, pool_out_weight,
        ))
    vmem = pl.BlockSpec(memory_space=pltpu.VMEM)
    anywhere = pl.BlockSpec(memory_space=pl.ANY)
    dma = pltpu.SemaphoreType.DMA
    return pl.pallas_call(
        functools.partial(kernel, n_sp, n_tp, n_x, states),
        out_shape=jax.ShapeDtypeStruct((rows, out_columns), bf16),
        in_specs=[anywhere, vmem] + [anywhere] * 4 + [vmem] + [anywhere] * 4 + [vmem, anywhere, vmem]
        + [anywhere] * 2,
        out_specs=vmem,
        scratch_shapes=[
            pltpu.VMEM((n_tp, rows, features), bf16),
            pltpu.VMEM((n_sp * in_rows, width), bf16),
            pltpu.VMEM((n_sp * in_rows, pool_width), bf16),
            pltpu.VMEM((n_sp * out_rows, out_columns), bf16),
            pltpu.VMEM((n_sp * out_rows, out_columns), bf16),
            pltpu.VMEM((rows, features * n_tp), bf16),
            pltpu.VMEM((2, 2, width, columns), bf16),
            pltpu.VMEM((2, 2, columns, width), bf16),
            pltpu.VMEM((pool_width, pool_width), bf16),
            pltpu.VMEM((2, rows, columns), f32),
            pltpu.VMEM((rows + window_reach, pool_width), bf16),
            pltpu.VMEM((window_reach, pool_width), bf16),
            pltpu.VMEM((n_sp, CHUNKS, columns), f32),
            pltpu.VMEM((2, n_tp, rows, width), bf16),
            pltpu.VMEM((rows, width), bf16),
            pltpu.VMEM((rows, pool_width), bf16),
            pltpu.VMEM((window_reach, pool_width), bf16),
            pltpu.VMEM((2, groups, states), f32),
            pltpu.VMEM((4, groups, SSM_GROUP, states), f32),
            pltpu.VMEM((pool_groups, POOL_GROUP, POOL_GROUP), bf16),
            pltpu.VMEM((2, columns), f32),
            dma((12,)),
            dma((4, 2, n_sp // 2, PIECES)),
            dma((4, 2, n_sp // 2, PIECES)),
            dma((n_tp - 1,)),
            dma((n_tp - 1,)),
            dma((2, n_tp - 1)),
            dma((2, n_tp - 1)),
            dma((2,)),
            dma((n_sp - 1,)),
            dma((n_sp - 1,)),
        ],
        compiler_params=pltpu.CompilerParams(
            collective_id=0, has_side_effects=True, vmem_limit_bytes=60 * 2**20
        ),
    )(
        tokens, norm_gain[None], state_in_weight, pool_in_weight, rate_real, rate_imag, log_step[None],
        jnp.swapaxes(input_real, 1, 2), jnp.swapaxes(input_imag, 1, 2), output_real, output_imag,
        skip_gain[None], pool_weight, pool_gain[None], state_out_weight, pool_out_weight,
    )


def solution(mesh):
    n_sp, n_tp = mesh.shape["sp"], mesh.shape["tp"]
    n_x = 2 ** ((n_sp.bit_length() - 1) // 2)
    both, whole = P("sp", "tp"), P()
    return jax.shard_map(
        functools.partial(body, n_sp, n_tp, n_x),
        mesh=mesh,
        in_specs=(both, whole, both, both) + (whole,) * 10 + (both, both),
        out_specs=both,
        check_vma=False,
    )
```
